32 devices in a mesh: fs: 8 (over z, y), tp: 4 (over x, core).
Axes of the slice: x: 2, y: 2, z: 4, core: 2. Of those that a mesh axis runs over, the one named last changes fastest.
Arguments:
- tokens: bfloat16 [640, 3072], P('tp'), may hold values from -6 to 6
- gain_first: float32 [3072], replicated, may hold values from 0.1 to 1.9
- gain_second: float32 [3072], replicated, may hold values from 0.1 to 1.9
- gate_first: float32 [3072, 8192], P('fs', 'tp'), may hold values from -0.109375 to 0.109375
- up_first: float32 [3072, 8192], P('fs', 'tp'), may hold values from -0.109375 to 0.109375
- down_first: float32 [8192, 3072], P('fs', 'tp'), may hold values from -0.09375 to 0.09375
- gate_second: float32 [3072, 8192], P('fs', 'tp'), may hold values from -0.109375 to 0.109375
- up_second: float32 [3072, 8192], P('fs', 'tp'), may hold values from -0.109375 to 0.109375
- down_second: float32 [8192, 3072], P('fs', 'tp'), may hold values from -0.09375 to 0.09375
Outputs:
- result_rows: bfloat16 [640, 3072], P('tp')
- serve_gate_first: bfloat16 [3072, 8192], P(None, 'fs')
- serve_up_first: bfloat16 [3072, 8192], P(None, 'fs')
- serve_down_first: bfloat16 [8192, 3072], P('fs')
- serve_gate_second: bfloat16 [3072, 8192], P(None, 'fs')
- serve_up_second: bfloat16 [3072, 8192], P(None, 'fs')
- serve_down_second: bfloat16 [8192, 3072], P('fs')
The draws below stay inside these ranges and needn't reach their ends.
All inputs are finite; a program needn't handle non-finite values.
Results may differ from the reference program's by a relative error of at most 0.011.
Values may be sent and summed in bfloat16 or wider, within the bound.
A program may use at most 192 MiB of HBM per device.

```python
import jax
import jax.numpy as jnp
from jax import lax

D = 3072
FF = 8192
TOKENS = 640


def with_spikes(drawn, own_key, source, target, shards_of, factor):
    def block_of(axis_at):
        return (jnp.arange(drawn.shape[axis_at]) // (drawn.shape[axis_at] // shards_of)).reshape((-1,) + (1,) * (drawn.ndim - 1 - axis_at))

    first = jax.random.permutation(own_key, shards_of)[block_of(target)]
    far = (block_of(target) + shards_of // 2) % shards_of
    return jnp.where((block_of(source) == first) | (block_of(source) == far), factor * drawn, drawn)


def level_of(stream_key, dims, split, smallest, largest):
    def one(dim, parts):
        draws = jax.random.uniform(jax.random.fold_in(jax.random.fold_in(stream_key, 6), dim), (parts,), jnp.float32, smallest / len(split), largest / len(split))
        return jnp.repeat(jnp.exp(draws), dims[dim] // parts).reshape((-1,) + (1,) * (len(dims) - dim - 1))

    level = one(*split[0])
    for cut in split[1:]:
        level = level * one(*cut)
    return level


def scatter_about(key, extent, deviation, most, shards=(), held_as=jnp.bfloat16):
    values = deviation * jax.random.normal(key, extent, jnp.float32)
    if shards:
        values = values * level_of(key, extent, shards, -0.22, 0.18)
    return jnp.clip(values, -most, most).astype(held_as)


def bell_draw_with(stream_key, dims, width, most, shards, heavy, kind=jnp.bfloat16):
    array = width * jax.random.normal(stream_key, dims, jnp.float32)
    if shards:
        array = array * level_of(stream_key, dims, shards, -0.22, 0.18)
    return jnp.clip(with_spikes(array, jax.random.fold_in(stream_key, 3), *heavy), -most, most).astype(kind)


def setup_inputs(seed: int = 0) -> dict:
    seeds = jax.random.split(jax.random.key(seed), 10)
    tokens = scatter_about(seeds[0], (TOKENS, D), 1.0, 6.0, ((0, 4),))
    gain_first = jnp.clip(1.0 + 0.18 * jax.random.normal(seeds[1], (D,), jnp.float32), 0.1, 1.9)
    gain_second = jnp.clip(1.0 + 0.18 * jax.random.normal(seeds[2], (D,), jnp.float32), 0.1, 1.9)
    gate_first = scatter_about(seeds[3], (D, FF), D ** -0.5, 0.109375, ((0, 8), (1, 4)), jnp.float32)
    up_first = scatter_about(seeds[4], (D, FF), D ** -0.5, 0.109375, ((0, 8), (1, 4)), jnp.float32)
    down_first = bell_draw_with(seeds[5], (FF, D), FF ** -0.5, 0.09375, ((0, 8), (1, 4)), (0, 1, 8, 2.0), jnp.float32)
    gate_second = scatter_about(seeds[6], (D, FF), D ** -0.5, 0.109375, ((0, 8), (1, 4)), jnp.float32)
    up_second = scatter_about(seeds[7], (D, FF), D ** -0.5, 0.109375, ((0, 8), (1, 4)), jnp.float32)
    down_second = bell_draw_with(seeds[8], (FF, D), FF ** -0.5, 0.09375, ((0, 8), (1, 4)), (0, 1, 8, 2.0), jnp.float32)
    return {"tokens": tokens, "gain_first": gain_first, "gain_second": gain_second, "gate_first": gate_first, "up_first": up_first, "down_first": down_first, "gate_second": gate_second, "up_second": up_second, "down_second": down_second}


def plain_norm(values):
    values = values.astype(jnp.float32)
    center = lax.optimization_barrier(jnp.mean(values, axis=-1, keepdims=True))
    spread = lax.optimization_barrier(jnp.mean(jnp.square(values - center), axis=-1, keepdims=True))
    return (values - center) * jax.lax.rsqrt(spread + 1e-05)

def fold_gain(weight, scales):
    return (scales[:, None] * weight).astype(jnp.bfloat16)

def half_step(normed, scales, w_gate, w_rising, w_down):
    gate_part = jnp.dot(normed, w_gate, preferred_element_type=jnp.float32)
    rising = jnp.dot(normed, w_rising, preferred_element_type=jnp.float32)
    hidden = (jax.nn.silu(gate_part) * rising).astype(jnp.bfloat16)
    block = jnp.dot(hidden, w_down, preferred_element_type=jnp.float32)
    mixed = 1.6817928 * scales[None, :] * normed.astype(jnp.float32) + 0.5 * block
    return plain_norm(mixed).astype(jnp.bfloat16)

def reference(tokens, gain_first, gain_second, gate_first, up_first, down_first, gate_second, up_second, down_second):
    serve_gate_first = fold_gain(gate_first, gain_first)
    serve_up_first = fold_gain(up_first, gain_first)
    serve_gate_second = fold_gain(gate_second, gain_second)
    serve_up_second = fold_gain(up_second, gain_second)
    serve_down_first = down_first.astype(jnp.bfloat16)
    serve_down_second = down_second.astype(jnp.bfloat16)
    normed_zero = plain_norm(tokens).astype(jnp.bfloat16)
    normed_one = half_step(normed_zero, gain_first, serve_gate_first, serve_up_first, serve_down_first)
    result_rows = half_step(normed_one, gain_second, serve_gate_second, serve_up_second, serve_down_second)
    return (result_rows, serve_gate_first, serve_up_first, serve_down_first, serve_gate_second, serve_up_second, serve_down_second)
```

```python
import functools

import jax
import jax.numpy as jnp
from jax import lax
from jax.experimental import pallas as pl
from jax.experimental.pallas import tpu as pltpu
from jax.sharding import PartitionSpec as P

MESH = pl.DeviceIdType.MESH
CORES = 2
SIDES = 2
RELAY = 6


def plain_norm(values):
    values = values.astype(jnp.float32)
    center = jnp.mean(values, axis=-1, keepdims=True)
    spread = jnp.mean(jnp.square(values - center), axis=-1, keepdims=True)
    return (values - center) * lax.rsqrt(spread + 1e-05)


def sum_over_hidden(partial_value):
    pieces = lax.all_to_all(
        partial_value.astype(jnp.bfloat16), "fs", split_axis=1, concat_axis=0, tiled=True
    )
    rows = partial_value.shape[0]
    pieces = pieces.reshape(-1, rows, pieces.shape[1]).astype(jnp.float32)
    summed = jnp.sum(pieces, axis=0).astype(jnp.bfloat16)
    return lax.all_gather(summed, "fs", axis=1, tiled=True).astype(jnp.float32)


def regroup(folded):
    spread = lax.all_to_all(folded, "tp", split_axis=0, concat_axis=1, tiled=True)
    parts = lax.axis_size("fs")
    rows = spread.shape[0]
    owned = lax.all_to_all(spread, "fs", split_axis=1, concat_axis=0, tiled=True)
    owned = owned.reshape(parts, rows, owned.shape[1])
    whole = lax.all_gather(owned, "tp", axis=1, tiled=True)
    return whole.reshape(-1, whole.shape[2])


def collect_plain(gate, up, down):
    return (
        regroup(gate),
        regroup(up),
        lax.all_gather(down, "tp", axis=1, tiled=True),
    )


def close_plain(partial_value, normed, scales):
    block = sum_over_hidden(partial_value)
    mixed = 1.6817928 * scales[None, :] * normed.astype(jnp.float32) + 0.5 * block
    return plain_norm(mixed).astype(jnp.bfloat16)


class Send:
    def __init__(self, when, src, dst, send, recv, to):
        self.when = when
        self.copy = pltpu.make_async_remote_copy(
            src_ref=src,
            dst_ref=dst,
            send_sem=send,
            recv_sem=recv,
            device_id=to,
            device_id_type=MESH,
        )

    def start(self):
        if self.when is None:
            self.copy.start()
        else:
            pl.when(self.when)(self.copy.start)

    def wait_send(self):
        if self.when is None:
            self.copy.wait_send()
        else:
            pl.when(self.when)(self.copy.wait_send)


def landed(ref, sem):
    pltpu.make_async_copy(ref, ref, sem).wait()


def collect_kernel(
    gate,
    up,
    down,
    whole_gate,
    whole_up,
    whole_down,
    passing,
    bounce,
    bounce_down,
    s_plane,
    s_cross,
    r_cross,
    s_pass,
    r_main,
    r_minor,
    s_main,
    s_minor,
    s_over,
    s_down,
    r_down,
    l_own,
    l_down,
):
    fs = lax.axis_index("fs")
    tp = lax.axis_index("tp")
    z, y = fs // SIDES, fs % SIDES
    x, c = tp // CORES, tp % CORES
    half = z // 2
    aligned = x == half
    primary = c == z % 2
    rows = gate.shape[0]
    width = whole_gate.shape[1]
    part = rows // RELAY
    main = rows - part
    here = lambda col: (fs, col)
    peer = (1 - x) * CORES + c
    sibling = x * CORES + 1 - c
    across = (1 - x) * CORES + 1 - c
    sources = (gate, up)
    targets = (whole_gate, whole_up)
    started = []

    def send(*args):
        one = Send(*args)
        one.start()
        started.append(one)

    def cols(ref, start, size, side):
        return ref.at[pl.ds(start, size), pl.ds(side * width, width)]

    def at(ref, owner, start, size):
        first = pl.multiple_of(owner * rows + start, 16)
        return ref.at[pl.ds(first, size), :]

    main_at = jnp.where(aligned, part, 0)
    over_at = jnp.where(aligned, main, 0)
    minor_at = jnp.where(aligned, 0, main)

    zone = x * CORES + c
    for m in range(2):
        for side in range(SIDES):
            owner = zone * SIDES + side
            unaligned = jnp.logical_not(aligned)
            send(
                unaligned,
                cols(sources[m], 0, main, side),
                passing.at[m, side],
                s_cross.at[m, side],
                r_cross.at[m, side],
                here(peer),
            )
            send(
                unaligned,
                cols(sources[m], part, main, side),
                at(targets[m], fs, part, main),
                s_plane.at[m, side],
                r_main.at[m, fs],
                (owner, tp),
            )
            send(
                jnp.logical_and(aligned, owner != fs),
                cols(sources[m], 0, rows, side),
                at(targets[m], fs, 0, rows),
                s_plane.at[m, side],
                r_main.at[m, fs],
                (owner, tp),
            )

    lanes = down.shape[1]

    def column(ref, col):
        return ref.at[:, pl.ds(pl.multiple_of(col * lanes, 128), lanes)]

    send(None, down, column(whole_down, tp), s_down.at[0], r_down.at[0], here(peer))
    send(None, down, column(whole_down, tp), s_down.at[1], r_down.at[1], here(sibling))

    home = jnp.logical_and(aligned, primary)

    def own(ref):
        return ref.at[:, pl.ds(pl.multiple_of(y * width, 128), width)]

    for m in range(2):
        send(
            home,
            own(sources[m]),
            at(targets[m], fs, 0, rows),
            s_over.at[m, fs],
            r_main.at[m, fs],
            here(peer),
        )
        send(
            home,
            own(sources[m]),
            at(targets[m], fs, 0, rows),
            s_main.at[m, fs],
            r_main.at[m, fs],
            here(sibling),
        )

    to_bounce = pltpu.make_async_copy(down, bounce_down, l_down)
    to_bounce.start()
    for m in range(2):
        fetch = pltpu.make_async_copy(own(sources[m]), bounce.at[m], l_own.at[m])
        pl.when(home)(fetch.start)
    to_bounce.wait()
    put_down = pltpu.make_async_copy(bounce_down, column(whole_down, tp), l_down)
    put_down.start()
    puts = []
    for m in range(2):
        fetch = pltpu.make_async_copy(own(sources[m]), bounce.at[m], l_own.at[m])
        put = pltpu.make_async_copy(
            bounce.at[m], at(targets[m], fs, 0, rows), l_own.at[m]
        )
        puts.append(put)
        pl.when(home)(fetch.wait)
        pl.when(home)(put.start)

    far_zone = (1 - x) * CORES + c
    for m in range(2):
        for side in range(SIDES):
            pl.when(aligned)(
                functools.partial(landed, passing.at[m, side], r_cross.at[m, side])
            )
            send(
                aligned,
                passing.at[m, side],
                at(targets[m], fs, 0, main),
                s_pass.at[m, side],
                r_main.at[m, fs],
                (far_zone * SIDES + side, tp),
            )

    for m in range(2):
        for step in range(2 * SIDES):
            owner = half * 2 * SIDES + (fs + step) % (2 * SIDES)
            is_home = owner == fs
            block = at(targets[m], owner, 0, rows)
            if step == 0:
                got = jnp.logical_and(primary, jnp.logical_not(aligned))
            else:
                got = primary
            pl.when(got)(functools.partial(landed, block, r_main.at[m, owner]))
            send(
                got,
                block,
                block,
                s_main.at[m, owner],
                r_main.at[m, owner],
                here(sibling),
            )
            if step:
                send(
                    jnp.logical_and(primary, aligned),
                    block,
                    block,
                    s_over.at[m, owner],
                    r_main.at[m, owner],
                    here(peer),
                )

    landed(column(whole_down, peer), r_down.at[0])
    send(
        None,
        column(whole_down, peer),
        column(whole_down, peer),
        s_down.at[2],
        r_down.at[2],
        here(sibling),
    )

    for m in range(2):
        for step in range(2 * SIDES):
            owner = (1 - half) * 2 * SIDES + (fs + step) % (2 * SIDES)
            block = at(targets[m], owner, main_at, main)
            over = at(targets[m], owner, over_at, part)
            pl.when(primary)(functools.partial(landed, block, r_main.at[m, owner]))
            send(
                primary,
                over,
                over,
                s_over.at[m, owner],
                r_minor.at[m, owner],
                here(peer),
            )
            send(
                primary,
                block,
                block,
                s_main.at[m, owner],
                r_main.at[m, owner],
                here(sibling),
            )
    for m in range(2):
        for step in range(2 * SIDES):
            owner = (1 - half) * 2 * SIDES + (fs + step) % (2 * SIDES)
            block = at(targets[m], owner, minor_at, part)
            pl.when(primary)(functools.partial(landed, block, r_minor.at[m, owner]))
            send(
                primary,
                block,
                block,
                s_minor.at[m, owner],
                r_minor.at[m, owner],
                here(sibling),
            )

    second = jnp.logical_not(primary)
    for m in range(2):
        for step in range(2 * SIDES):
            owner = half * 2 * SIDES + (fs + step) % (2 * SIDES)
            pl.when(second)(
                functools.partial(
                    landed, at(targets[m], owner, 0, rows), r_main.at[m, owner]
                )
            )
            owner = (1 - half) * 2 * SIDES + (fs + step) % (2 * SIDES)
            pl.when(second)(
                functools.partial(
                    landed, at(targets[m], owner, main_at, main), r_main.at[m, owner]
                )
            )
            pl.when(second)(
                functools.partial(
                    landed, at(targets[m], owner, minor_at, part), r_minor.at[m, owner]
                )
            )
    landed(column(whole_down, sibling), r_down.at[1])
    landed(column(whole_down, across), r_down.at[2])
    put_down.wait()
    for put in puts:
        pl.when(home)(put.wait)
    for one in started:
        one.wait_send()


def collect(gate, up, down):
    rows, columns = gate.shape
    fs, tp = lax.axis_size("fs"), lax.axis_size("tp")
    width = columns * tp // fs
    main = rows - rows // RELAY
    grid_like = jax.ShapeDtypeStruct((rows * fs, width), jnp.bfloat16)
    any_place = pl.BlockSpec(memory_space=pl.ANY)
    dma = pltpu.SemaphoreType.DMA
    return pl.pallas_call(
        collect_kernel,
        out_shape=(
            grid_like,
            grid_like,
            jax.ShapeDtypeStruct((down.shape[0], down.shape[1] * tp), jnp.bfloat16),
        ),
        in_specs=[any_place] * 3,
        out_specs=(any_place,) * 3,
        scratch_shapes=[
            pltpu.VMEM((2, SIDES, main, width), jnp.bfloat16),
            pltpu.VMEM((2, rows, width), jnp.bfloat16),
            pltpu.VMEM(down.shape, jnp.bfloat16),
            dma((2, SIDES)),
            dma((2, SIDES)),
            dma((2, SIDES)),
            dma((2, SIDES)),
            dma((2, fs)),
            dma((2, fs)),
            dma((2, fs)),
            dma((2, fs)),
            dma((2, fs)),
            dma((3,)),
            dma((3,)),
            dma((2,)),
            dma(()),
        ],
        compiler_params=pltpu.CompilerParams(has_side_effects=True),
    )(gate, up, down)


def close_kernel(
    partial_value, normed, scales, out, landing, summed, full, s_part, r_part, s_sum, r_sum
):
    fs = lax.axis_index("fs")
    tp = lax.axis_index("tp")
    count = lax.axis_size("fs")
    rows, width = summed.shape

    def lanes(index):
        return pl.ds(pl.multiple_of(index * width, 128), width)

    copies = []
    for step in range(1, count):
        to = (fs + step) % count
        copy = pltpu.make_async_remote_copy(
            src_ref=partial_value.at[:, lanes(to)],
            dst_ref=landing.at[step - 1],
            send_sem=s_part.at[step - 1],
            recv_sem=r_part.at[step - 1],
            device_id=(to, tp),
            device_id_type=MESH,
        )
        copy.start()
        copies.append(copy)
    for copy in copies:
        copy.wait_recv()
    total = partial_value[:, lanes(fs)].astype(jnp.float32)
    for step in range(1, count):
        total += landing[step - 1].astype(jnp.float32)
    summed[...] = total.astype(jnp.bfloat16)
    sums = []
    for step in range(1, count):
        to = (fs + step) % count
        copy = pltpu.make_async_remote_copy(
            src_ref=summed,
            dst_ref=full.at[fs],
            send_sem=s_sum.at[step - 1],
            recv_sem=r_sum.at[step - 1],
            device_id=(to, tp),
            device_id_type=MESH,
        )
        copy.start()
        sums.append(copy)
    full[fs] = summed[...]
    for copy in sums:
        copy.wait_recv()
    step = 16

    def norm(index, carry):
        some = pl.ds(pl.multiple_of(index * step, step), step)
        block = jnp.concatenate(
            [full[k, some, :].astype(jnp.float32) for k in range(count)], axis=1
        )
        mixed = 1.6817928 * scales[...] * normed[some, :].astype(jnp.float32) + 0.5 * block
        out[some, :] = plain_norm(mixed).astype(jnp.bfloat16)
        return carry

    lax.fori_loop(0, rows // step, norm, 0)
    for copy in copies + sums:
        copy.wait_send()


def close(partial_value, normed, scales):
    rows, width = normed.shape
    count = lax.axis_size("fs")
    piece = width // count
    vmem = pl.BlockSpec(memory_space=pltpu.VMEM)
    dma = pltpu.SemaphoreType.DMA
    return pl.pallas_call(
        close_kernel,
        out_shape=jax.ShapeDtypeStruct((rows, width), jnp.bfloat16),
        in_specs=[vmem] * 3,
        out_specs=vmem,
        scratch_shapes=[
            pltpu.VMEM((count - 1, rows, piece), jnp.bfloat16),
            pltpu.VMEM((rows, piece), jnp.bfloat16),
            pltpu.VMEM((count, rows, piece), jnp.bfloat16),
            dma((count - 1,)),
            dma((count - 1,)),
            dma((count - 1,)),
            dma((count - 1,)),
        ],
        compiler_params=pltpu.CompilerParams(has_side_effects=True),
    )(partial_value.astype(jnp.bfloat16), normed, scales[None, :])


def on_device(
    use_kernels,
    tokens,
    gain_first,
    gain_second,
    gate_first,
    up_first,
    down_first,
    gate_second,
    up_second,
    down_second,
):
    row_count = gate_first.shape[0]
    offset = lax.axis_index("fs") * row_count
    bring = collect if use_kernels else collect_plain
    finish = close if use_kernels else close_plain

    def fold_gain(weight, scales):
        picked = lax.dynamic_slice_in_dim(scales, offset, row_count, 0)
        return (picked[:, None] * weight).astype(jnp.bfloat16)

    def half_step(normed, scales, w_gate, w_rising, w_down):
        gate_part = jnp.dot(normed, w_gate, preferred_element_type=jnp.float32)
        rising = jnp.dot(normed, w_rising, preferred_element_type=jnp.float32)
        hidden = (jax.nn.silu(gate_part) * rising).astype(jnp.bfloat16)
        partial_value = jnp.dot(hidden, w_down, preferred_element_type=jnp.float32)
        return finish(partial_value, normed, scales)

    first = bring(
        fold_gain(gate_first, gain_first),
        fold_gain(up_first, gain_first),
        down_first.astype(jnp.bfloat16),
    )
    second = bring(
        fold_gain(gate_second, gain_second),
        fold_gain(up_second, gain_second),
        down_second.astype(jnp.bfloat16),
    )
    normed_zero = plain_norm(tokens).astype(jnp.bfloat16)
    normed_one = half_step(normed_zero, gain_first, *first)
    result_rows = half_step(normed_one, gain_second, *second)
    return (result_rows, *first, *second)


def solution(mesh):
    fs, tp = mesh.shape["fs"], mesh.shape["tp"]
    use_kernels = tp == 2 * CORES and fs == tp * SIDES
    placed = (P("tp", None), P(), P()) + (P("fs", "tp"),) * 6
    served = (P(None, "fs"), P(None, "fs"), P("fs", None))
    return jax.shard_map(
        functools.partial(on_device, use_kernels),
        mesh=mesh,
        in_specs=placed,
        out_specs=(P("tp", None),) + served + served,
        check_vma=False,
    )
```

```python
import functools

import jax
import jax.numpy as jnp
from jax import lax
from jax.experimental import pallas as pl
from jax.experimental.pallas import tpu as pltpu
from jax.sharding import PartitionSpec as P

MESH = pl.DeviceIdType.MESH
CORES = 2
SIDES = 2
CUTS = 4
RELAY = 6


def plain_norm(values):
    values = values.astype(jnp.float32)
    center = jnp.mean(values, axis=-1, keepdims=True)
    spread = jnp.mean(jnp.square(values - center), axis=-1, keepdims=True)
    return (values - center) * lax.rsqrt(spread + 1e-05)


def sum_over_hidden(partial_value):
    pieces = lax.all_to_all(
        partial_value.astype(jnp.bfloat16), "fs", split_axis=1, concat_axis=0, tiled=True
    )
    rows = partial_value.shape[0]
    pieces = pieces.reshape(-1, rows, pieces.shape[1]).astype(jnp.float32)
    summed = jnp.sum(pieces, axis=0).astype(jnp.bfloat16)
    return lax.all_gather(summed, "fs", axis=1, tiled=True).astype(jnp.float32)


def regroup(folded):
    spread = lax.all_to_all(folded, "tp", split_axis=0, concat_axis=1, tiled=True)
    parts = lax.axis_size("fs")
    rows = spread.shape[0]
    owned = lax.all_to_all(spread, "fs", split_axis=1, concat_axis=0, tiled=True)
    owned = owned.reshape(parts, rows, owned.shape[1])
    whole = lax.all_gather(owned, "tp", axis=1, tiled=True)
    return whole.reshape(-1, whole.shape[2])


def collect_plain(gate, up, down):
    return (
        regroup(gate),
        regroup(up),
        lax.all_gather(down, "tp", axis=1, tiled=True),
    )


def close_plain(partial_value, normed, scales):
    block = sum_over_hidden(partial_value)
    mixed = 1.6817928 * scales[None, :] * normed.astype(jnp.float32) + 0.5 * block
    return plain_norm(mixed).astype(jnp.bfloat16)


class Send:
    def __init__(self, when, src, dst, send, recv, to):
        self.when = when
        self.copy = pltpu.make_async_remote_copy(
            src_ref=src,
            dst_ref=dst,
            send_sem=send,
            recv_sem=recv,
            device_id=to,
            device_id_type=MESH,
        )

    def start(self):
        if self.when is None:
            self.copy.start()
        else:
            pl.when(self.when)(self.copy.start)

    def wait_send(self):
        if self.when is None:
            self.copy.wait_send()
        else:
            pl.when(self.when)(self.copy.wait_send)


def landed(ref, sem):
    pltpu.make_async_copy(ref, ref, sem).wait()


def collect_kernel(
    gate,
    up,
    down,
    whole_gate,
    whole_up,
    whole_down,
    passing,
    bounce,
    bounce_down,
    s_plane,
    s_cross,
    r_cross,
    s_pass,
    r_main,
    r_minor,
    s_main,
    s_minor,
    s_over,
    s_down,
    r_down,
    l_own,
    l_down,
):
    fs = lax.axis_index("fs")
    tp = lax.axis_index("tp")
    z, y = fs // SIDES, fs % SIDES
    x, c = tp // CORES, tp % CORES
    half = z // 2
    aligned = x == half
    primary = c == z % 2
    rows = gate.shape[0]
    width = whole_gate.shape[1]
    part = rows // RELAY
    main = rows - part
    here = lambda col: (fs, col)
    peer = (1 - x) * CORES + c
    sibling = x * CORES + 1 - c
    across = (1 - x) * CORES + 1 - c
    sources = (gate, up)
    targets = (whole_gate, whole_up)
    started = []

    def send(*args):
        one = Send(*args)
        one.start()
        started.append(one)

    def cols(ref, start, size, side):
        return ref.at[pl.ds(start, size), pl.ds(side * width, width)]

    def at(ref, owner, start, size):
        first = pl.multiple_of(owner * rows + start, 16)
        return ref.at[pl.ds(first, size), :]

    main_at = jnp.where(aligned, part, 0)
    over_at = jnp.where(aligned, main, 0)
    minor_at = jnp.where(aligned, 0, main)

    zone = x * CORES + c
    for m in range(2):
        for side in range(SIDES):
            owner = zone * SIDES + side
            unaligned = jnp.logical_not(aligned)
            for k in range(RELAY - 1):
                send(
                    unaligned,
                    cols(sources[m], k * part, part, side),
                    passing.at[m, side, k],
                    s_cross.at[m, side, k],
                    r_cross.at[m, side, k],
                    here(peer),
                )
            send(
                unaligned,
                cols(sources[m], part, main, side),
                at(targets[m], fs, part, main),
                s_plane.at[m, side],
                r_main.at[m, fs],
                (owner, tp),
            )
            send(
                jnp.logical_and(aligned, owner != fs),
                cols(sources[m], 0, rows, side),
                at(targets[m], fs, 0, rows),
                s_plane.at[m, side],
                r_main.at[m, fs],
                (owner, tp),
            )

    lanes = down.shape[1]

    def column(ref, col):
        return ref.at[:, pl.ds(pl.multiple_of(col * lanes, 128), lanes)]

    send(None, down, column(whole_down, tp), s_down.at[0], r_down.at[0], here(peer))
    send(None, down, column(whole_down, tp), s_down.at[1], r_down.at[1], here(sibling))

    home = jnp.logical_and(aligned, primary)

    def own(ref):
        return ref.at[:, pl.ds(pl.multiple_of(y * width, 128), width)]

    for m in range(2):
        send(
            home,
            own(sources[m]),
            at(targets[m], fs, 0, rows),
            s_over.at[m, fs],
            r_main.at[m, fs],
            here(peer),
        )
        send(
            home,
            own(sources[m]),
            at(targets[m], fs, 0, rows),
            s_main.at[m, fs],
            r_main.at[m, fs],
            here(sibling),
        )

    to_bounce = pltpu.make_async_copy(down, bounce_down, l_down)
    to_bounce.start()
    for m in range(2):
        fetch = pltpu.make_async_copy(own(sources[m]), bounce.at[m], l_own.at[m])
        pl.when(home)(fetch.start)
    to_bounce.wait()
    put_down = pltpu.make_async_copy(bounce_down, column(whole_down, tp), l_down)
    put_down.start()
    puts = []
    for m in range(2):
        fetch = pltpu.make_async_copy(own(sources[m]), bounce.at[m], l_own.at[m])
        put = pltpu.make_async_copy(
            bounce.at[m], at(targets[m], fs, 0, rows), l_own.at[m]
        )
        puts.append(put)
        pl.when(home)(fetch.wait)
        pl.when(home)(put.start)

    far_zone = (1 - x) * CORES + c
    for m in range(2):
        for side in range(SIDES):
            for k in range(RELAY - 1):
                held = passing.at[m, side, k]
                pl.when(aligned)(
                    functools.partial(landed, held, r_cross.at[m, side, k])
                )
                send(
                    aligned,
                    held,
                    at(targets[m], fs, k * part, part),
                    s_pass.at[m, side, k],
                    r_main.at[m, fs],
                    (far_zone * SIDES + side, tp),
                )

    for m in range(2):
        for step in range(2 * SIDES):
            owner = half * 2 * SIDES + (fs + step) % (2 * SIDES)
            is_home = owner == fs
            block = at(targets[m], owner, 0, rows)
            if step == 0:
                got = jnp.logical_and(primary, jnp.logical_not(aligned))
            else:
                got = primary
            pl.when(got)(functools.partial(landed, block, r_main.at[m, owner]))
            send(
                got,
                block,
                block,
                s_main.at[m, owner],
                r_main.at[m, owner],
                here(sibling),
            )
            if step:
                send(
                    jnp.logical_and(primary, aligned),
                    block,
                    block,
                    s_over.at[m, owner],
                    r_main.at[m, owner],
                    here(peer),
                )

    landed(column(whole_down, peer), r_down.at[0])
    send(
        None,
        column(whole_down, peer),
        column(whole_down, peer),
        s_down.at[2],
        r_down.at[2],
        here(sibling),
    )

    for m in range(2):
        for step in range(2 * SIDES):
            owner = (1 - half) * 2 * SIDES + (fs + step) % (2 * SIDES)
            block = at(targets[m], owner, main_at, main)
            over = at(targets[m], owner, over_at, part)
            pl.when(primary)(functools.partial(landed, block, r_main.at[m, owner]))
            send(
                primary,
                over,
                over,
                s_over.at[m, owner],
                r_minor.at[m, owner],
                here(peer),
            )
            send(
                primary,
                block,
                block,
                s_main.at[m, owner],
                r_main.at[m, owner],
                here(sibling),
            )
    for m in range(2):
        for step in range(2 * SIDES):
            owner = (1 - half) * 2 * SIDES + (fs + step) % (2 * SIDES)
            block = at(targets[m], owner, minor_at, part)
            pl.when(primary)(functools.partial(landed, block, r_minor.at[m, owner]))
            send(
                primary,
                block,
                block,
                s_minor.at[m, owner],
                r_minor.at[m, owner],
                here(sibling),
            )

    second = jnp.logical_not(primary)
    for m in range(2):
        for step in range(2 * SIDES):
            owner = half * 2 * SIDES + (fs + step) % (2 * SIDES)
            pl.when(second)(
                functools.partial(
                    landed, at(targets[m], owner, 0, rows), r_main.at[m, owner]
                )
            )
            owner = (1 - half) * 2 * SIDES + (fs + step) % (2 * SIDES)
            pl.when(second)(
                functools.partial(
                    landed, at(targets[m], owner, main_at, main), r_main.at[m, owner]
                )
            )
            pl.when(second)(
                functools.partial(
                    landed, at(targets[m], owner, minor_at, part), r_minor.at[m, owner]
                )
            )
    landed(column(whole_down, sibling), r_down.at[1])
    landed(column(whole_down, across), r_down.at[2])
    put_down.wait()
    for put in puts:
        pl.when(home)(put.wait)
    for one in started:
        one.wait_send()


def collect(gate, up, down):
    rows, columns = gate.shape
    fs, tp = lax.axis_size("fs"), lax.axis_size("tp")
    width = columns * tp // fs
    part = rows // RELAY
    grid_like = jax.ShapeDtypeStruct((rows * fs, width), jnp.bfloat16)
    any_place = pl.BlockSpec(memory_space=pl.ANY)
    dma = pltpu.SemaphoreType.DMA
    return pl.pallas_call(
        collect_kernel,
        out_shape=(
            grid_like,
            grid_like,
            jax.ShapeDtypeStruct((down.shape[0], down.shape[1] * tp), jnp.bfloat16),
        ),
        in_specs=[any_place] * 3,
        out_specs=(any_place,) * 3,
        scratch_shapes=[
            pltpu.VMEM((2, SIDES, RELAY - 1, part, width), jnp.bfloat16),
            pltpu.VMEM((2, rows, width), jnp.bfloat16),
            pltpu.VMEM(down.shape, jnp.bfloat16),
            dma((2, SIDES)),
            dma((2, SIDES, RELAY - 1)),
            dma((2, SIDES, RELAY - 1)),
            dma((2, SIDES, RELAY - 1)),
            dma((2, fs)),
            dma((2, fs)),
            dma((2, fs)),
            dma((2, fs)),
            dma((2, fs)),
            dma((3,)),
            dma((3,)),
            dma((2,)),
            dma(()),
        ],
        compiler_params=pltpu.CompilerParams(has_side_effects=True),
    )(gate, up, down)


def half_kernel(
    normed,
    gate,
    up,
    down,
    serve_gate,
    serve_up,
    serve_down,
    partial_value,
    v_gate,
    v_up,
    v_down,
    gate_sum,
    up_sum,
    arrive,
    leave,
):
    deep = gate.shape[0] // CUTS
    wide = down.shape[1] // CUTS

    def rows_of(ref, k):
        return ref.at[pl.ds(k * deep, deep), :]

    def lanes_of(ref, k):
        return ref.at[:, pl.ds(k * wide, wide)]

    plan = [(gate, v_gate, serve_gate, rows_of), (up, v_up, serve_up, rows_of)]
    plan.append((down, v_down, serve_down, lanes_of))

    def coming(m, k):
        src, held, _, cut = plan[m]
        return pltpu.make_async_copy(cut(src, k), cut(held, k), arrive.at[m, k])

    def going(m, k):
        _, held, dst, cut = plan[m]
        return pltpu.make_async_copy(cut(held, k), cut(dst, k), leave.at[m, k])

    for k in range(CUTS):
        coming(0, k).start()
        coming(1, k).start()
    for k in range(CUTS):
        coming(2, k).start()
    for k in range(CUTS):
        n = normed[:, k * deep : (k + 1) * deep]
        for m, total in ((0, gate_sum), (1, up_sum)):
            coming(m, k).wait()
            going(m, k).start()
            term = jnp.dot(
                n,
                plan[m][1][k * deep : (k + 1) * deep, :],
                preferred_element_type=jnp.float32,
            )
            if k:
                total[...] += term
            else:
                total[...] = term
    hidden = (jax.nn.silu(gate_sum[...]) * up_sum[...]).astype(jnp.bfloat16)
    for k in range(CUTS):
        coming(2, k).wait()
        going(2, k).start()
        partial_value[:, k * wide : (k + 1) * wide] = jnp.dot(
            hidden,
            v_down[:, k * wide : (k + 1) * wide],
            preferred_element_type=jnp.float32,
        ).astype(jnp.bfloat16)
    for m in range(3):
        for k in range(CUTS):
            going(m, k).wait()


def half_block(normed, gate, up, down):
    rows, width = normed.shape
    vmem = pl.BlockSpec(memory_space=pltpu.VMEM)
    any_place = pl.BlockSpec(memory_space=pl.ANY)
    same = lambda a: jax.ShapeDtypeStruct(a.shape, a.dtype)
    *served, partial_value = pl.pallas_call(
        half_kernel,
        out_shape=(same(gate), same(up), same(down), same(normed)),
        in_specs=[vmem] + [any_place] * 3,
        out_specs=(any_place,) * 3 + (vmem,),
        scratch_shapes=[
            pltpu.VMEM(gate.shape, gate.dtype),
            pltpu.VMEM(up.shape, up.dtype),
            pltpu.VMEM(down.shape, down.dtype),
            pltpu.VMEM((rows, gate.shape[1]), jnp.float32),
            pltpu.VMEM((rows, gate.shape[1]), jnp.float32),
            pltpu.SemaphoreType.DMA((3, CUTS)),
            pltpu.SemaphoreType.DMA((3, CUTS)),
        ],
        compiler_params=pltpu.CompilerParams(vmem_limit_bytes=60 * 2**20),
        cost_estimate=pl.CostEstimate(
            flops=6 * rows * gate.size, bytes_accessed=12 * gate.size, transcendentals=0
        ),
    )(normed, gate, up, down)
    return served, partial_value


def half_block_plain(normed, w_gate, w_rising, w_down):
    gate_part = jnp.dot(normed, w_gate, preferred_element_type=jnp.float32)
    rising = jnp.dot(normed, w_rising, preferred_element_type=jnp.float32)
    hidden = (jax.nn.silu(gate_part) * rising).astype(jnp.bfloat16)
    partial_value = jnp.dot(hidden, w_down, preferred_element_type=jnp.float32)
    return (w_gate, w_rising, w_down), partial_value


def close_kernel(
    partial_value, normed, scales, out, landing, summed, full, s_part, r_part, s_sum, r_sum
):
    fs = lax.axis_index("fs")
    tp = lax.axis_index("tp")
    count = lax.axis_size("fs")
    rows, width = summed.shape

    def lanes(index):
        return pl.ds(pl.multiple_of(index * width, 128), width)

    copies = []
    for step in range(1, count):
        to = (fs + step) % count
        copy = pltpu.make_async_remote_copy(
            src_ref=partial_value.at[:, lanes(to)],
            dst_ref=landing.at[step - 1],
            send_sem=s_part.at[step - 1],
            recv_sem=r_part.at[step - 1],
            device_id=(to, tp),
            device_id_type=MESH,
        )
        copy.start()
        copies.append(copy)
    for copy in copies:
        copy.wait_recv()
    total = partial_value[:, lanes(fs)].astype(jnp.float32)
    for step in range(1, count):
        total += landing[step - 1].astype(jnp.float32)
    summed[...] = total.astype(jnp.bfloat16)
    sums = []
    for step in range(1, count):
        to = (fs + step) % count
        copy = pltpu.make_async_remote_copy(
            src_ref=summed,
            dst_ref=full.at[fs],
            send_sem=s_sum.at[step - 1],
            recv_sem=r_sum.at[step - 1],
            device_id=(to, tp),
            device_id_type=MESH,
        )
        copy.start()
        sums.append(copy)
    full[fs] = summed[...]
    for copy in sums:
        copy.wait_recv()
    step = 16

    def norm(index, carry):
        some = pl.ds(pl.multiple_of(index * step, step), step)
        block = jnp.concatenate(
            [full[k, some, :].astype(jnp.float32) for k in range(count)], axis=1
        )
        mixed = 1.6817928 * scales[...] * normed[some, :].astype(jnp.float32) + 0.5 * block
        out[some, :] = plain_norm(mixed).astype(jnp.bfloat16)
        return carry

    lax.fori_loop(0, rows // step, norm, 0)
    for copy in copies + sums:
        copy.wait_send()


def close(partial_value, normed, scales):
    rows, width = normed.shape
    count = lax.axis_size("fs")
    piece = width // count
    vmem = pl.BlockSpec(memory_space=pltpu.VMEM)
    dma = pltpu.SemaphoreType.DMA
    return pl.pallas_call(
        close_kernel,
        out_shape=jax.ShapeDtypeStruct((rows, width), jnp.bfloat16),
        in_specs=[vmem] * 3,
        out_specs=vmem,
        scratch_shapes=[
            pltpu.VMEM((count - 1, rows, piece), jnp.bfloat16),
            pltpu.VMEM((rows, piece), jnp.bfloat16),
            pltpu.VMEM((count, rows, piece), jnp.bfloat16),
            dma((count - 1,)),
            dma((count - 1,)),
            dma((count - 1,)),
            dma((count - 1,)),
        ],
        compiler_params=pltpu.CompilerParams(has_side_effects=True),
    )(partial_value.astype(jnp.bfloat16), normed, scales[None, :])


def on_device(
    use_kernels,
    tokens,
    gain_first,
    gain_second,
    gate_first,
    up_first,
    down_first,
    gate_second,
    up_second,
    down_second,
):
    row_count = gate_first.shape[0]
    offset = lax.axis_index("fs") * row_count
    bring = collect if use_kernels else collect_plain
    work = half_block if use_kernels else half_block_plain
    finish = close if use_kernels else close_plain

    def fold_gain(weight, scales):
        picked = lax.dynamic_slice_in_dim(scales, offset, row_count, 0)
        return (picked[:, None] * weight).astype(jnp.bfloat16)

    first = bring(
        fold_gain(gate_first, gain_first),
        fold_gain(up_first, gain_first),
        down_first.astype(jnp.bfloat16),
    )
    second = bring(
        fold_gain(gate_second, gain_second),
        fold_gain(up_second, gain_second),
        down_second.astype(jnp.bfloat16),
    )
    normed_zero = plain_norm(tokens).astype(jnp.bfloat16)
    first, partial_value = work(normed_zero, *first)
    normed_one = finish(partial_value, normed_zero, gain_first)
    second, partial_value = work(normed_one, *second)
    result_rows = finish(partial_value, normed_one, gain_second)
    return (result_rows, *first, *second)


def solution(mesh):
    fs, tp = mesh.shape["fs"], mesh.shape["tp"]
    use_kernels = tp == 2 * CORES and fs == tp * SIDES
    placed = (P("tp", None), P(), P()) + (P("fs", "tp"),) * 6
    served = (P(None, "fs"), P(None, "fs"), P("fs", None))
    return jax.shard_map(
        functools.partial(on_device, use_kernels),
        mesh=mesh,
        in_specs=placed,
        out_specs=(P("tp", None),) + served + served,
        check_vma=False,
    )
```

```python
import functools

import jax
import jax.numpy as jnp
from jax import lax
from jax.experimental import pallas as pl
from jax.experimental.pallas import tpu as pltpu
from jax.sharding import PartitionSpec as P

MESH = pl.DeviceIdType.MESH
CORES = 2
SIDES = 2
CUTS = 4
RELAY = 6


def plain_norm(values):
    values = values.astype(jnp.float32)
    center = jnp.mean(values, axis=-1, keepdims=True)
    spread = jnp.mean(jnp.square(values - center), axis=-1, keepdims=True)
    return (values - center) * lax.rsqrt(spread + 1e-05)


def sum_over_hidden(partial_value):
    pieces = lax.all_to_all(
        partial_value.astype(jnp.bfloat16), "fs", split_axis=1, concat_axis=0, tiled=True
    )
    rows = partial_value.shape[0]
    pieces = pieces.reshape(-1, rows, pieces.shape[1]).astype(jnp.float32)
    summed = jnp.sum(pieces, axis=0).astype(jnp.bfloat16)
    return lax.all_gather(summed, "fs", axis=1, tiled=True).astype(jnp.float32)


def regroup(folded):
    spread = lax.all_to_all(folded, "tp", split_axis=0, concat_axis=1, tiled=True)
    parts = lax.axis_size("fs")
    rows = spread.shape[0]
    owned = lax.all_to_all(spread, "fs", split_axis=1, concat_axis=0, tiled=True)
    owned = owned.reshape(parts, rows, owned.shape[1])
    whole = lax.all_gather(owned, "tp", axis=1, tiled=True)
    return whole.reshape(-1, whole.shape[2])


def collect_plain(gate, up, down):
    return (
        regroup(gate),
        regroup(up),
        lax.all_gather(down, "tp", axis=1, tiled=True),
    )


def half_step_plain(normed, scales, w_gate, w_rising, w_down):
    gate_part = jnp.dot(normed, w_gate, preferred_element_type=jnp.float32)
    rising = jnp.dot(normed, w_rising, preferred_element_type=jnp.float32)
    hidden = (jax.nn.silu(gate_part) * rising).astype(jnp.bfloat16)
    partial_value = jnp.dot(hidden, w_down, preferred_element_type=jnp.float32)
    block = sum_over_hidden(partial_value)
    mixed = 1.6817928 * scales[None, :] * normed.astype(jnp.float32) + 0.5 * block
    return plain_norm(mixed).astype(jnp.bfloat16)


class Send:
    def __init__(self, when, src, dst, send, recv, to):
        self.when = when
        self.copy = pltpu.make_async_remote_copy(
            src_ref=src,
            dst_ref=dst,
            send_sem=send,
            recv_sem=recv,
            device_id=to,
            device_id_type=MESH,
        )

    def start(self):
        if self.when is None:
            self.copy.start()
        else:
            pl.when(self.when)(self.copy.start)

    def wait_send(self):
        if self.when is None:
            self.copy.wait_send()
        else:
            pl.when(self.when)(self.copy.wait_send)


def landed(ref, sem):
    pltpu.make_async_copy(ref, ref, sem).wait()


class Hand:
    def __init__(self, place, send, sources, wholes, down, whole_down, scratch, sems):
        self.__dict__.update(place)
        self.send = send
        self.sources, self.wholes = sources, wholes
        self.down, self.whole_down = down, whole_down
        self.passing, self.bounce, self.bounce_down = scratch
        (
            self.s_plane,
            self.s_cross,
            self.r_cross,
            self.s_pass,
            self.r_main,
            self.r_minor,
            self.s_main,
            self.s_minor,
            self.s_over,
            self.s_down,
            self.r_down,
            self.l_own,
            self.l_down,
        ) = sems
        self.rows = sources[0].shape[0]
        self.width = wholes[0].shape[1]
        self.part = self.rows // RELAY
        self.main = self.rows - self.part
        self.main_at = jnp.where(self.aligned, self.part, 0)
        self.over_at = jnp.where(self.aligned, self.main, 0)
        self.minor_at = jnp.where(self.aligned, 0, self.main)

    def here(self, col):
        return (self.fs, col)

    def cols(self, m, start, size, side):
        return self.sources[m].at[pl.ds(start, size), pl.ds(side * self.width, self.width)]

    def at(self, m, owner, start, size):
        first = pl.multiple_of(owner * self.rows + start, 16)
        return self.wholes[m].at[pl.ds(first, size), :]

    def column(self, col):
        lanes = self.down.shape[1]
        return self.whole_down.at[:, pl.ds(pl.multiple_of(col * lanes, 128), lanes)]

    def own(self, m):
        first = pl.multiple_of(self.y * self.width, 128)
        return self.sources[m].at[:, pl.ds(first, self.width)]

    def cross(self, m, side):
        for k in range(RELAY - 1):
            self.send(
                jnp.logical_not(self.aligned),
                self.cols(m, k * self.part, self.part, side),
                self.passing.at[m, side, k],
                self.s_cross.at[m, side, k],
                self.r_cross.at[m, side, k],
                self.here(self.peer),
            )

    def plane_far(self, m, side):
        self.send(
            jnp.logical_not(self.aligned),
            self.cols(m, self.part, self.main, side),
            self.at(m, self.fs, self.part, self.main),
            self.s_plane.at[m, side],
            self.r_main.at[m, self.fs],
            (self.tp * SIDES + side, self.tp),
        )

    def plane_near(self, m, side):
        owner = self.tp * SIDES + side
        self.send(
            jnp.logical_and(self.aligned, owner != self.fs),
            self.cols(m, 0, self.rows, side),
            self.at(m, self.fs, 0, self.rows),
            self.s_plane.at[m, side],
            self.r_main.at[m, self.fs],
            (owner, self.tp),
        )

    def send_down(self, when):
        for k, to in enumerate((self.peer, self.sibling)):
            self.send(
                when,
                self.down,
                self.column(self.tp),
                self.s_down.at[k],
                self.r_down.at[k],
                self.here(to),
            )

    def home_block(self):
        home = jnp.logical_and(self.aligned, self.primary)
        for m in range(2):
            for sem, to in ((self.s_over, self.peer), (self.s_main, self.sibling)):
                self.send(
                    home,
                    self.own(m),
                    self.at(m, self.fs, 0, self.rows),
                    sem.at[m, self.fs],
                    self.r_main.at[m, self.fs],
                    self.here(to),
                )

    def fetches(self):
        yield None, pltpu.make_async_copy(self.down, self.bounce_down, self.l_down)
        for m in range(2):
            yield jnp.logical_and(self.aligned, self.primary), pltpu.make_async_copy(
                self.own(m), self.bounce.at[m], self.l_own.at[m]
            )

    def puts(self):
        yield None, pltpu.make_async_copy(
            self.bounce_down, self.column(self.tp), self.l_down
        )
        for m in range(2):
            yield jnp.logical_and(self.aligned, self.primary), pltpu.make_async_copy(
                self.bounce.at[m], self.at(m, self.fs, 0, self.rows), self.l_own.at[m]
            )

    def keep(self):
        for when, copy in self.fetches():
            guarded(when, copy.start)
        for when, copy in self.fetches():
            guarded(when, copy.wait)
        for when, copy in self.puts():
            guarded(when, copy.start)

    def kept(self):
        for when, copy in self.puts():
            guarded(when, copy.wait)

    def relay(self, m, side):
        zone = (1 - self.x) * CORES + self.c
        for k in range(RELAY - 1):
            held = self.passing.at[m, side, k]
            guarded(self.aligned, landed, held, self.r_cross.at[m, side, k])
            self.send(
                self.aligned,
                held,
                self.at(m, self.fs, k * self.part, self.part),
                self.s_pass.at[m, side, k],
                self.r_main.at[m, self.fs],
                (zone * SIDES + side, self.tp),
            )

    def near(self, step):
        return self.half * 2 * SIDES + (self.fs + step) % (2 * SIDES)

    def far(self, step):
        return (1 - self.half) * 2 * SIDES + (self.fs + step) % (2 * SIDES)

    def whole_block(self, m, step):
        owner = self.near(step)
        block = self.at(m, owner, 0, self.rows)
        got = self.primary
        if step == 0:
            got = jnp.logical_and(got, jnp.logical_not(self.aligned))
        guarded(got, landed, block, self.r_main.at[m, owner])
        if step:
            self.send(
                jnp.logical_and(self.primary, self.aligned),
                block,
                block,
                self.s_over.at[m, owner],
                self.r_main.at[m, owner],
                self.here(self.peer),
            )
        self.send(
            got,
            block,
            block,
            self.s_main.at[m, owner],
            self.r_main.at[m, owner],
            self.here(self.sibling),
        )

    def pass_down(self):
        got = self.column(self.peer)
        landed(got, self.r_down.at[0])
        self.send(
            None, got, got, self.s_down.at[2], self.r_down.at[2], self.here(self.sibling)
        )

    def main_block(self, m, step):
        owner = self.far(step)
        block = self.at(m, owner, self.main_at, self.main)
        over = self.at(m, owner, self.over_at, self.part)
        guarded(self.primary, landed, block, self.r_main.at[m, owner])
        self.send(
            self.primary,
            over,
            over,
            self.s_over.at[m, owner],
            self.r_minor.at[m, owner],
            self.here(self.peer),
        )
        self.send(
            self.primary,
            block,
            block,
            self.s_main.at[m, owner],
            self.r_main.at[m, owner],
            self.here(self.sibling),
        )

    def minor_block(self, m, step):
        owner = self.far(step)
        block = self.at(m, owner, self.minor_at, self.part)
        guarded(self.primary, landed, block, self.r_minor.at[m, owner])
        self.send(
            self.primary,
            block,
            block,
            self.s_minor.at[m, owner],
            self.r_minor.at[m, owner],
            self.here(self.sibling),
        )

    def second(self):
        other = jnp.logical_not(self.primary)
        for m in range(2):
            for step in range(2 * SIDES):
                owner = self.near(step)
                block = self.at(m, owner, 0, self.rows)
                guarded(other, landed, block, self.r_main.at[m, owner])
                owner = self.far(step)
                block = self.at(m, owner, self.main_at, self.main)
                guarded(other, landed, block, self.r_main.at[m, owner])
                block = self.at(m, owner, self.minor_at, self.part)
                guarded(other, landed, block, self.r_minor.at[m, owner])
        landed(self.column(self.sibling), self.r_down.at[1])
        landed(self.column((1 - self.x) * CORES + 1 - self.c), self.r_down.at[2])


def guarded(when, act, *args):
    if when is None:
        act(*args)
    else:
        pl.when(when)(functools.partial(act, *args))


class Close:
    def __init__(self, place, send, partial_value, landing, summed, full, sems):
        self.__dict__.update(place)
        self.send = send
        self.partial_value, self.landing = partial_value, landing
        self.summed, self.full = summed, full
        self.s_part, self.r_part, self.s_sum, self.r_sum = sems
        self.count = full.shape[0]

    def lanes(self, index):
        width = self.summed.shape[1]
        return pl.ds(pl.multiple_of(index * width, 128), width)

    def scatter(self):
        for step in range(1, self.count):
            to = (self.fs + step) % self.count
            self.send(
                None,
                self.partial_value.at[:, self.lanes(to)],
                self.landing.at[step - 1],
                self.s_part.at[step - 1],
                self.r_part.at[step - 1],
                (to, self.tp),
            )

    def spread(self):
        for step in range(1, self.count):
            landed(self.landing.at[step - 1], self.r_part.at[step - 1])
        total = self.partial_value[:, self.lanes(self.fs)].astype(jnp.float32)
        for step in range(1, self.count):
            total += self.landing[step - 1].astype(jnp.float32)
        self.summed[...] = total.astype(jnp.bfloat16)
        for step in range(1, self.count):
            to = (self.fs + step) % self.count
            self.send(
                None,
                self.summed,
                self.full.at[self.fs],
                self.s_sum.at[step - 1],
                self.r_sum.at[step - 1],
                (to, self.tp),
            )
        self.full[self.fs] = self.summed[...]

    def norm(self, normed, scales, out):
        for step in range(1, self.count):
            came = (self.fs + self.count - step) % self.count
            landed(self.full.at[came], self.r_sum.at[step - 1])
        tall = 16

        def some_rows(index, carry):
            some = pl.ds(pl.multiple_of(index * tall, tall), tall)
            block = jnp.concatenate(
                [self.full[k, some, :].astype(jnp.float32) for k in range(self.count)],
                axis=1,
            )
            mixed = 1.6817928 * scales[...] * normed[some, :].astype(jnp.float32)
            out[some, :] = plain_norm(mixed + 0.5 * block).astype(jnp.bfloat16)
            return carry

        lax.fori_loop(0, out.shape[0] // tall, some_rows, 0)


def placing():
    fs = lax.axis_index("fs")
    tp = lax.axis_index("tp")
    z, x, c = fs // SIDES, tp // CORES, tp % CORES
    return dict(
        fs=fs,
        tp=tp,
        y=fs % SIDES,
        x=x,
        c=c,
        half=z // 2,
        aligned=x == z // 2,
        primary=c == z % 2,
        peer=(1 - x) * CORES + c,
        sibling=x * CORES + 1 - c,
    )


def sender():
    started = []

    def send(*args):
        one = Send(*args)
        one.start()
        started.append(one)

    return send, started


def multiply(normed, plan, sums, partial_value, arrive, leave):
    deep = plan[0][0].shape[0] // CUTS
    wide = plan[2][0].shape[1] // CUTS

    def cut(m, ref, k):
        if m < 2:
            return ref.at[pl.ds(k * deep, deep), :]
        return ref.at[:, pl.ds(k * wide, wide)]

    def coming(m, k):
        src, held, _ = plan[m]
        return pltpu.make_async_copy(cut(m, src, k), cut(m, held, k), arrive.at[m, k])

    def going(m, k):
        _, held, dst = plan[m]
        return pltpu.make_async_copy(cut(m, held, k), cut(m, dst, k), leave.at[m, k])

    def arrived(m, k):
        coming(m, k).wait()
        if plan[m][2] is not None:
            going(m, k).start()

    for k in range(CUTS):
        coming(0, k).start()
        coming(1, k).start()
    for k in range(CUTS):
        coming(2, k).start()
    for k in range(CUTS):
        n = normed[:, k * deep : (k + 1) * deep]
        for m, total in enumerate(sums):
            arrived(m, k)
            term = jnp.dot(
                n,
                plan[m][1][k * deep : (k + 1) * deep, :],
                preferred_element_type=jnp.float32,
            )
            if k:
                total[...] += term
            else:
                total[...] = term
    hidden = (jax.nn.silu(sums[0][...]) * sums[1][...]).astype(jnp.bfloat16)
    for k in range(CUTS):
        arrived(2, k)
        partial_value[:, k * wide : (k + 1) * wide] = jnp.dot(
            hidden,
            plan[2][1][:, k * wide : (k + 1) * wide],
            preferred_element_type=jnp.float32,
        ).astype(jnp.bfloat16)
    return [
        going(m, k) for m in range(3) if plan[m][2] is not None for k in range(CUTS)
    ]


def collect_kernel(*refs):
    (g1, u1, d1, g2, u2, d2, normed, scales), refs = refs[:8], refs[8:]
    (w1, v1, x1, w2, v2, x2, out), refs = refs[:7], refs[7:]
    (passing, bounce, bounce_down), refs = refs[:3], refs[3:]
    (hold_gate, hold_up, hold_down, gate_sum, up_sum), refs = refs[:5], refs[5:]
    (partial_value, landing, summed, full), refs = refs[:4], refs[4:]
    sems, refs = refs[:13], refs[13:]
    arrive, close_sems = refs[0], refs[1:]
    place = placing()
    aligned = place["aligned"]
    unaligned = jnp.logical_not(aligned)
    send, started = sender()
    one, two = (
        Hand(
            place,
            send,
            (gate, up),
            (whole_gate, whole_up),
            down,
            whole_down,
            (passing.at[h], bounce.at[h], bounce_down.at[h]),
            [sem.at[h] for sem in sems],
        )
        for h, (gate, up, down, whole_gate, whole_up, whole_down) in enumerate(
            ((g1, u1, d1, w1, v1, x1), (g2, u2, d2, w2, v2, x2))
        )
    )
    close = Close(place, send, partial_value, landing, summed, full, close_sems)
    turns = [(m, side) for m in range(2) for side in range(SIDES)]

    for m, side in turns:
        one.cross(m, side)
        one.plane_far(m, side)
        one.plane_near(m, side)
    one.send_down(None)
    one.home_block()
    two.cross(0, 0)
    two.plane_far(0, 0)
    two.cross(0, 1)
    one.keep()
    one.relay(0, 0)
    one.whole_block(0, 0)
    one.whole_block(0, 1)
    one.relay(0, 1)
    one.whole_block(0, 2)
    one.whole_block(0, 3)
    one.relay(1, 0)
    one.whole_block(1, 0)
    one.whole_block(1, 1)
    one.relay(1, 1)
    one.whole_block(1, 2)
    one.whole_block(1, 3)
    for m, side in turns:
        two.plane_near(m, side)
    two.send_down(aligned)
    two.home_block()
    one.pass_down()
    for step in range(2 * SIDES):
        one.main_block(0, step)
    two.plane_far(0, 1)
    for step in range(2 * SIDES):
        one.main_block(1, step)
    two.relay(0, 0)
    for m in range(2):
        for step in range(2 * SIDES):
            one.minor_block(m, step)
    one.second()
    one.kept()
    two.relay(0, 1)
    two.cross(1, 0)
    multiply(
        normed,
        ((w1, hold_gate, None), (v1, hold_up, None), (x1, hold_down, None)),
        (gate_sum, up_sum),
        partial_value,
        arrive,
        None,
    )
    close.scatter()
    two.plane_far(1, 0)
    two.cross(1, 1)
    two.send_down(unaligned)
    two.keep()
    two.whole_block(0, 0)
    two.whole_block(0, 1)
    two.whole_block(0, 2)
    close.spread()
    two.plane_far(1, 1)
    two.relay(1, 0)
    two.whole_block(0, 3)
    two.whole_block(1, 0)
    two.whole_block(1, 1)
    two.relay(1, 1)
    two.whole_block(1, 2)
    two.whole_block(1, 3)
    two.pass_down()
    close.norm(normed, scales, out)
    for m in range(2):
        for step in range(2 * SIDES):
            two.main_block(m, step)
    for m in range(2):
        for step in range(2 * SIDES):
            two.minor_block(m, step)
    two.second()
    two.kept()
    for copy in started:
        copy.wait_send()


def collect(first, second, normed, scales):
    gate, _, down = first
    rows, columns = gate.shape
    fs, tp = lax.axis_size("fs"), lax.axis_size("tp")
    width = columns * tp // fs
    part = rows // RELAY
    tall, wide = normed.shape
    piece = wide // fs
    whole = jax.ShapeDtypeStruct((rows * fs, width), jnp.bfloat16)
    whole_down = jax.ShapeDtypeStruct((down.shape[0], down.shape[1] * tp), jnp.bfloat16)
    any_place = pl.BlockSpec(memory_space=pl.ANY)
    vmem = pl.BlockSpec(memory_space=pltpu.VMEM)
    dma = pltpu.SemaphoreType.DMA
    held = lambda *shape: pltpu.VMEM(shape, jnp.bfloat16)
    relayed = dma((2, 2, SIDES, RELAY - 1))
    by_owner = dma((2, 2, fs))
    *weights, normed_one = pl.pallas_call(
        collect_kernel,
        out_shape=(whole, whole, whole_down) * 2
        + (jax.ShapeDtypeStruct(normed.shape, normed.dtype),),
        in_specs=[any_place] * 6 + [vmem] * 2,
        out_specs=(any_place,) * 6 + (vmem,),
        scratch_shapes=[
            held(2, 2, SIDES, RELAY - 1, part, width),
            held(2, 2, rows, width),
            held(2, *down.shape),
            held(*whole.shape),
            held(*whole.shape),
            held(*whole_down.shape),
            pltpu.VMEM((tall, width), jnp.float32),
            pltpu.VMEM((tall, width), jnp.float32),
            held(tall, wide),
            held(fs - 1, tall, piece),
            held(tall, piece),
            held(fs, tall, piece),
            dma((2, 2, SIDES)),
            relayed,
            relayed,
            relayed,
            by_owner,
            by_owner,
            by_owner,
            by_owner,
            by_owner,
            dma((2, 3)),
            dma((2, 3)),
            dma((2, 2)),
            dma((2,)),
            dma((3, CUTS)),
            dma((fs - 1,)),
            dma((fs - 1,)),
            dma((fs - 1,)),
            dma((fs - 1,)),
        ],
        compiler_params=pltpu.CompilerParams(
            has_side_effects=True, vmem_limit_bytes=60 * 2**20
        ),
    )(*first, *second, normed, scales[None, :])
    return weights[:3], weights[3:], normed_one


def serve_kernel(*refs):
    normed, refs = refs[0], refs[1:]
    first, second, refs = refs[:3], refs[3:6], refs[6:]
    out_first, out_second, refs = refs[:3], refs[3:6], refs[6:]
    partial_value, refs = refs[0], refs[1:]
    held_first, held_second, refs = refs[:3], refs[3:6], refs[6:]
    gate_sum, up_sum, arrive, leave, through, away = refs
    ins = [
        pltpu.make_async_copy(first[m], held_first[m], through.at[m]) for m in range(3)
    ]
    outs = [
        pltpu.make_async_copy(held_first[m], out_first[m], away.at[m]) for m in range(3)
    ]
    goings = multiply(
        normed,
        list(zip(second, held_second, out_second)),
        (gate_sum, up_sum),
        partial_value,
        arrive,
        leave,
    )
    for copy in ins:
        copy.start()
    for copy, next_copy in zip(ins, outs):
        copy.wait()
        next_copy.start()
    for copy in goings + outs:
        copy.wait()


def serve(normed, first, second):
    rows, width = normed.shape
    gate = first[0]
    vmem = pl.BlockSpec(memory_space=pltpu.VMEM)
    any_place = pl.BlockSpec(memory_space=pl.ANY)
    same = lambda a: jax.ShapeDtypeStruct(a.shape, a.dtype)
    dma = pltpu.SemaphoreType.DMA
    weights = (*first, *second)
    *served, partial_value = pl.pallas_call(
        serve_kernel,
        out_shape=tuple(same(a) for a in weights) + (same(normed),),
        in_specs=[vmem] + [any_place] * 6,
        out_specs=(any_place,) * 6 + (vmem,),
        scratch_shapes=[pltpu.VMEM(a.shape, a.dtype) for a in weights]
        + [
            pltpu.VMEM((rows, gate.shape[1]), jnp.float32),
            pltpu.VMEM((rows, gate.shape[1]), jnp.float32),
            dma((3, CUTS)),
            dma((3, CUTS)),
            dma((3,)),
            dma((3,)),
        ],
        compiler_params=pltpu.CompilerParams(vmem_limit_bytes=60 * 2**20),
        cost_estimate=pl.CostEstimate(
            flops=6 * rows * gate.size, bytes_accessed=24 * gate.size, transcendentals=0
        ),
    )(normed, *weights)
    return served[:3], served[3:], partial_value


def close_kernel(
    partial_value, normed, scales, out, landing, summed, full, *sems
):
    send, started = sender()
    close = Close(placing(), send, partial_value, landing, summed, full, sems)
    close.scatter()
    close.spread()
    close.norm(normed, scales, out)
    for copy in started:
        copy.wait_send()


def close(partial_value, normed, scales):
    rows, width = normed.shape
    count = lax.axis_size("fs")
    piece = width // count
    vmem = pl.BlockSpec(memory_space=pltpu.VMEM)
    dma = pltpu.SemaphoreType.DMA
    return pl.pallas_call(
        close_kernel,
        out_shape=jax.ShapeDtypeStruct((rows, width), jnp.bfloat16),
        in_specs=[vmem] * 3,
        out_specs=vmem,
        scratch_shapes=[
            pltpu.VMEM((count - 1, rows, piece), jnp.bfloat16),
            pltpu.VMEM((rows, piece), jnp.bfloat16),
            pltpu.VMEM((count, rows, piece), jnp.bfloat16),
            dma((count - 1,)),
            dma((count - 1,)),
            dma((count - 1,)),
            dma((count - 1,)),
        ],
        compiler_params=pltpu.CompilerParams(has_side_effects=True),
    )(partial_value, normed, scales[None, :])


def on_device(
    use_kernels,
    tokens,
    gain_first,
    gain_second,
    gate_first,
    up_first,
    down_first,
    gate_second,
    up_second,
    down_second,
):
    row_count = gate_first.shape[0]
    offset = lax.axis_index("fs") * row_count

    def fold_gain(weight, scales):
        picked = lax.dynamic_slice_in_dim(scales, offset, row_count, 0)
        return (picked[:, None] * weight).astype(jnp.bfloat16)

    first = (
        fold_gain(gate_first, gain_first),
        fold_gain(up_first, gain_first),
        down_first.astype(jnp.bfloat16),
    )
    second = (
        fold_gain(gate_second, gain_second),
        fold_gain(up_second, gain_second),
        down_second.astype(jnp.bfloat16),
    )
    normed_zero = plain_norm(tokens).astype(jnp.bfloat16)
    if use_kernels:
        first, second, normed_one = collect(first, second, normed_zero, gain_first)
        first, second, partial_value = serve(normed_one, first, second)
        result_rows = close(partial_value, normed_one, gain_second)
    else:
        first, second = collect_plain(*first), collect_plain(*second)
        normed_one = half_step_plain(normed_zero, gain_first, *first)
        result_rows = half_step_plain(normed_one, gain_second, *second)
    return (result_rows, *first, *second)


def solution(mesh):
    fs, tp = mesh.shape["fs"], mesh.shape["tp"]
    use_kernels = tp == 2 * CORES and fs == tp * SIDES
    placed = (P("tp", None), P(), P()) + (P("fs", "tp"),) * 6
    served = (P(None, "fs"), P(None, "fs"), P("fs", None))
    return jax.shard_map(
        functools.partial(on_device, use_kernels),
        mesh=mesh,
        in_specs=placed,
        out_specs=(P("tp", None),) + served + served,
        check_vma=False,
    )
```

```python
import functools

import jax
import jax.numpy as jnp
from jax import lax
from jax.experimental import pallas as pl
from jax.experimental.pallas import tpu as pltpu
from jax.sharding import PartitionSpec as P

MESH = pl.DeviceIdType.MESH
CORES = 2
SIDES = 2
CUTS = 4
RELAY = 6


def plain_norm(values):
    values = values.astype(jnp.float32)
    center = jnp.mean(values, axis=-1, keepdims=True)
    spread = jnp.mean(jnp.square(values - center), axis=-1, keepdims=True)
    return (values - center) * lax.rsqrt(spread + 1e-05)


def sum_over_hidden(partial_value):
    pieces = lax.all_to_all(
        partial_value.astype(jnp.bfloat16), "fs", split_axis=1, concat_axis=0, tiled=True
    )
    rows = partial_value.shape[0]
    pieces = pieces.reshape(-1, rows, pieces.shape[1]).astype(jnp.float32)
    summed = jnp.sum(pieces, axis=0).astype(jnp.bfloat16)
    return lax.all_gather(summed, "fs", axis=1, tiled=True).astype(jnp.float32)


def regroup(folded):
    spread = lax.all_to_all(folded, "tp", split_axis=0, concat_axis=1, tiled=True)
    parts = lax.axis_size("fs")
    rows = spread.shape[0]
    owned = lax.all_to_all(spread, "fs", split_axis=1, concat_axis=0, tiled=True)
    owned = owned.reshape(parts, rows, owned.shape[1])
    whole = lax.all_gather(owned, "tp", axis=1, tiled=True)
    return whole.reshape(-1, whole.shape[2])


def collect_plain(gate, up, down):
    return (
        regroup(gate),
        regroup(up),
        lax.all_gather(down, "tp", axis=1, tiled=True),
    )


def half_step_plain(normed, scales, w_gate, w_rising, w_down):
    gate_part = jnp.dot(normed, w_gate, preferred_element_type=jnp.float32)
    rising = jnp.dot(normed, w_rising, preferred_element_type=jnp.float32)
    hidden = (jax.nn.silu(gate_part) * rising).astype(jnp.bfloat16)
    partial_value = jnp.dot(hidden, w_down, preferred_element_type=jnp.float32)
    block = sum_over_hidden(partial_value)
    mixed = 1.6817928 * scales[None, :] * normed.astype(jnp.float32) + 0.5 * block
    return plain_norm(mixed).astype(jnp.bfloat16)


class Send:
    def __init__(self, when, src, dst, send, recv, to):
        self.when = when
        self.copy = pltpu.make_async_remote_copy(
            src_ref=src,
            dst_ref=dst,
            send_sem=send,
            recv_sem=recv,
            device_id=to,
            device_id_type=MESH,
        )

    def start(self):
        if self.when is None:
            self.copy.start()
        else:
            pl.when(self.when)(self.copy.start)

    def wait_send(self):
        if self.when is None:
            self.copy.wait_send()
        else:
            pl.when(self.when)(self.copy.wait_send)


def landed(ref, sem):
    pltpu.make_async_copy(ref, ref, sem).wait()


class Hand:
    def __init__(self, place, send, sources, wholes, down, whole_down, scratch, sems):
        self.__dict__.update(place)
        self.send = send
        self.sources, self.wholes = sources, wholes
        self.down, self.whole_down = down, whole_down
        self.passing, self.bounce, self.bounce_down = scratch
        (
            self.s_plane,
            self.s_cross,
            self.r_cross,
            self.s_pass,
            self.r_main,
            self.r_minor,
            self.s_main,
            self.s_minor,
            self.s_over,
            self.s_down,
            self.r_down,
            self.l_own,
            self.l_down,
        ) = sems
        self.rows = sources[0].shape[0]
        self.width = wholes[0].shape[1]
        self.part = self.rows // RELAY
        self.main = self.rows - self.part
        self.main_at = jnp.where(self.aligned, self.part, 0)
        self.over_at = jnp.where(self.aligned, self.main, 0)
        self.minor_at = jnp.where(self.aligned, 0, self.main)

    def here(self, col):
        return (self.fs, col)

    def cols(self, m, start, size, side):
        return self.sources[m].at[pl.ds(start, size), pl.ds(side * self.width, self.width)]

    def at(self, m, owner, start, size):
        first = pl.multiple_of(owner * self.rows + start, 16)
        return self.wholes[m].at[pl.ds(first, size), :]

    def column(self, col):
        lanes = self.down.shape[1]
        return self.whole_down.at[:, pl.ds(pl.multiple_of(col * lanes, 128), lanes)]

    def own(self, m):
        first = pl.multiple_of(self.y * self.width, 128)
        return self.sources[m].at[:, pl.ds(first, self.width)]

    def cross(self, m, side):
        for k in range(RELAY - 1):
            self.send(
                jnp.logical_not(self.aligned),
                self.cols(m, k * self.part, self.part, side),
                self.passing.at[m, side, k],
                self.s_cross.at[m, side, k],
                self.r_cross.at[m, side, k],
                self.here(self.peer),
            )

    def plane_far(self, m, side):
        self.send(
            jnp.logical_not(self.aligned),
            self.cols(m, self.part, self.main, side),
            self.at(m, self.fs, self.part, self.main),
            self.s_plane.at[m, side],
            self.r_main.at[m, self.fs],
            (self.tp * SIDES + side, self.tp),
        )

    def plane_near(self, m, side):
        owner = self.tp * SIDES + side
        self.send(
            jnp.logical_and(self.aligned, owner != self.fs),
            self.cols(m, 0, self.rows, side),
            self.at(m, self.fs, 0, self.rows),
            self.s_plane.at[m, side],
            self.r_main.at[m, self.fs],
            (owner, self.tp),
        )

    def send_down(self, when):
        for k, to in enumerate((self.peer, self.sibling)):
            self.send(
                when,
                self.down,
                self.column(self.tp),
                self.s_down.at[k],
                self.r_down.at[k],
                self.here(to),
            )

    def home_block(self):
        home = jnp.logical_and(self.aligned, self.primary)
        for m in range(2):
            for sem, to in ((self.s_over, self.peer), (self.s_main, self.sibling)):
                self.send(
                    home,
                    self.own(m),
                    self.at(m, self.fs, 0, self.rows),
                    sem.at[m, self.fs],
                    self.r_main.at[m, self.fs],
                    self.here(to),
                )

    def fetches(self):
        yield None, pltpu.make_async_copy(self.down, self.bounce_down, self.l_down)
        for m in range(2):
            yield jnp.logical_and(self.aligned, self.primary), pltpu.make_async_copy(
                self.own(m), self.bounce.at[m], self.l_own.at[m]
            )

    def puts(self):
        yield None, pltpu.make_async_copy(
            self.bounce_down, self.column(self.tp), self.l_down
        )
        for m in range(2):
            yield jnp.logical_and(self.aligned, self.primary), pltpu.make_async_copy(
                self.bounce.at[m], self.at(m, self.fs, 0, self.rows), self.l_own.at[m]
            )

    def keep(self):
        for when, copy in self.fetches():
            guarded(when, copy.start)
        for when, copy in self.fetches():
            guarded(when, copy.wait)
        for when, copy in self.puts():
            guarded(when, copy.start)

    def kept(self):
        for when, copy in self.puts():
            guarded(when, copy.wait)

    def relay(self, m, side):
        zone = (1 - self.x) * CORES + self.c
        for k in range(RELAY - 1):
            held = self.passing.at[m, side, k]
            guarded(self.aligned, landed, held, self.r_cross.at[m, side, k])
            self.send(
                self.aligned,
                held,
                self.at(m, self.fs, k * self.part, self.part),
                self.s_pass.at[m, side, k],
                self.r_main.at[m, self.fs],
                (zone * SIDES + side, self.tp),
            )

    def near(self, step):
        return self.half * 2 * SIDES + (self.fs + step) % (2 * SIDES)

    def far(self, step):
        return (1 - self.half) * 2 * SIDES + (self.fs + step) % (2 * SIDES)

    def whole_block(self, m, step):
        owner = self.near(step)
        block = self.at(m, owner, 0, self.rows)
        got = self.primary
        if step == 0:
            got = jnp.logical_and(got, jnp.logical_not(self.aligned))
        guarded(got, landed, block, self.r_main.at[m, owner])
        if step:
            self.send(
                jnp.logical_and(self.primary, self.aligned),
                block,
                block,
                self.s_over.at[m, owner],
                self.r_main.at[m, owner],
                self.here(self.peer),
            )
        self.send(
            got,
            block,
            block,
            self.s_main.at[m, owner],
            self.r_main.at[m, owner],
            self.here(self.sibling),
        )

    def pass_down(self):
        got = self.column(self.peer)
        landed(got, self.r_down.at[0])
        self.send(
            None, got, got, self.s_down.at[2], self.r_down.at[2], self.here(self.sibling)
        )

    def main_block(self, m, step):
        owner = self.far(step)
        block = self.at(m, owner, self.main_at, self.main)
        over = self.at(m, owner, self.over_at, self.part)
        guarded(self.primary, landed, block, self.r_main.at[m, owner])
        self.send(
            self.primary,
            over,
            over,
            self.s_over.at[m, owner],
            self.r_minor.at[m, owner],
            self.here(self.peer),
        )
        self.send(
            self.primary,
            block,
            block,
            self.s_main.at[m, owner],
            self.r_main.at[m, owner],
            self.here(self.sibling),
        )

    def minor_block(self, m, step):
        owner = self.far(step)
        block = self.at(m, owner, self.minor_at, self.part)
        guarded(self.primary, landed, block, self.r_minor.at[m, owner])
        self.send(
            self.primary,
            block,
            block,
            self.s_minor.at[m, owner],
            self.r_minor.at[m, owner],
            self.here(self.sibling),
        )

    def second(self):
        other = jnp.logical_not(self.primary)
        for m in range(2):
            for step in range(2 * SIDES):
                owner = self.near(step)
                block = self.at(m, owner, 0, self.rows)
                guarded(other, landed, block, self.r_main.at[m, owner])
                owner = self.far(step)
                block = self.at(m, owner, self.main_at, self.main)
                guarded(other, landed, block, self.r_main.at[m, owner])
                block = self.at(m, owner, self.minor_at, self.part)
                guarded(other, landed, block, self.r_minor.at[m, owner])
        landed(self.column(self.sibling), self.r_down.at[1])
        landed(self.column((1 - self.x) * CORES + 1 - self.c), self.r_down.at[2])


def guarded(when, act, *args):
    if when is None:
        act(*args)
    else:
        pl.when(when)(functools.partial(act, *args))


class Close:
    def __init__(self, place, send, partial_value, beside, halves, along, full, sems):
        self.__dict__.update(place)
        self.send = send
        self.partial_value, self.beside = partial_value, beside
        self.halves, self.along, self.full = halves, along, full
        (
            self.s_y,
            self.r_y,
            self.s_z,
            self.r_z,
            self.s_up,
            self.r_up,
            self.s_side,
            self.r_side,
        ) = sems
        self.zones = beside.shape[0]

    def piece(self, zone, side):
        width = self.full.shape[2]
        first = (zone * SIDES + side) * width
        return pl.ds(pl.multiple_of(first, 128), width)

    def zone(self, step):
        return (self.z + self.zones + step) % self.zones

    def held(self, zone, side):
        return self.full.at[zone * SIDES + side]

    def scatter(self):
        for step in (*range(1, self.zones), 0):
            self.send(
                None,
                self.partial_value.at[:, self.piece(self.zone(step), 1 - self.y)],
                self.beside.at[step],
                self.s_y.at[step],
                self.r_y.at[step],
                (self.z * SIDES + 1 - self.y, self.tp),
            )

    def both_sides(self, step):
        landed(self.beside.at[step], self.r_y.at[step])
        mine = self.partial_value[:, self.piece(self.zone(step), self.y)]
        return mine.astype(jnp.float32) + self.beside[step].astype(jnp.float32)

    def halve(self):
        for step in range(1, self.zones):
            self.halves[step - 1] = self.both_sides(step).astype(jnp.bfloat16)
            self.send(
                None,
                self.halves.at[step - 1],
                self.along.at[step - 1],
                self.s_z.at[step - 1],
                self.r_z.at[step - 1],
                (self.zone(step) * SIDES + self.y, self.tp),
            )

    def to_side(self, step, block):
        self.send(
            None,
            block,
            block,
            self.s_side.at[step],
            self.r_side.at[step],
            (self.z * SIDES + 1 - self.y, self.tp),
        )

    def spread(self):
        total = self.both_sides(0)
        for step in range(1, self.zones):
            landed(self.along.at[step - 1], self.r_z.at[step - 1])
            total += self.along[step - 1].astype(jnp.float32)
        self.full[self.fs] = total.astype(jnp.bfloat16)
        block = self.held(self.z, self.y)
        for step in range(1, self.zones):
            self.send(
                None,
                block,
                block,
                self.s_up.at[step - 1],
                self.r_up.at[step - 1],
                (self.zone(step) * SIDES + self.y, self.tp),
            )
        self.to_side(0, block)

    def side(self):
        for step in range(1, self.zones):
            block = self.held(self.zone(-step), self.y)
            landed(block, self.r_up.at[step - 1])
            self.to_side(step, block)

    def norm(self, normed, scales, out):
        for step in range(self.zones):
            landed(self.held(self.zone(-step), 1 - self.y), self.r_side.at[step])

        def mixed(some):
            block = jnp.concatenate(
                [
                    self.full[k, some, :].astype(jnp.float32)
                    for k in range(self.full.shape[0])
                ],
                axis=1,
            )
            old = 1.6817928 * scales[...] * normed[some, :].astype(jnp.float32)
            return old + 0.5 * block

        norm_rows(mixed, out)


def norm_rows(values, out):
    tall = 16

    def some_rows(index, carry):
        some = pl.ds(pl.multiple_of(index * tall, tall), tall)
        out[some, :] = plain_norm(values(some)).astype(jnp.bfloat16)
        return carry

    lax.fori_loop(0, out.shape[0] // tall, some_rows, 0)


def greet(partners):
    barrier = pltpu.get_barrier_semaphore()
    for partner in partners:
        pl.semaphore_signal(barrier, inc=1, device_id=partner, device_id_type=MESH)
    pl.semaphore_wait(barrier, len(partners))


def close_scratch(rows, width, count):
    held = lambda many: pltpu.VMEM((many, rows, width // count), jnp.bfloat16)
    zones = count // SIDES
    dma = pltpu.SemaphoreType.DMA
    sems = [dma((many,)) for many in (zones, zones - 1, zones - 1, zones)]
    return [held(zones), held(zones - 1), held(zones - 1), held(count)] + [
        sem for sem in sems for _ in range(2)
    ]


def placing():
    fs = lax.axis_index("fs")
    tp = lax.axis_index("tp")
    z, x, c = fs // SIDES, tp // CORES, tp % CORES
    return dict(
        fs=fs,
        tp=tp,
        z=z,
        y=fs % SIDES,
        x=x,
        c=c,
        half=z // 2,
        aligned=x == z // 2,
        primary=c == z % 2,
        peer=(1 - x) * CORES + c,
        sibling=x * CORES + 1 - c,
    )


def sender():
    started = []

    def send(*args):
        one = Send(*args)
        one.start()
        started.append(one)

    return send, started


def multiply(normed, plan, sums, partial_value, arrive, leave, others=()):
    deep = plan[0][0].shape[0] // CUTS
    wide = plan[2][0].shape[1] // CUTS

    def cut(m, ref, k):
        if m < 2:
            return ref.at[pl.ds(k * deep, deep), :]
        return ref.at[:, pl.ds(k * wide, wide)]

    def coming(m, k):
        src, held, _ = plan[m]
        return pltpu.make_async_copy(cut(m, src, k), cut(m, held, k), arrive.at[m, k])

    def going(m, k):
        _, held, dst = plan[m]
        return pltpu.make_async_copy(cut(m, held, k), cut(m, dst, k), leave.at[m, k])

    def arrived(m, k):
        coming(m, k).wait()
        if plan[m][2] is not None:
            going(m, k).start()

    for k in range(CUTS):
        coming(0, k).start()
        coming(1, k).start()
    for k in range(CUTS):
        coming(2, k).start()
    for copy in others:
        copy.start()
    for k in range(CUTS):
        n = normed[:, k * deep : (k + 1) * deep]
        for m, total in enumerate(sums):
            arrived(m, k)
            term = jnp.dot(
                n,
                plan[m][1][k * deep : (k + 1) * deep, :],
                preferred_element_type=jnp.float32,
            )
            if k:
                total[...] += term
            else:
                total[...] = term
    hidden = (jax.nn.silu(sums[0][...]) * sums[1][...]).astype(jnp.bfloat16)
    for k in range(CUTS):
        arrived(2, k)
        partial_value[:, k * wide : (k + 1) * wide] = jnp.dot(
            hidden,
            plan[2][1][:, k * wide : (k + 1) * wide],
            preferred_element_type=jnp.float32,
        ).astype(jnp.bfloat16)
    return [
        going(m, k) for m in range(3) if plan[m][2] is not None for k in range(CUTS)
    ]


def collect_kernel(*refs):
    (g1, u1, d1, g2, u2, d2, tokens, scales), refs = refs[:8], refs[8:]
    (w1, v1, x1, w2, v2, x2, out), refs = refs[:7], refs[7:]
    (passing, bounce, bounce_down), refs = refs[:3], refs[3:]
    (hold_gate, hold_up, hold_down, gate_sum, up_sum), refs = refs[:5], refs[5:]
    (normed, partial_value), refs = refs[:2], refs[2:]
    sems, refs = refs[:13], refs[13:]
    arrive, close_scratches = refs[0], refs[1:]
    place = placing()
    fs, tp = place["fs"], place["tp"]
    count = lax.axis_size("fs")
    greet(
        [((fs + step) % count, tp) for step in range(1, count)]
        + [(fs, place["peer"]), (fs, place["sibling"])]
    )
    aligned = place["aligned"]
    unaligned = jnp.logical_not(aligned)
    send, started = sender()
    one, two = (
        Hand(
            place,
            send,
            (gate, up),
            (whole_gate, whole_up),
            down,
            whole_down,
            (passing.at[h], bounce.at[h], bounce_down.at[h]),
            [sem.at[h] for sem in sems],
        )
        for h, (gate, up, down, whole_gate, whole_up, whole_down) in enumerate(
            ((g1, u1, d1, w1, v1, x1), (g2, u2, d2, w2, v2, x2))
        )
    )
    close = Close(place, send, partial_value, *close_scratches[:4], close_scratches[4:])
    turns = [(m, side) for m in range(2) for side in range(SIDES)]

    for m, side in turns:
        one.cross(m, side)
        one.plane_far(m, side)
        one.plane_near(m, side)
    one.send_down(None)
    one.home_block()
    two.cross(0, 0)
    two.plane_far(0, 0)
    two.cross(0, 1)
    one.keep()
    one.relay(0, 0)
    one.whole_block(0, 0)
    one.whole_block(0, 1)
    one.relay(0, 1)
    one.whole_block(0, 2)
    one.whole_block(0, 3)
    one.relay(1, 0)
    one.whole_block(1, 0)
    one.whole_block(1, 1)
    one.relay(1, 1)
    one.whole_block(1, 2)
    one.whole_block(1, 3)
    for m, side in turns:
        two.plane_near(m, side)
    two.send_down(aligned)
    two.home_block()
    norm_rows(lambda some: tokens[some, :], normed)
    one.pass_down()
    for step in range(2 * SIDES):
        one.main_block(0, step)
    two.plane_far(0, 1)
    for step in range(2 * SIDES):
        one.main_block(1, step)
    two.relay(0, 0)
    for m in range(2):
        for step in range(2 * SIDES):
            one.minor_block(m, step)
    one.second()
    one.kept()
    two.relay(0, 1)
    two.cross(1, 0)
    multiply(
        normed,
        ((w1, hold_gate, None), (v1, hold_up, None), (x1, hold_down, None)),
        (gate_sum, up_sum),
        partial_value,
        arrive,
        None,
    )
    close.scatter()
    two.cross(1, 1)
    two.send_down(unaligned)
    two.keep()
    two.whole_block(0, 0)
    close.halve()
    two.plane_far(1, 0)
    two.relay(1, 0)
    two.whole_block(0, 1)
    two.whole_block(0, 2)
    close.spread()
    two.plane_far(1, 1)
    two.relay(1, 1)
    two.whole_block(0, 3)
    two.whole_block(1, 0)
    two.whole_block(1, 1)
    two.whole_block(1, 2)
    two.whole_block(1, 3)
    close.side()
    two.pass_down()
    close.norm(normed, scales, out)
    for m in range(2):
        for step in range(2 * SIDES):
            two.main_block(m, step)
    for m in range(2):
        for step in range(2 * SIDES):
            two.minor_block(m, step)
    two.second()
    two.kept()
    for copy in started:
        copy.wait_send()


def collect(first, second, tokens, scales):
    gate, _, down = first
    rows, columns = gate.shape
    fs, tp = lax.axis_size("fs"), lax.axis_size("tp")
    width = columns * tp // fs
    part = rows // RELAY
    tall, wide = tokens.shape
    whole = jax.ShapeDtypeStruct((rows * fs, width), jnp.bfloat16)
    whole_down = jax.ShapeDtypeStruct((down.shape[0], down.shape[1] * tp), jnp.bfloat16)
    any_place = pl.BlockSpec(memory_space=pl.ANY)
    vmem = pl.BlockSpec(memory_space=pltpu.VMEM)
    dma = pltpu.SemaphoreType.DMA
    held = lambda *shape: pltpu.VMEM(shape, jnp.bfloat16)
    relayed = dma((2, 2, SIDES, RELAY - 1))
    by_owner = dma((2, 2, fs))
    *weights, normed_one = pl.pallas_call(
        collect_kernel,
        out_shape=(whole, whole, whole_down) * 2
        + (jax.ShapeDtypeStruct(tokens.shape, tokens.dtype),),
        in_specs=[any_place] * 6 + [vmem] * 2,
        out_specs=(any_place,) * 6 + (vmem,),
        scratch_shapes=[
            held(2, 2, SIDES, RELAY - 1, part, width),
            held(2, 2, rows, width),
            held(2, *down.shape),
            held(*whole.shape),
            held(*whole.shape),
            held(*whole_down.shape),
            pltpu.VMEM((tall, width), jnp.float32),
            pltpu.VMEM((tall, width), jnp.float32),
            held(tall, wide),
            held(tall, wide),
            dma((2, 2, SIDES)),
            relayed,
            relayed,
            relayed,
            by_owner,
            by_owner,
            by_owner,
            by_owner,
            by_owner,
            dma((2, 3)),
            dma((2, 3)),
            dma((2, 2)),
            dma((2,)),
            dma((3, CUTS)),
            *close_scratch(tall, wide, fs),
        ],
        compiler_params=pltpu.CompilerParams(
            has_side_effects=True, collective_id=0, vmem_limit_bytes=60 * 2**20
        ),
    )(*first, *second, tokens, scales[None, :])
    return weights[:3], weights[3:], normed_one


def serve_kernel(*refs):
    normed, refs = refs[0], refs[1:]
    first, second, refs = refs[:3], refs[3:6], refs[6:]
    out_first, out_second, refs = refs[:3], refs[3:6], refs[6:]
    partial_value, refs = refs[0], refs[1:]
    held_first, held_second, refs = refs[:3], refs[3:6], refs[6:]
    gate_sum, up_sum, arrive, leave, through, away = refs
    ins = [
        pltpu.make_async_copy(first[m], held_first[m], through.at[m]) for m in range(3)
    ]
    outs = [
        pltpu.make_async_copy(held_first[m], out_first[m], away.at[m]) for m in range(3)
    ]
    goings = multiply(
        normed,
        list(zip(second, held_second, out_second)),
        (gate_sum, up_sum),
        partial_value,
        arrive,
        leave,
        ins,
    )
    for copy, next_copy in zip(ins, outs):
        copy.wait()
        next_copy.start()
    for copy in goings + outs:
        copy.wait()


def serve(normed, first, second):
    rows, width = normed.shape
    gate = first[0]
    vmem = pl.BlockSpec(memory_space=pltpu.VMEM)
    any_place = pl.BlockSpec(memory_space=pl.ANY)
    same = lambda a: jax.ShapeDtypeStruct(a.shape, a.dtype)
    dma = pltpu.SemaphoreType.DMA
    weights = (*first, *second)
    *served, partial_value = pl.pallas_call(
        serve_kernel,
        out_shape=tuple(same(a) for a in weights) + (same(normed),),
        in_specs=[vmem] + [any_place] * 6,
        out_specs=(any_place,) * 6 + (vmem,),
        scratch_shapes=[pltpu.VMEM(a.shape, a.dtype) for a in weights]
        + [
            pltpu.VMEM((rows, gate.shape[1]), jnp.float32),
            pltpu.VMEM((rows, gate.shape[1]), jnp.float32),
            dma((3, CUTS)),
            dma((3, CUTS)),
            dma((3,)),
            dma((3,)),
        ],
        compiler_params=pltpu.CompilerParams(vmem_limit_bytes=60 * 2**20),
        cost_estimate=pl.CostEstimate(
            flops=6 * rows * gate.size, bytes_accessed=24 * gate.size, transcendentals=0
        ),
    )(normed, *weights)
    return served[:3], served[3:], partial_value


def close_kernel(partial_value, normed, scales, out, *scratches):
    place = placing()
    send, started = sender()
    close = Close(place, send, partial_value, *scratches[:4], scratches[4:])
    greet(
        [(close.zone(step) * SIDES + close.y, close.tp) for step in range(1, close.zones)]
        + [(close.z * SIDES + 1 - close.y, close.tp)]
    )
    close.scatter()
    close.halve()
    close.spread()
    close.side()
    close.norm(normed, scales, out)
    for copy in started:
        copy.wait_send()


def close(partial_value, normed, scales):
    rows, width = normed.shape
    vmem = pl.BlockSpec(memory_space=pltpu.VMEM)
    return pl.pallas_call(
        close_kernel,
        out_shape=jax.ShapeDtypeStruct((rows, width), jnp.bfloat16),
        in_specs=[vmem] * 3,
        out_specs=vmem,
        scratch_shapes=close_scratch(rows, width, lax.axis_size("fs")),
        compiler_params=pltpu.CompilerParams(has_side_effects=True, collective_id=1),
    )(partial_value, normed, scales[None, :])


def on_device(
    use_kernels,
    tokens,
    gain_first,
    gain_second,
    gate_first,
    up_first,
    down_first,
    gate_second,
    up_second,
    down_second,
):
    row_count = gate_first.shape[0]
    offset = lax.axis_index("fs") * row_count

    def fold_gain(weight, scales):
        picked = lax.dynamic_slice_in_dim(scales, offset, row_count, 0)
        return (picked[:, None] * weight).astype(jnp.bfloat16)

    first = (
        fold_gain(gate_first, gain_first),
        fold_gain(up_first, gain_first),
        down_first.astype(jnp.bfloat16),
    )
    second = (
        fold_gain(gate_second, gain_second),
        fold_gain(up_second, gain_second),
        down_second.astype(jnp.bfloat16),
    )
    if use_kernels:
        first, second, normed_one = collect(first, second, tokens, gain_first)
        first, second, partial_value = serve(normed_one, first, second)
        result_rows = close(partial_value, normed_one, gain_second)
    else:
        first, second = collect_plain(*first), collect_plain(*second)
        normed_zero = plain_norm(tokens).astype(jnp.bfloat16)
        normed_one = half_step_plain(normed_zero, gain_first, *first)
        result_rows = half_step_plain(normed_one, gain_second, *second)
    return (result_rows, *first, *second)


def solution(mesh):
    fs, tp = mesh.shape["fs"], mesh.shape["tp"]
    use_kernels = tp == 2 * CORES and fs == tp * SIDES
    placed = (P("tp", None), P(), P()) + (P("fs", "tp"),) * 6
    served = (P(None, "fs"), P(None, "fs"), P("fs", None))
    return jax.shard_map(
        functools.partial(on_device, use_kernels),
        mesh=mesh,
        in_specs=placed,
        out_specs=(P("tp", None),) + served + served,
        check_vma=False,
    )
```

```python
import functools

import jax
import jax.numpy as jnp
from jax import lax
from jax.experimental import pallas as pl
from jax.experimental.pallas import tpu as pltpu
from jax.sharding import PartitionSpec as P

MESH = pl.DeviceIdType.MESH
CORES = 2
SIDES = 2
COLLECT_VMEM = 20 * 2**20
SERVE_VMEM = 16 * 2**20
CUTS = 4
FAR = 5, 24
CHUNKS = 4


def plain_norm(values):
    values = values.astype(jnp.float32)
    center = jnp.mean(values, axis=-1, keepdims=True)
    spread = jnp.mean(jnp.square(values - center), axis=-1, keepdims=True)
    return (values - center) * lax.rsqrt(spread + 1e-05)


def sum_over_hidden(partial_value):
    pieces = lax.all_to_all(
        partial_value.astype(jnp.bfloat16), "fs", split_axis=1, concat_axis=0, tiled=True
    )
    rows = partial_value.shape[0]
    pieces = pieces.reshape(-1, rows, pieces.shape[1]).astype(jnp.float32)
    summed = jnp.sum(pieces, axis=0).astype(jnp.bfloat16)
    return lax.all_gather(summed, "fs", axis=1, tiled=True).astype(jnp.float32)


def regroup(folded):
    spread = lax.all_to_all(folded, "tp", split_axis=0, concat_axis=1, tiled=True)
    parts = lax.axis_size("fs")
    rows = spread.shape[0]
    owned = lax.all_to_all(spread, "fs", split_axis=1, concat_axis=0, tiled=True)
    owned = owned.reshape(parts, rows, owned.shape[1])
    whole = lax.all_gather(owned, "tp", axis=1, tiled=True)
    return whole.reshape(-1, whole.shape[2])


def collect_plain(gate, up, down):
    return (
        regroup(gate),
        regroup(up),
        lax.all_gather(down, "tp", axis=1, tiled=True),
    )


def half_step_plain(normed, scales, w_gate, w_rising, w_down):
    gate_part = jnp.dot(normed, w_gate, preferred_element_type=jnp.float32)
    rising = jnp.dot(normed, w_rising, preferred_element_type=jnp.float32)
    hidden = (jax.nn.silu(gate_part) * rising).astype(jnp.bfloat16)
    partial_value = jnp.dot(hidden, w_down, preferred_element_type=jnp.float32)
    block = sum_over_hidden(partial_value)
    mixed = 1.6817928 * scales[None, :] * normed.astype(jnp.float32) + 0.5 * block
    return plain_norm(mixed).astype(jnp.bfloat16)


class Send:
    def __init__(self, when, src, dst, send, recv, to):
        self.when = when
        self.copy = pltpu.make_async_remote_copy(
            src_ref=src,
            dst_ref=dst,
            send_sem=send,
            recv_sem=recv,
            device_id=to,
            device_id_type=MESH,
        )

    def start(self):
        if self.when is None:
            self.copy.start()
        else:
            pl.when(self.when)(self.copy.start)

    def wait_send(self):
        if self.when is None:
            self.copy.wait_send()
        else:
            pl.when(self.when)(self.copy.wait_send)


def landed(ref, sem):
    pltpu.make_async_copy(ref, ref, sem).wait()


def far_part(rows):
    return rows * FAR[0] // FAR[1] // 16 * 16


def chunks(rows):
    edges = [rows // 16 * k // CHUNKS * 16 for k in range(CHUNKS + 1)]
    return [(a, b - a) for a, b in zip(edges, edges[1:])]


class Hand:
    def __init__(self, place, send, sources, wholes, down, whole_down, scratch, sems):
        self.__dict__.update(place)
        self.send = send
        self.sources, self.wholes = sources, wholes
        self.down, self.whole_down = down, whole_down
        self.passing = scratch
        (
            self.s_plane,
            self.s_cross,
            self.r_cross,
            self.s_pass,
            self.r_main,
            self.r_minor,
            self.s_main,
            self.s_minor,
            self.s_over,
            self.s_down,
            self.r_down,
            self.l_own,
            self.l_down,
        ) = sems
        self.rows = sources[0].shape[0]
        self.width = wholes[0].shape[1]
        self.part = far_part(self.rows)
        self.main = self.rows - self.part
        self.main_at = jnp.where(self.aligned, self.part, 0)
        self.over_at = jnp.where(self.aligned, self.main, 0)
        self.minor_at = jnp.where(self.aligned, 0, self.main)

    def here(self, col):
        return (self.fs, col)

    def cols(self, m, start, size, side):
        return self.sources[m].at[pl.ds(start, size), pl.ds(side * self.width, self.width)]

    def at(self, m, owner, start, size):
        first = pl.multiple_of(owner * self.rows + start, 16)
        return self.wholes[m].at[pl.ds(first, size), :]

    def column(self, col):
        lanes = self.down.shape[1]
        return self.whole_down.at[:, pl.ds(pl.multiple_of(col * lanes, 128), lanes)]

    def own(self, m):
        first = pl.multiple_of(self.y * self.width, 128)
        return self.sources[m].at[:, pl.ds(first, self.width)]

    def cross(self, m, side):
        for k, (start, size) in enumerate(chunks(self.main)):
            self.send(
                jnp.logical_not(self.aligned),
                self.cols(m, start, size, side),
                self.passing.at[m, side, pl.ds(start, size)],
                self.s_cross.at[m, side, k],
                self.r_cross.at[m, side, k],
                self.here(self.peer),
            )

    def plane_far(self, m, side):
        self.send(
            jnp.logical_not(self.aligned),
            self.cols(m, self.part, self.main, side),
            self.at(m, self.fs, self.part, self.main),
            self.s_plane.at[m, side],
            self.r_main.at[m, self.fs],
            (self.tp * SIDES + side, self.tp),
        )

    def plane_near(self, m, side):
        owner = self.tp * SIDES + side
        self.send(
            jnp.logical_and(self.aligned, owner != self.fs),
            self.cols(m, 0, self.rows, side),
            self.at(m, self.fs, 0, self.rows),
            self.s_plane.at[m, side],
            self.r_main.at[m, self.fs],
            (owner, self.tp),
        )

    def send_down(self, when):
        for k, to in enumerate((self.peer, self.sibling)):
            self.send(
                when,
                self.down,
                self.column(self.tp),
                self.s_down.at[k],
                self.r_down.at[k],
                self.here(to),
            )

    def home_block(self):
        home = jnp.logical_and(self.aligned, self.primary)
        for m in range(2):
            for sem, to in ((self.s_over, self.peer), (self.s_main, self.sibling)):
                self.send(
                    home,
                    self.own(m),
                    self.at(m, self.fs, 0, self.rows),
                    sem.at[m, self.fs],
                    self.r_main.at[m, self.fs],
                    self.here(to),
                )

    def own_copies(self):
        yield None, pltpu.make_async_copy(self.down, self.column(self.tp), self.l_down)
        for m in range(2):
            yield jnp.logical_and(self.aligned, self.primary), pltpu.make_async_copy(
                self.own(m), self.at(m, self.fs, 0, self.rows), self.l_own.at[m]
            )

    def keep(self):
        for when, copy in self.own_copies():
            guarded(when, copy.start)

    def kept(self):
        for when, copy in self.own_copies():
            guarded(when, copy.wait)

    def relay(self, m, side):
        zone = (1 - self.x) * CORES + self.c
        for k, (start, size) in enumerate(chunks(self.main)):
            held = self.passing.at[m, side, pl.ds(start, size)]
            guarded(self.aligned, landed, held, self.r_cross.at[m, side, k])
            self.send(
                self.aligned,
                held,
                self.at(m, self.fs, start, size),
                self.s_pass.at[m, side, k],
                self.r_main.at[m, self.fs],
                (zone * SIDES + side, self.tp),
            )

    def near(self, step):
        return self.half * 2 * SIDES + (self.fs + step) % (2 * SIDES)

    def far(self, step):
        return (1 - self.half) * 2 * SIDES + (self.fs + step) % (2 * SIDES)

    def whole_block(self, m, step):
        owner = self.near(step)
        block = self.at(m, owner, 0, self.rows)
        got = self.primary
        if step == 0:
            got = jnp.logical_and(got, jnp.logical_not(self.aligned))
        guarded(got, landed, block, self.r_main.at[m, owner])
        if step:
            self.send(
                jnp.logical_and(self.primary, self.aligned),
                block,
                block,
                self.s_over.at[m, owner],
                self.r_main.at[m, owner],
                self.here(self.peer),
            )
        self.send(
            got,
            block,
            block,
            self.s_main.at[m, owner],
            self.r_main.at[m, owner],
            self.here(self.sibling),
        )

    def pass_down(self):
        got = self.column(self.peer)
        landed(got, self.r_down.at[0])
        self.send(
            None, got, got, self.s_down.at[2], self.r_down.at[2], self.here(self.sibling)
        )

    def main_block(self, m, step):
        owner = self.far(step)
        block = self.at(m, owner, self.main_at, self.main)
        over = self.at(m, owner, self.over_at, self.part)
        guarded(self.primary, landed, block, self.r_main.at[m, owner])
        self.send(
            self.primary,
            over,
            over,
            self.s_over.at[m, owner],
            self.r_minor.at[m, owner],
            self.here(self.peer),
        )
        self.send(
            self.primary,
            block,
            block,
            self.s_main.at[m, owner],
            self.r_main.at[m, owner],
            self.here(self.sibling),
        )

    def minor_block(self, m, step):
        owner = self.far(step)
        block = self.at(m, owner, self.minor_at, self.part)
        guarded(self.primary, landed, block, self.r_minor.at[m, owner])
        self.send(
            self.primary,
            block,
            block,
            self.s_minor.at[m, owner],
            self.r_minor.at[m, owner],
            self.here(self.sibling),
        )

    def second(self):
        other = jnp.logical_not(self.primary)
        for m in range(2):
            for step in range(2 * SIDES):
                owner = self.near(step)
                block = self.at(m, owner, 0, self.rows)
                guarded(other, landed, block, self.r_main.at[m, owner])
                owner = self.far(step)
                block = self.at(m, owner, self.main_at, self.main)
                guarded(other, landed, block, self.r_main.at[m, owner])
                block = self.at(m, owner, self.minor_at, self.part)
                guarded(other, landed, block, self.r_minor.at[m, owner])
        landed(self.column(self.sibling), self.r_down.at[1])
        landed(self.column((1 - self.x) * CORES + 1 - self.c), self.r_down.at[2])


def guarded(when, act, *args):
    if when is None:
        act(*args)
    else:
        pl.when(when)(functools.partial(act, *args))


class Close:
    def __init__(self, place, send, partial_value, beside, halves, along, full, sems):
        self.__dict__.update(place)
        self.send = send
        self.partial_value, self.beside = partial_value, beside
        self.halves, self.along, self.full = halves, along, full
        (
            self.s_y,
            self.r_y,
            self.s_z,
            self.r_z,
            self.s_up,
            self.r_up,
            self.s_side,
            self.r_side,
        ) = sems
        self.zones = beside.shape[0]

    def piece(self, zone, side):
        width = self.full.shape[2]
        first = (zone * SIDES + side) * width
        return pl.ds(pl.multiple_of(first, 128), width)

    def zone(self, step):
        return (self.z + self.zones + step) % self.zones

    def held(self, zone, side):
        return self.full.at[zone * SIDES + side]

    def scatter(self):
        for step in (*range(1, self.zones), 0):
            self.send(
                None,
                self.partial_value.at[:, self.piece(self.zone(step), 1 - self.y)],
                self.beside.at[step],
                self.s_y.at[step],
                self.r_y.at[step],
                (self.z * SIDES + 1 - self.y, self.tp),
            )

    def both_sides(self, step):
        landed(self.beside.at[step], self.r_y.at[step])
        mine = self.partial_value[:, self.piece(self.zone(step), self.y)]
        return mine.astype(jnp.float32) + self.beside[step].astype(jnp.float32)

    def halve(self):
        for step in range(1, self.zones):
            self.halves[step - 1] = self.both_sides(step).astype(jnp.bfloat16)
            self.send(
                None,
                self.halves.at[step - 1],
                self.along.at[step - 1],
                self.s_z.at[step - 1],
                self.r_z.at[step - 1],
                (self.zone(step) * SIDES + self.y, self.tp),
            )

    def to_side(self, step, block):
        self.send(
            None,
            block,
            block,
            self.s_side.at[step],
            self.r_side.at[step],
            (self.z * SIDES + 1 - self.y, self.tp),
        )

    def spread(self):
        total = self.both_sides(0)
        for step in range(1, self.zones):
            landed(self.along.at[step - 1], self.r_z.at[step - 1])
            total += self.along[step - 1].astype(jnp.float32)
        self.full[self.fs] = total.astype(jnp.bfloat16)
        block = self.held(self.z, self.y)
        for step in range(1, self.zones):
            self.send(
                None,
                block,
                block,
                self.s_up.at[step - 1],
                self.r_up.at[step - 1],
                (self.zone(step) * SIDES + self.y, self.tp),
            )
        self.to_side(0, block)

    def side(self):
        for step in range(1, self.zones):
            block = self.held(self.zone(-step), self.y)
            landed(block, self.r_up.at[step - 1])
            self.to_side(step, block)

    def norm(self, normed, scales, out):
        for step in range(self.zones):
            landed(self.held(self.zone(-step), 1 - self.y), self.r_side.at[step])

        def mixed(some):
            block = jnp.concatenate(
                [
                    self.full[k, some, :].astype(jnp.float32)
                    for k in range(self.full.shape[0])
                ],
                axis=1,
            )
            old = 1.6817928 * scales[...] * normed[some, :].astype(jnp.float32)
            return old + 0.5 * block

        norm_rows(mixed, out)


def norm_rows(values, out):
    tall = 16

    def some_rows(index, carry):
        some = pl.ds(pl.multiple_of(index * tall, tall), tall)
        out[some, :] = plain_norm(values(some)).astype(jnp.bfloat16)
        return carry

    lax.fori_loop(0, out.shape[0] // tall, some_rows, 0)


def greet(partners):
    barrier = pltpu.get_barrier_semaphore()
    for partner in partners:
        pl.semaphore_signal(barrier, inc=1, device_id=partner, device_id_type=MESH)
    pl.semaphore_wait(barrier, len(partners))


def close_scratch(rows, width, count):
    held = lambda many: pltpu.VMEM((many, rows, width // count), jnp.bfloat16)
    zones = count // SIDES
    dma = pltpu.SemaphoreType.DMA
    sems = [dma((many,)) for many in (zones, zones - 1, zones - 1, zones)]
    return [held(zones), held(zones - 1), held(zones - 1), held(count)] + [
        sem for sem in sems for _ in range(2)
    ]


def placing():
    fs = lax.axis_index("fs")
    tp = lax.axis_index("tp")
    z, x, c = fs // SIDES, tp // CORES, tp % CORES
    return dict(
        fs=fs,
        tp=tp,
        z=z,
        y=fs % SIDES,
        x=x,
        c=c,
        half=z // 2,
        aligned=x == z // 2,
        primary=c == z % 2,
        peer=(1 - x) * CORES + c,
        sibling=x * CORES + 1 - c,
    )


def sender():
    started = []

    def send(*args):
        one = Send(*args)
        one.start()
        started.append(one)

    return send, started


def multiply(normed, weights, sums, partial_value):
    gate, up, down = weights
    deep = gate.shape[0] // CUTS
    wide = down.shape[1] // CUTS
    for k in range(CUTS):
        n = normed[:, k * deep : (k + 1) * deep]
        for weight, total in zip((gate, up), sums):
            term = jnp.dot(
                n,
                weight[k * deep : (k + 1) * deep, :],
                preferred_element_type=jnp.float32,
            )
            if k:
                total[...] += term
            else:
                total[...] = term
    hidden = (jax.nn.silu(sums[0][...]) * sums[1][...]).astype(jnp.bfloat16)
    for k in range(CUTS):
        partial_value[:, k * wide : (k + 1) * wide] = jnp.dot(
            hidden,
            down[:, k * wide : (k + 1) * wide],
            preferred_element_type=jnp.float32,
        ).astype(jnp.bfloat16)


def collect_kernel(*refs):
    (g1, u1, d1, g2, u2, d2, tokens, scales), refs = refs[:8], refs[8:]
    (w1, v1, x1, w2, v2, x2, out), refs = refs[:7], refs[7:]
    passing, refs = refs[0], refs[1:]
    (gate_sum, up_sum), refs = refs[:2], refs[2:]
    (normed, partial_value), refs = refs[:2], refs[2:]
    sems, refs = refs[:13], refs[13:]
    close_scratches = refs
    place = placing()
    fs, tp = place["fs"], place["tp"]
    count = lax.axis_size("fs")
    greet(
        [((fs + step) % count, tp) for step in range(1, count)]
        + [(fs, place["peer"]), (fs, place["sibling"])]
    )
    aligned = place["aligned"]
    unaligned = jnp.logical_not(aligned)
    send, started = sender()
    one, two = (
        Hand(
            place,
            send,
            (gate, up),
            (whole_gate, whole_up),
            down,
            whole_down,
            passing.at[h],
            [sem.at[h] for sem in sems],
        )
        for h, (gate, up, down, whole_gate, whole_up, whole_down) in enumerate(
            ((g1, u1, d1, w1, v1, x1), (g2, u2, d2, w2, v2, x2))
        )
    )
    close = Close(place, send, partial_value, *close_scratches[:4], close_scratches[4:])
    turns = [(m, side) for m in range(2) for side in range(SIDES)]

    for m, side in turns:
        one.cross(m, side)
        one.plane_far(m, side)
        one.plane_near(m, side)
    one.send_down(None)
    one.home_block()
    two.cross(0, 0)
    two.plane_far(0, 0)
    one.keep()
    one.relay(0, 0)
    one.whole_block(0, 0)
    one.whole_block(0, 1)
    one.relay(0, 1)
    one.whole_block(0, 2)
    one.whole_block(0, 3)
    one.relay(1, 0)
    one.whole_block(1, 0)
    one.whole_block(1, 1)
    one.relay(1, 1)
    one.whole_block(1, 2)
    one.whole_block(1, 3)
    for m, side in turns:
        two.plane_near(m, side)
    norm_rows(lambda some: tokens[some, :], normed)
    one.pass_down()
    for step in range(2 * SIDES):
        one.main_block(0, step)
    two.home_block()
    two.cross(0, 1)
    two.plane_far(0, 1)
    for step in range(2 * SIDES):
        one.main_block(1, step)
    two.send_down(aligned)
    two.relay(0, 0)
    for step in range(2 * SIDES):
        one.minor_block(0, step)
    for step in range(2 * SIDES):
        one.minor_block(1, step)
    two.relay(0, 1)
    one.second()
    one.kept()
    two.cross(1, 0)
    multiply(
        normed,
        (w1, v1, x1),
        (gate_sum, up_sum),
        partial_value,
    )
    close.scatter()
    two.cross(1, 1)
    two.send_down(unaligned)
    two.keep()
    two.whole_block(0, 0)
    close.halve()
    two.plane_far(1, 0)
    two.relay(1, 0)
    two.whole_block(0, 1)
    two.whole_block(0, 2)
    close.spread()
    two.plane_far(1, 1)
    two.relay(1, 1)
    two.whole_block(0, 3)
    two.whole_block(1, 0)
    two.whole_block(1, 1)
    two.whole_block(1, 2)
    two.whole_block(1, 3)
    two.pass_down()
    for step in range(2 * SIDES):
        two.main_block(0, step)
    close.side()
    for step in range(2 * SIDES):
        two.main_block(1, step)
    close.norm(normed, scales, out)
    for step in range(2 * SIDES):
        two.minor_block(0, step)
    for step in range(2 * SIDES):
        two.minor_block(1, step)
    two.second()
    two.kept()
    for copy in started:
        copy.wait_send()


def collect(first, second, tokens, scales):
    gate, _, down = first
    rows, columns = gate.shape
    fs, tp = lax.axis_size("fs"), lax.axis_size("tp")
    width = columns * tp // fs
    main = rows - far_part(rows)
    tall, wide = tokens.shape
    whole = pltpu.VMEM((rows * fs, width), jnp.bfloat16)
    whole_down = pltpu.VMEM((down.shape[0], down.shape[1] * tp), jnp.bfloat16)
    any_place = pl.BlockSpec(memory_space=pl.ANY)
    vmem = pl.BlockSpec(memory_space=pltpu.VMEM)
    dma = pltpu.SemaphoreType.DMA
    held = lambda *shape: pltpu.VMEM(shape, jnp.bfloat16)
    relayed = dma((2, 2, SIDES, CHUNKS))
    by_owner = dma((2, 2, fs))
    *weights, normed_one = pl.pallas_call(
        collect_kernel,
        out_shape=(whole, whole, whole_down) * 2
        + (jax.ShapeDtypeStruct(tokens.shape, tokens.dtype),),
        in_specs=[any_place] * 6 + [vmem] * 2,
        out_specs=(vmem,) * 7,
        scratch_shapes=[
            held(2, 2, SIDES, main, width),
            pltpu.VMEM((tall, width), jnp.float32),
            pltpu.VMEM((tall, width), jnp.float32),
            held(tall, wide),
            held(tall, wide),
            dma((2, 2, SIDES)),
            relayed,
            relayed,
            relayed,
            by_owner,
            by_owner,
            by_owner,
            by_owner,
            by_owner,
            dma((2, 3)),
            dma((2, 3)),
            dma((2, 2)),
            dma((2,)),
            *close_scratch(tall, wide, fs),
        ],
        compiler_params=pltpu.CompilerParams(
            has_side_effects=True, collective_id=0, vmem_limit_bytes=COLLECT_VMEM
        ),
    )(*first, *second, tokens, scales[None, :])
    return weights[:3], weights[3:], normed_one


def serve_kernel(*refs):
    normed, refs = refs[0], refs[1:]
    weights, served, refs = refs[:6], refs[6:12], refs[12:]
    partial_value, gate_sum, up_sum, leave = refs
    copies = [
        pltpu.make_async_copy(weights[m], served[m], leave.at[m]) for m in range(6)
    ]
    for copy in copies:
        copy.start()
    multiply(normed, weights[3:], (gate_sum, up_sum), partial_value)
    for copy in copies:
        copy.wait()


def serve(normed, first, second):
    rows, width = normed.shape
    gate = first[0]
    vmem = pl.BlockSpec(memory_space=pltpu.VMEM)
    any_place = pl.BlockSpec(memory_space=pl.ANY)
    same = lambda a: jax.ShapeDtypeStruct(a.shape, a.dtype)
    weights = (*first, *second)
    sums = pltpu.VMEM((rows, gate.shape[1]), jnp.float32)
    *served, partial_value = pl.pallas_call(
        serve_kernel,
        out_shape=tuple(same(a) for a in weights) + (same(normed),),
        in_specs=[vmem] * 7,
        out_specs=(any_place,) * 6 + (vmem,),
        scratch_shapes=[sums, sums, pltpu.SemaphoreType.DMA((6,))],
        compiler_params=pltpu.CompilerParams(vmem_limit_bytes=SERVE_VMEM),
        cost_estimate=pl.CostEstimate(
            flops=6 * rows * gate.size, bytes_accessed=12 * gate.size, transcendentals=0
        ),
    )(normed, *(pltpu.with_memory_space_constraint(a, pltpu.VMEM) for a in weights))
    return served[:3], served[3:], partial_value


def close_kernel(partial_value, normed, scales, out, *scratches):
    place = placing()
    send, started = sender()
    close = Close(place, send, partial_value, *scratches[:4], scratches[4:])
    greet(
        [(close.zone(step) * SIDES + close.y, close.tp) for step in range(1, close.zones)]
        + [(close.z * SIDES + 1 - close.y, close.tp)]
    )
    close.scatter()
    close.halve()
    close.spread()
    close.side()
    close.norm(normed, scales, out)
    for copy in started:
        copy.wait_send()


def close(partial_value, normed, scales):
    rows, width = normed.shape
    vmem = pl.BlockSpec(memory_space=pltpu.VMEM)
    return pl.pallas_call(
        close_kernel,
        out_shape=jax.ShapeDtypeStruct((rows, width), jnp.bfloat16),
        in_specs=[vmem] * 3,
        out_specs=vmem,
        scratch_shapes=close_scratch(rows, width, lax.axis_size("fs")),
        compiler_params=pltpu.CompilerParams(has_side_effects=True, collective_id=1),
    )(partial_value, normed, scales[None, :])


def on_device(
    use_kernels,
    tokens,
    gain_first,
    gain_second,
    gate_first,
    up_first,
    down_first,
    gate_second,
    up_second,
    down_second,
):
    row_count = gate_first.shape[0]
    offset = lax.axis_index("fs") * row_count

    def fold_gain(weight, scales):
        picked = lax.dynamic_slice_in_dim(scales, offset, row_count, 0)
        return (picked[:, None] * weight).astype(jnp.bfloat16)

    first = (
        fold_gain(gate_first, gain_first),
        fold_gain(up_first, gain_first),
        down_first.astype(jnp.bfloat16),
    )
    second = (
        fold_gain(gate_second, gain_second),
        fold_gain(up_second, gain_second),
        down_second.astype(jnp.bfloat16),
    )
    if use_kernels:
        first, second, normed_one = collect(first, second, tokens, gain_first)
        first, second, partial_value = serve(normed_one, first, second)
        result_rows = close(partial_value, normed_one, gain_second)
    else:
        first, second = collect_plain(*first), collect_plain(*second)
        normed_zero = plain_norm(tokens).astype(jnp.bfloat16)
        normed_one = half_step_plain(normed_zero, gain_first, *first)
        result_rows = half_step_plain(normed_one, gain_second, *second)
    return (result_rows, *first, *second)


def solution(mesh):
    fs, tp = mesh.shape["fs"], mesh.shape["tp"]
    use_kernels = tp == 2 * CORES and fs == tp * SIDES
    placed = (P("tp", None), P(), P()) + (P("fs", "tp"),) * 6
    served = (P(None, "fs"), P(None, "fs"), P("fs", None))
    return jax.shard_map(
        functools.partial(on_device, use_kernels),
        mesh=mesh,
        in_specs=placed,
        out_specs=(P("tp", None),) + served + served,
        check_vma=False,
    )
```

```python
import functools

import jax
import jax.numpy as jnp
from jax import lax
from jax.experimental import pallas as pl
from jax.experimental.pallas import tpu as pltpu
from jax.sharding import PartitionSpec as P

MESH = pl.DeviceIdType.MESH
CORES = 2
SIDES = 2
COLLECT_VMEM = 21 * 2**20
SERVE_VMEM = 16 * 2**20
CUTS = 4
FAR = 5, 24
CHUNKS = 4


def plain_norm(values):
    values = values.astype(jnp.float32)
    center = jnp.mean(values, axis=-1, keepdims=True)
    spread = jnp.mean(jnp.square(values - center), axis=-1, keepdims=True)
    return (values - center) * lax.rsqrt(spread + 1e-05)


def sum_over_hidden(partial_value):
    pieces = lax.all_to_all(
        partial_value.astype(jnp.bfloat16), "fs", split_axis=1, concat_axis=0, tiled=True
    )
    rows = partial_value.shape[0]
    pieces = pieces.reshape(-1, rows, pieces.shape[1]).astype(jnp.float32)
    summed = jnp.sum(pieces, axis=0).astype(jnp.bfloat16)
    return lax.all_gather(summed, "fs", axis=1, tiled=True).astype(jnp.float32)


def regroup(folded):
    spread = lax.all_to_all(folded, "tp", split_axis=0, concat_axis=1, tiled=True)
    parts = lax.axis_size("fs")
    rows = spread.shape[0]
    owned = lax.all_to_all(spread, "fs", split_axis=1, concat_axis=0, tiled=True)
    owned = owned.reshape(parts, rows, owned.shape[1])
    whole = lax.all_gather(owned, "tp", axis=1, tiled=True)
    return whole.reshape(-1, whole.shape[2])


def collect_plain(gate, up, down):
    return (
        regroup(gate),
        regroup(up),
        lax.all_gather(down, "tp", axis=1, tiled=True),
    )


def half_step_plain(normed, scales, w_gate, w_rising, w_down):
    gate_part = jnp.dot(normed, w_gate, preferred_element_type=jnp.float32)
    rising = jnp.dot(normed, w_rising, preferred_element_type=jnp.float32)
    hidden = (jax.nn.silu(gate_part) * rising).astype(jnp.bfloat16)
    partial_value = jnp.dot(hidden, w_down, preferred_element_type=jnp.float32)
    block = sum_over_hidden(partial_value)
    mixed = 1.6817928 * scales[None, :] * normed.astype(jnp.float32) + 0.5 * block
    return plain_norm(mixed).astype(jnp.bfloat16)


class Send:
    def __init__(self, when, src, dst, send, recv, to):
        self.when = when
        self.copy = pltpu.make_async_remote_copy(
            src_ref=src,
            dst_ref=dst,
            send_sem=send,
            recv_sem=recv,
            device_id=to,
            device_id_type=MESH,
        )

    def start(self):
        if self.when is None:
            self.copy.start()
        else:
            pl.when(self.when)(self.copy.start)

    def wait_send(self):
        if self.when is None:
            self.copy.wait_send()
        else:
            pl.when(self.when)(self.copy.wait_send)


def landed(ref, sem):
    pltpu.make_async_copy(ref, ref, sem).wait()


def far_part(rows):
    return rows * FAR[0] // FAR[1] // 16 * 16


def chunks(rows):
    edges = [rows // 16 * k // CHUNKS * 16 for k in range(CHUNKS + 1)]
    return [(a, b - a) for a, b in zip(edges, edges[1:])]


class Hand:
    def __init__(self, place, send, sources, wholes, down, whole_down, scratch, sems):
        self.__dict__.update(place)
        self.send = send
        self.sources, self.wholes = sources, wholes
        self.down, self.whole_down = down, whole_down
        self.passing = scratch
        (
            self.s_plane,
            self.s_cross,
            self.r_cross,
            self.s_pass,
            self.r_main,
            self.r_minor,
            self.s_main,
            self.s_minor,
            self.s_over,
            self.s_down,
            self.r_down,
            self.l_own,
        ) = sems
        self.rows = sources[0].shape[0]
        self.width = wholes[0].shape[1]
        self.part = far_part(self.rows)
        self.main = self.rows - self.part
        self.main_at = jnp.where(self.aligned, self.part, 0)
        self.over_at = jnp.where(self.aligned, self.main, 0)
        self.minor_at = jnp.where(self.aligned, 0, self.main)

    def here(self, col):
        return (self.fs, col)

    def cols(self, m, start, size, side):
        return self.sources[m].at[pl.ds(start, size), pl.ds(side * self.width, self.width)]

    def at(self, m, owner, start, size):
        first = pl.multiple_of(owner * self.rows + start, 16)
        return self.wholes[m].at[pl.ds(first, size), :]

    def column(self, col):
        lanes = self.down.shape[1]
        return self.whole_down.at[:, pl.ds(pl.multiple_of(col * lanes, 128), lanes)]

    def own(self, m):
        first = pl.multiple_of(self.y * self.width, 128)
        return self.sources[m].at[:, pl.ds(first, self.width)]

    def cross(self, m, side):
        for k, (start, size) in enumerate(chunks(self.main)):
            self.send(
                jnp.logical_not(self.aligned),
                self.cols(m, start, size, side),
                self.passing.at[m, side, pl.ds(start, size)],
                self.s_cross.at[m, side, k],
                self.r_cross.at[m, side, k],
                self.here(self.peer),
            )

    def plane_far(self, m, side):
        self.send(
            jnp.logical_not(self.aligned),
            self.cols(m, self.part, self.main, side),
            self.at(m, self.fs, self.part, self.main),
            self.s_plane.at[m, side],
            self.r_main.at[m, self.fs],
            (self.tp * SIDES + side, self.tp),
        )

    def plane_near(self, m, side):
        owner = self.tp * SIDES + side
        self.send(
            jnp.logical_and(self.aligned, owner != self.fs),
            self.cols(m, 0, self.rows, side),
            self.at(m, self.fs, 0, self.rows),
            self.s_plane.at[m, side],
            self.r_main.at[m, self.fs],
            (owner, self.tp),
        )

    def send_down(self, when):
        for k, to in enumerate((self.peer, self.sibling)):
            self.send(
                when,
                self.down,
                self.column(self.tp),
                self.s_down.at[k],
                self.r_down.at[k],
                self.here(to),
            )

    def home_block(self):
        home = jnp.logical_and(self.aligned, self.primary)
        for m in range(2):
            for sem, to in ((self.s_over, self.peer), (self.s_main, self.sibling)):
                self.send(
                    home,
                    self.own(m),
                    self.at(m, self.fs, 0, self.rows),
                    sem.at[m, self.fs],
                    self.r_main.at[m, self.fs],
                    self.here(to),
                )

    def fold_down(self, trained, stage, sem):
        lanes = self.down.shape[1]
        mine = pl.ds(pl.multiple_of(self.tp * lanes, 128), lanes)

        def put(rows, tile):
            self.down[rows, :] = tile.astype(jnp.bfloat16)
            self.whole_down[rows, mine] = tile.astype(jnp.bfloat16)

        by_tiles(trained, stage, sem, put)

    def fold_wide(self, m, trained, scales, stage, sem):
        def put(rows, tile):
            self.sources[m][rows, :] = (scales[rows, :] * tile).astype(jnp.bfloat16)

        by_tiles(trained, stage, sem, put)

    def keep_folded(self):
        mine = pl.ds(pl.multiple_of(self.y * self.width, 128), self.width)

        def tile(index, carry):
            rows = pl.ds(pl.multiple_of(index * 16, 16), 16)
            first = pl.multiple_of(self.fs * self.rows + index * 16, 16)
            for m in range(2):
                self.wholes[m][pl.ds(first, 16), :] = self.sources[m][rows, mine]
            return carry

        def block():
            lax.fori_loop(0, self.rows // 16, tile, 0)

        guarded(jnp.logical_and(self.aligned, self.primary), block)

    def own_copies(self):
        for m in range(2):
            yield jnp.logical_and(self.aligned, self.primary), pltpu.make_async_copy(
                self.own(m), self.at(m, self.fs, 0, self.rows), self.l_own.at[m]
            )

    def keep(self):
        for when, copy in self.own_copies():
            guarded(when, copy.start)

    def kept(self):
        for when, copy in self.own_copies():
            guarded(when, copy.wait)

    def relay(self, m, side):
        zone = (1 - self.x) * CORES + self.c
        for k, (start, size) in enumerate(chunks(self.main)):
            held = self.passing.at[m, side, pl.ds(start, size)]
            guarded(self.aligned, landed, held, self.r_cross.at[m, side, k])
            self.send(
                self.aligned,
                held,
                self.at(m, self.fs, start, size),
                self.s_pass.at[m, side, k],
                self.r_main.at[m, self.fs],
                (zone * SIDES + side, self.tp),
            )

    def near(self, step):
        return self.half * 2 * SIDES + (self.fs + step) % (2 * SIDES)

    def far(self, step):
        return (1 - self.half) * 2 * SIDES + (self.fs + step) % (2 * SIDES)

    def whole_block(self, m, step):
        owner = self.near(step)
        block = self.at(m, owner, 0, self.rows)
        got = self.primary
        if step == 0:
            got = jnp.logical_and(got, jnp.logical_not(self.aligned))
        guarded(got, landed, block, self.r_main.at[m, owner])
        if step:
            self.send(
                jnp.logical_and(self.primary, self.aligned),
                block,
                block,
                self.s_over.at[m, owner],
                self.r_main.at[m, owner],
                self.here(self.peer),
            )
        self.send(
            got,
            block,
            block,
            self.s_main.at[m, owner],
            self.r_main.at[m, owner],
            self.here(self.sibling),
        )

    def pass_down(self):
        got = self.column(self.peer)
        landed(got, self.r_down.at[0])
        self.send(
            None, got, got, self.s_down.at[2], self.r_down.at[2], self.here(self.sibling)
        )

    def main_block(self, m, step):
        owner = self.far(step)
        block = self.at(m, owner, self.main_at, self.main)
        over = self.at(m, owner, self.over_at, self.part)
        guarded(self.primary, landed, block, self.r_main.at[m, owner])
        self.send(
            self.primary,
            over,
            over,
            self.s_over.at[m, owner],
            self.r_minor.at[m, owner],
            self.here(self.peer),
        )
        self.send(
            self.primary,
            block,
            block,
            self.s_main.at[m, owner],
            self.r_main.at[m, owner],
            self.here(self.sibling),
        )

    def minor_block(self, m, step):
        owner = self.far(step)
        block = self.at(m, owner, self.minor_at, self.part)
        guarded(self.primary, landed, block, self.r_minor.at[m, owner])
        self.send(
            self.primary,
            block,
            block,
            self.s_minor.at[m, owner],
            self.r_minor.at[m, owner],
            self.here(self.sibling),
        )

    def second(self):
        other = jnp.logical_not(self.primary)
        for m in range(2):
            for step in range(2 * SIDES):
                owner = self.near(step)
                block = self.at(m, owner, 0, self.rows)
                guarded(other, landed, block, self.r_main.at[m, owner])
                owner = self.far(step)
                block = self.at(m, owner, self.main_at, self.main)
                guarded(other, landed, block, self.r_main.at[m, owner])
                block = self.at(m, owner, self.minor_at, self.part)
                guarded(other, landed, block, self.r_minor.at[m, owner])
        landed(self.column(self.sibling), self.r_down.at[1])
        landed(self.column((1 - self.x) * CORES + 1 - self.c), self.r_down.at[2])


def guarded(when, act, *args):
    if when is None:
        act(*args)
    else:
        pl.when(when)(functools.partial(act, *args))


def beside_zone(zone):
    return zone + 1 - 2 * (zone % 2)


class Close:
    def __init__(self, place, send, partial_value, beside, halves, along, full, sems):
        self.__dict__.update(place)
        self.send = send
        self.partial_value, self.beside = partial_value, beside
        self.halves, self.along, self.full = halves, along, full
        (
            self.s_y,
            self.r_y,
            self.s_z,
            self.r_z,
            self.s_up,
            self.r_up,
            self.s_side,
            self.r_side,
        ) = sems
        self.zones = beside.shape[0]
        self.near = beside_zone(self.z)
        self.over = (self.z + 2) % self.zones
        self.last = beside_zone(self.over)

    def piece(self, zone, side):
        width = self.full.shape[2]
        first = (zone * SIDES + side) * width
        return pl.ds(pl.multiple_of(first, 128), width)

    def zone(self, step):
        return (self.z + self.zones + step) % self.zones

    def held(self, zone, side):
        return self.full.at[zone * SIDES + side]

    def scatter(self):
        for step in (*range(1, self.zones), 0):
            self.send(
                None,
                self.partial_value.at[:, self.piece(self.zone(step), 1 - self.y)],
                self.beside.at[step],
                self.s_y.at[step],
                self.r_y.at[step],
                (self.z * SIDES + 1 - self.y, self.tp),
            )

    def both_sides(self, step):
        landed(self.beside.at[step], self.r_y.at[step])
        mine = self.partial_value[:, self.piece(self.zone(step), self.y)]
        return mine.astype(jnp.float32) + self.beside[step].astype(jnp.float32)

    def halve(self):
        for step in range(1, self.zones):
            self.halves[step - 1] = self.both_sides(step).astype(jnp.bfloat16)
            self.send(
                None,
                self.halves.at[step - 1],
                self.along.at[step - 1],
                self.s_z.at[step - 1],
                self.r_z.at[step - 1],
                (self.zone(step) * SIDES + self.y, self.tp),
            )

    def to_side(self, step, block):
        self.send(
            None,
            block,
            block,
            self.s_side.at[step],
            self.r_side.at[step],
            (self.z * SIDES + 1 - self.y, self.tp),
        )

    def to_zone(self, kind, block, zone):
        self.send(
            None,
            block,
            block,
            self.s_up.at[kind],
            self.r_up.at[kind],
            (zone * SIDES + self.y, self.tp),
        )

    def spread(self):
        total = self.both_sides(0)
        for step in range(1, self.zones):
            landed(self.along.at[step - 1], self.r_z.at[step - 1])
            total += self.along[step - 1].astype(jnp.float32)
        self.full[self.fs] = total.astype(jnp.bfloat16)
        block = self.held(self.z, self.y)
        self.to_zone(0, block, self.over)
        self.to_zone(1, block, self.near)
        self.to_side(0, block)

    def pass_on(self):
        block = self.held(self.over, self.y)
        landed(block, self.r_up.at[0])
        self.to_zone(2, block, self.near)
        self.to_side(1, block)

    def side(self):
        for kind, zone in ((1, self.near), (2, self.last)):
            block = self.held(zone, self.y)
            landed(block, self.r_up.at[kind])
            self.to_side(kind + 1, block)

    def norm(self, normed, scales, out):
        for step, zone in enumerate((self.z, self.over, self.near, self.last)):
            landed(self.held(zone, 1 - self.y), self.r_side.at[step])

        def mixed(some):
            block = jnp.concatenate(
                [
                    self.full[k, some, :].astype(jnp.float32)
                    for k in range(self.full.shape[0])
                ],
                axis=1,
            )
            old = 1.6817928 * scales[...] * normed[some, :].astype(jnp.float32)
            return old + 0.5 * block

        norm_rows(mixed, out)


def norm_rows(values, out):
    tall = 16

    def some_rows(index, carry):
        some = pl.ds(pl.multiple_of(index * tall, tall), tall)
        out[some, :] = plain_norm(values(some)).astype(jnp.bfloat16)
        return carry

    lax.fori_loop(0, out.shape[0] // tall, some_rows, 0)


def greet(partners, meanwhile=None):
    barrier = pltpu.get_barrier_semaphore()
    for partner in partners:
        pl.semaphore_signal(barrier, inc=1, device_id=partner, device_id_type=MESH)
    if meanwhile is not None:
        meanwhile()
    pl.semaphore_wait(barrier, len(partners))


def by_tiles(src, stage, sem, put):
    tall = stage.shape[1]
    count = src.shape[0] // tall

    def fetch(k):
        return pltpu.make_async_copy(
            src.at[pl.ds(k * tall, tall), :], stage.at[k % 2], sem.at[k % 2]
        )

    fetch(0).start()
    for k in range(count):
        if k + 1 < count:
            fetch(k + 1).start()
        fetch(k).wait()

        def tile(index, carry, k=k):
            first = pl.multiple_of(index * 16, 16)
            rows = pl.ds(pl.multiple_of(k * tall + index * 16, 16), 16)
            put(rows, stage[k % 2, pl.ds(first, 16), :])
            return carry

        lax.fori_loop(0, tall // 16, tile, 0)


def close_scratch(rows, width, count):
    held = lambda many: pltpu.VMEM((many, rows, width // count), jnp.bfloat16)
    zones = count // SIDES
    dma = pltpu.SemaphoreType.DMA
    sems = [dma((many,)) for many in (zones, zones - 1, zones - 1, zones)]
    return [held(zones), held(zones - 1), held(zones - 1), held(count)] + [
        sem for sem in sems for _ in range(2)
    ]


def placing():
    fs = lax.axis_index("fs")
    tp = lax.axis_index("tp")
    z, x, c = fs // SIDES, tp // CORES, tp % CORES
    return dict(
        fs=fs,
        tp=tp,
        z=z,
        y=fs % SIDES,
        x=x,
        c=c,
        half=z // 2,
        aligned=x == z // 2,
        primary=c == z % 2,
        peer=(1 - x) * CORES + c,
        sibling=x * CORES + 1 - c,
    )


def sender():
    started = []

    def send(*args):
        one = Send(*args)
        one.start()
        started.append(one)

    return send, started


def multiply(normed, weights, sums, partial_value):
    gate, up, down = weights
    deep = gate.shape[0] // CUTS
    wide = down.shape[1] // CUTS
    for k in range(CUTS):
        n = normed[:, k * deep : (k + 1) * deep]
        for weight, total in zip((gate, up), sums):
            term = jnp.dot(
                n,
                weight[k * deep : (k + 1) * deep, :],
                preferred_element_type=jnp.float32,
            )
            if k:
                total[...] += term
            else:
                total[...] = term
    hidden = (jax.nn.silu(sums[0][...]) * sums[1][...]).astype(jnp.bfloat16)
    for k in range(CUTS):
        partial_value[:, k * wide : (k + 1) * wide] = jnp.dot(
            hidden,
            down[:, k * wide : (k + 1) * wide],
            preferred_element_type=jnp.float32,
        ).astype(jnp.bfloat16)


def collect_kernel(*refs):
    (g1, u1, t1, tg2, tu2, t2, tokens, scales, picked), refs = refs[:9], refs[9:]
    (w1, v1, x1, w2, v2, x2, out), refs = refs[:7], refs[7:]
    (passing, folded, d1, d2), refs = refs[:4], refs[4:]
    (stage_wide, stage_down, stage_sem), refs = refs[:3], refs[3:]
    (gate_sum, up_sum), refs = refs[:2], refs[2:]
    (normed, partial_value), refs = refs[:2], refs[2:]
    sems, refs = refs[:12], refs[12:]
    close_scratches = refs
    place = placing()
    fs, tp = place["fs"], place["tp"]
    count = lax.axis_size("fs")
    aligned = place["aligned"]
    unaligned = jnp.logical_not(aligned)
    send, started = sender()
    one, two = (
        Hand(
            place,
            send,
            (gate, up),
            (whole_gate, whole_up),
            down,
            whole_down,
            passing.at[h],
            [sem.at[h] for sem in sems],
        )
        for h, (gate, up, down, whole_gate, whole_up, whole_down) in enumerate(
            ((g1, u1, d1, w1, v1, x1), (folded.at[0], folded.at[1], d2, w2, v2, x2))
        )
    )
    close = Close(place, send, partial_value, *close_scratches[:4], close_scratches[4:])
    turns = [(m, side) for m in range(2) for side in range(SIDES)]
    greet(
        [((fs + step) % count, tp) for step in range(1, count)]
        + [(fs, place["peer"]), (fs, place["sibling"])],
        lambda: one.fold_down(t1, stage_down, stage_sem.at[0]),
    )

    for m, side in turns:
        one.cross(m, side)
        one.plane_far(m, side)
        one.plane_near(m, side)
    one.send_down(None)
    one.home_block()
    one.keep()
    one.relay(0, 0)
    two.fold_wide(0, tg2, picked, stage_wide, stage_sem.at[1])
    two.fold_wide(1, tu2, picked, stage_wide, stage_sem.at[1])
    two.fold_down(t2, stage_down, stage_sem.at[0])
    two.keep_folded()
    two.cross(0, 0)
    two.plane_far(0, 0)
    one.whole_block(0, 0)
    one.whole_block(0, 1)
    one.relay(0, 1)
    one.whole_block(0, 2)
    one.whole_block(0, 3)
    one.relay(1, 0)
    one.whole_block(1, 0)
    one.whole_block(1, 1)
    one.relay(1, 1)
    one.whole_block(1, 2)
    one.whole_block(1, 3)
    for m, side in turns:
        two.plane_near(m, side)
    norm_rows(lambda some: tokens[some, :], normed)
    one.pass_down()
    for step in range(2 * SIDES):
        one.main_block(0, step)
    two.home_block()
    two.cross(0, 1)
    two.plane_far(0, 1)
    for step in range(2 * SIDES):
        one.main_block(1, step)
    two.send_down(aligned)
    two.relay(0, 0)
    for step in range(2 * SIDES):
        one.minor_block(0, step)
    for step in range(2 * SIDES):
        one.minor_block(1, step)
    two.relay(0, 1)
    one.second()
    one.kept()
    two.cross(1, 0)
    multiply(
        normed,
        (w1, v1, x1),
        (gate_sum, up_sum),
        partial_value,
    )
    close.scatter()
    two.cross(1, 1)
    two.send_down(unaligned)
    two.whole_block(0, 0)
    close.halve()
    two.plane_far(1, 0)
    two.relay(1, 0)
    two.whole_block(0, 1)
    two.whole_block(0, 2)
    close.spread()
    two.plane_far(1, 1)
    two.relay(1, 1)
    two.whole_block(0, 3)
    two.whole_block(1, 0)
    two.whole_block(1, 1)
    two.whole_block(1, 2)
    two.whole_block(1, 3)
    close.pass_on()
    two.pass_down()
    for step in range(2 * SIDES):
        two.main_block(0, step)
    close.side()
    for step in range(2 * SIDES):
        two.main_block(1, step)
    close.norm(normed, scales, out)
    for step in range(2 * SIDES):
        two.minor_block(0, step)
    for step in range(2 * SIDES):
        two.minor_block(1, step)
    two.second()
    for copy in started:
        copy.wait_send()


def collect(first, second, tokens, scales, picked):
    gate, _, down = first
    rows, columns = gate.shape
    fs, tp = lax.axis_size("fs"), lax.axis_size("tp")
    width = columns * tp // fs
    main = rows - far_part(rows)
    tall, wide = tokens.shape
    whole = pltpu.VMEM((rows * fs, width), jnp.bfloat16)
    whole_down = pltpu.VMEM((down.shape[0], down.shape[1] * tp), jnp.bfloat16)
    any_place = pl.BlockSpec(memory_space=pl.ANY)
    vmem = pl.BlockSpec(memory_space=pltpu.VMEM)
    dma = pltpu.SemaphoreType.DMA
    held = lambda *shape: pltpu.VMEM(shape, jnp.bfloat16)
    relayed = dma((2, 2, SIDES, CHUNKS))
    by_owner = dma((2, 2, fs))
    *weights, normed_one = pl.pallas_call(
        collect_kernel,
        out_shape=(whole, whole, whole_down) * 2
        + (pltpu.VMEM(tokens.shape, tokens.dtype),),
        in_specs=[any_place] * 6 + [vmem] * 3,
        out_specs=(vmem,) * 7,
        scratch_shapes=[
            held(2, 2, SIDES, main, width),
            held(2, *gate.shape),
            held(*down.shape),
            held(*down.shape),
            pltpu.VMEM((2, gate.shape[0] // CUTS, gate.shape[1]), jnp.float32),
            pltpu.VMEM((2, down.shape[0] // CUTS, down.shape[1]), jnp.float32),
            dma((2, 2)),
            pltpu.VMEM((tall, width), jnp.float32),
            pltpu.VMEM((tall, width), jnp.float32),
            held(tall, wide),
            held(tall, wide),
            dma((2, 2, SIDES)),
            relayed,
            relayed,
            relayed,
            by_owner,
            by_owner,
            by_owner,
            by_owner,
            by_owner,
            dma((2, 3)),
            dma((2, 3)),
            dma((2, 2)),
            *close_scratch(tall, wide, fs),
        ],
        compiler_params=pltpu.CompilerParams(
            has_side_effects=True, collective_id=0, vmem_limit_bytes=COLLECT_VMEM
        ),
    )(*first, *second, tokens, scales[None, :], picked[:, None])
    return weights[:3], weights[3:], normed_one


def in_vmem(*arrays):
    return [pltpu.with_memory_space_constraint(a, pltpu.VMEM) for a in arrays]


def serve_kernel(*refs):
    normed, refs = refs[0], refs[1:]
    weights, served, refs = refs[:6], refs[6:12], refs[12:]
    partial_value, gate_sum, up_sum, leave = refs
    copies = [
        pltpu.make_async_copy(weights[m], served[m], leave.at[m]) for m in range(6)
    ]
    for copy in copies:
        copy.start()
    multiply(normed, weights[3:], (gate_sum, up_sum), partial_value)
    for copy in copies:
        copy.wait()


def serve(normed, first, second):
    rows, width = normed.shape
    gate = first[0]
    vmem = pl.BlockSpec(memory_space=pltpu.VMEM)
    any_place = pl.BlockSpec(memory_space=pl.ANY)
    same = lambda a: jax.ShapeDtypeStruct(a.shape, a.dtype)
    weights = (*first, *second)
    sums = pltpu.VMEM((rows, gate.shape[1]), jnp.float32)
    *served, partial_value = pl.pallas_call(
        serve_kernel,
        out_shape=tuple(same(a) for a in weights)
        + (pltpu.VMEM(normed.shape, normed.dtype),),
        in_specs=[vmem] * 7,
        out_specs=(any_place,) * 6 + (vmem,),
        scratch_shapes=[sums, sums, pltpu.SemaphoreType.DMA((6,))],
        compiler_params=pltpu.CompilerParams(vmem_limit_bytes=SERVE_VMEM),
        cost_estimate=pl.CostEstimate(
            flops=6 * rows * gate.size, bytes_accessed=12 * gate.size, transcendentals=0
        ),
    )(*in_vmem(normed, *weights))
    return served[:3], served[3:], partial_value


def close_kernel(partial_value, normed, scales, out, *scratches):
    place = placing()
    send, started = sender()
    close = Close(place, send, partial_value, *scratches[:4], scratches[4:])
    greet(
        [(close.zone(step) * SIDES + close.y, close.tp) for step in range(1, close.zones)]
        + [(close.z * SIDES + 1 - close.y, close.tp)]
    )
    close.scatter()
    close.halve()
    close.spread()
    close.pass_on()
    close.side()
    close.norm(normed, scales, out)
    for copy in started:
        copy.wait_send()


def close(partial_value, normed, scales):
    rows, width = normed.shape
    vmem = pl.BlockSpec(memory_space=pltpu.VMEM)
    return pl.pallas_call(
        close_kernel,
        out_shape=pltpu.VMEM((rows, width), jnp.bfloat16),
        in_specs=[vmem] * 3,
        out_specs=vmem,
        scratch_shapes=close_scratch(rows, width, lax.axis_size("fs")),
        compiler_params=pltpu.CompilerParams(
            has_side_effects=True, collective_id=1, vmem_limit_bytes=SERVE_VMEM
        ),
    )(*in_vmem(partial_value, normed), scales[None, :])


def on_device(
    use_kernels,
    tokens,
    gain_first,
    gain_second,
    gate_first,
    up_first,
    down_first,
    gate_second,
    up_second,
    down_second,
):
    row_count = gate_first.shape[0]
    offset = lax.axis_index("fs") * row_count
    pick = lambda scales: lax.dynamic_slice_in_dim(scales, offset, row_count, 0)

    def fold_gain(weight, scales):
        return (pick(scales)[:, None] * weight).astype(jnp.bfloat16)

    gate, up = fold_gain(gate_first, gain_first), fold_gain(up_first, gain_first)
    if use_kernels:
        first, second, normed_one = collect(
            (gate, up, down_first),
            (gate_second, up_second, down_second),
            tokens,
            gain_first,
            pick(gain_second),
        )
        first, second, partial_value = serve(normed_one, first, second)
        result_rows = close(partial_value, normed_one, gain_second)
    else:
        first = collect_plain(gate, up, down_first.astype(jnp.bfloat16))
        second = collect_plain(
            fold_gain(gate_second, gain_second),
            fold_gain(up_second, gain_second),
            down_second.astype(jnp.bfloat16),
        )
        normed_zero = plain_norm(tokens).astype(jnp.bfloat16)
        normed_one = half_step_plain(normed_zero, gain_first, *first)
        result_rows = half_step_plain(normed_one, gain_second, *second)
    return (result_rows, *first, *second)


def solution(mesh):
    fs, tp = mesh.shape["fs"], mesh.shape["tp"]
    use_kernels = tp == 2 * CORES and fs == tp * SIDES
    placed = (P("tp", None), P(), P()) + (P("fs", "tp"),) * 6
    served = (P(None, "fs"), P(None, "fs"), P("fs", None))
    return jax.shard_map(
        functools.partial(on_device, use_kernels),
        mesh=mesh,
        in_specs=placed,
        out_specs=(P("tp", None),) + served + served,
        check_vma=False,
    )
```

```python
import functools

import jax
import jax.numpy as jnp
from jax import lax
from jax.experimental import pallas as pl
from jax.experimental.pallas import tpu as pltpu
from jax.sharding import PartitionSpec as P

MESH = pl.DeviceIdType.MESH
CORES = 2
SIDES = 2
COLLECT_VMEM = 24 * 2**20
SERVE_VMEM = 24 * 2**20
CUTS = 4
FAR = 5, 24
CHUNKS = 4


def plain_norm(values):
    values = values.astype(jnp.float32)
    center = jnp.mean(values, axis=-1, keepdims=True)
    spread = jnp.mean(jnp.square(values - center), axis=-1, keepdims=True)
    return (values - center) * lax.rsqrt(spread + 1e-05)


def sum_over_hidden(partial_value):
    pieces = lax.all_to_all(
        partial_value.astype(jnp.bfloat16), "fs", split_axis=1, concat_axis=0, tiled=True
    )
    rows = partial_value.shape[0]
    pieces = pieces.reshape(-1, rows, pieces.shape[1]).astype(jnp.float32)
    summed = jnp.sum(pieces, axis=0).astype(jnp.bfloat16)
    return lax.all_gather(summed, "fs", axis=1, tiled=True).astype(jnp.float32)


def regroup(folded):
    spread = lax.all_to_all(folded, "tp", split_axis=0, concat_axis=1, tiled=True)
    parts = lax.axis_size("fs")
    rows = spread.shape[0]
    owned = lax.all_to_all(spread, "fs", split_axis=1, concat_axis=0, tiled=True)
    owned = owned.reshape(parts, rows, owned.shape[1])
    whole = lax.all_gather(owned, "tp", axis=1, tiled=True)
    return whole.reshape(-1, whole.shape[2])


def collect_plain(gate, up, down):
    return (
        regroup(gate),
        regroup(up),
        lax.all_gather(down, "tp", axis=1, tiled=True),
    )


def half_step_plain(normed, scales, w_gate, w_rising, w_down):
    gate_part = jnp.dot(normed, w_gate, preferred_element_type=jnp.float32)
    rising = jnp.dot(normed, w_rising, preferred_element_type=jnp.float32)
    hidden = (jax.nn.silu(gate_part) * rising).astype(jnp.bfloat16)
    partial_value = jnp.dot(hidden, w_down, preferred_element_type=jnp.float32)
    block = sum_over_hidden(partial_value)
    mixed = 1.6817928 * scales[None, :] * normed.astype(jnp.float32) + 0.5 * block
    return plain_norm(mixed).astype(jnp.bfloat16)


class Send:
    def __init__(self, when, src, dst, send, recv, to):
        self.when = when
        self.copy = pltpu.make_async_remote_copy(
            src_ref=src,
            dst_ref=dst,
            send_sem=send,
            recv_sem=recv,
            device_id=to,
            device_id_type=MESH,
        )

    def start(self):
        if self.when is None:
            self.copy.start()
        else:
            pl.when(self.when)(self.copy.start)

    def wait_send(self):
        if self.when is None:
            self.copy.wait_send()
        else:
            pl.when(self.when)(self.copy.wait_send)


def landed(ref, sem):
    pltpu.make_async_copy(ref, ref, sem).wait()


def far_part(rows):
    return rows * FAR[0] // FAR[1] // 16 * 16


def chunks(rows):
    edges = [rows // 16 * k // CHUNKS * 16 for k in range(CHUNKS + 1)]
    return [(a, b - a) for a, b in zip(edges, edges[1:])]


class Hand:
    def __init__(self, place, send, sources, wholes, down, whole_down, scratch, sems):
        self.__dict__.update(place)
        self.send = send
        self.sources, self.wholes = sources, wholes
        self.down, self.whole_down = down, whole_down
        self.passing = scratch
        (
            self.s_plane,
            self.s_cross,
            self.r_cross,
            self.s_pass,
            self.r_main,
            self.r_minor,
            self.s_main,
            self.s_minor,
            self.s_over,
            self.s_down,
            self.r_down,
        ) = sems
        self.rows = sources[0].shape[0]
        self.width = wholes[0].shape[1]
        self.part = far_part(self.rows)
        self.main = self.rows - self.part
        self.main_at = jnp.where(self.aligned, self.part, 0)
        self.over_at = jnp.where(self.aligned, self.main, 0)
        self.minor_at = jnp.where(self.aligned, 0, self.main)

    def here(self, col):
        return (self.fs, col)

    def cols(self, m, start, size, side):
        return self.sources[m].at[pl.ds(start, size), pl.ds(side * self.width, self.width)]

    def at(self, m, owner, start, size):
        first = pl.multiple_of(owner * self.rows + start, 16)
        return self.wholes[m].at[pl.ds(first, size), :]

    def column(self, col):
        lanes = self.down.shape[1]
        return self.whole_down.at[:, pl.ds(pl.multiple_of(col * lanes, 128), lanes)]

    def own(self, m):
        first = pl.multiple_of(self.y * self.width, 128)
        return self.sources[m].at[:, pl.ds(first, self.width)]

    def cross(self, m, side):
        for k, (start, size) in enumerate(chunks(self.main)):
            self.send(
                jnp.logical_not(self.aligned),
                self.cols(m, start, size, side),
                self.passing.at[m, side, pl.ds(start, size)],
                self.s_cross.at[m, side, k],
                self.r_cross.at[m, side, k],
                self.here(self.peer),
            )

    def plane_far(self, m, side):
        self.send(
            jnp.logical_not(self.aligned),
            self.cols(m, self.part, self.main, side),
            self.at(m, self.fs, self.part, self.main),
            self.s_plane.at[m, side],
            self.r_main.at[m, self.fs],
            (self.tp * SIDES + side, self.tp),
        )

    def plane_near(self, m, side):
        owner = self.tp * SIDES + side
        self.send(
            jnp.logical_and(self.aligned, owner != self.fs),
            self.cols(m, 0, self.rows, side),
            self.at(m, self.fs, 0, self.rows),
            self.s_plane.at[m, side],
            self.r_main.at[m, self.fs],
            (owner, self.tp),
        )

    def send_down(self, when):
        for k, to in enumerate((self.peer, self.sibling)):
            self.send(
                when,
                self.down,
                self.column(self.tp),
                self.s_down.at[k],
                self.r_down.at[k],
                self.here(to),
            )

    def home_block(self):
        home = jnp.logical_and(self.aligned, self.primary)
        for m in range(2):
            for sem, to in ((self.s_over, self.peer), (self.s_main, self.sibling)):
                self.send(
                    home,
                    self.own(m),
                    self.at(m, self.fs, 0, self.rows),
                    sem.at[m, self.fs],
                    self.r_main.at[m, self.fs],
                    self.here(to),
                )

    def fold_down(self, trained, stage, sem):
        lanes = self.down.shape[1]
        mine = pl.ds(pl.multiple_of(self.tp * lanes, 128), lanes)

        def put(rows, tile):
            self.down[rows, :] = tile.astype(jnp.bfloat16)
            self.whole_down[rows, mine] = tile.astype(jnp.bfloat16)

        by_tiles(trained, stage, sem, put)

    def fold_wide(self, m, trained, scales, stage, sem):
        def put(rows, tile):
            self.sources[m][rows, :] = (scales[rows, :] * tile).astype(jnp.bfloat16)

        by_tiles(trained, stage, sem, put)

    def keep_folded(self):
        mine = pl.ds(pl.multiple_of(self.y * self.width, 128), self.width)

        def tile(index, carry):
            rows = pl.ds(pl.multiple_of(index * 16, 16), 16)
            first = pl.multiple_of(self.fs * self.rows + index * 16, 16)
            for m in range(2):
                self.wholes[m][pl.ds(first, 16), :] = self.sources[m][rows, mine]
            return carry

        def block():
            lax.fori_loop(0, self.rows // 16, tile, 0)

        guarded(jnp.logical_and(self.aligned, self.primary), block)

    def relay(self, m, side):
        zone = (1 - self.x) * CORES + self.c
        for k, (start, size) in enumerate(chunks(self.main)):
            held = self.passing.at[m, side, pl.ds(start, size)]
            guarded(self.aligned, landed, held, self.r_cross.at[m, side, k])
            self.send(
                self.aligned,
                held,
                self.at(m, self.fs, start, size),
                self.s_pass.at[m, side, k],
                self.r_main.at[m, self.fs],
                (zone * SIDES + side, self.tp),
            )

    def near(self, step):
        return self.half * 2 * SIDES + (self.fs + step) % (2 * SIDES)

    def far(self, step):
        return (1 - self.half) * 2 * SIDES + (self.fs + step) % (2 * SIDES)

    def whole_block(self, m, step):
        owner = self.near(step)
        block = self.at(m, owner, 0, self.rows)
        got = self.primary
        if step == 0:
            got = jnp.logical_and(got, jnp.logical_not(self.aligned))
        guarded(got, landed, block, self.r_main.at[m, owner])
        if step:
            self.send(
                jnp.logical_and(self.primary, self.aligned),
                block,
                block,
                self.s_over.at[m, owner],
                self.r_main.at[m, owner],
                self.here(self.peer),
            )
        self.send(
            got,
            block,
            block,
            self.s_main.at[m, owner],
            self.r_main.at[m, owner],
            self.here(self.sibling),
        )

    def pass_down(self):
        got = self.column(self.peer)
        landed(got, self.r_down.at[0])
        self.send(
            None, got, got, self.s_down.at[2], self.r_down.at[2], self.here(self.sibling)
        )

    def main_block(self, m, step):
        owner = self.far(step)
        block = self.at(m, owner, self.main_at, self.main)
        over = self.at(m, owner, self.over_at, self.part)
        guarded(self.primary, landed, block, self.r_main.at[m, owner])
        self.send(
            self.primary,
            over,
            over,
            self.s_over.at[m, owner],
            self.r_minor.at[m, owner],
            self.here(self.peer),
        )
        self.send(
            self.primary,
            block,
            block,
            self.s_main.at[m, owner],
            self.r_main.at[m, owner],
            self.here(self.sibling),
        )

    def minor_block(self, m, step):
        owner = self.far(step)
        block = self.at(m, owner, self.minor_at, self.part)
        guarded(self.primary, landed, block, self.r_minor.at[m, owner])
        self.send(
            self.primary,
            block,
            block,
            self.s_minor.at[m, owner],
            self.r_minor.at[m, owner],
            self.here(self.sibling),
        )

    def second(self):
        other = jnp.logical_not(self.primary)
        for m in range(2):
            for step in range(2 * SIDES):
                owner = self.near(step)
                block = self.at(m, owner, 0, self.rows)
                guarded(other, landed, block, self.r_main.at[m, owner])
                owner = self.far(step)
                block = self.at(m, owner, self.main_at, self.main)
                guarded(other, landed, block, self.r_main.at[m, owner])
                block = self.at(m, owner, self.minor_at, self.part)
                guarded(other, landed, block, self.r_minor.at[m, owner])
        landed(self.column(self.sibling), self.r_down.at[1])
        landed(self.column((1 - self.x) * CORES + 1 - self.c), self.r_down.at[2])


def guarded(when, act, *args):
    if when is None:
        act(*args)
    else:
        pl.when(when)(functools.partial(act, *args))


def beside_zone(zone):
    return zone + 1 - 2 * (zone % 2)


class Close:
    def __init__(self, place, send, partial_value, beside, halves, along, full, sems):
        self.__dict__.update(place)
        self.send = send
        self.partial_value, self.beside = partial_value, beside
        self.halves, self.along, self.full = halves, along, full
        (
            self.s_y,
            self.r_y,
            self.s_z,
            self.r_z,
            self.s_up,
            self.r_up,
            self.s_side,
            self.r_side,
        ) = sems
        self.zones = beside.shape[0]
        self.near = beside_zone(self.z)
        self.over = (self.z + 2) % self.zones
        self.last = beside_zone(self.over)

    def piece(self, zone, side):
        width = self.full.shape[2]
        first = (zone * SIDES + side) * width
        return pl.ds(pl.multiple_of(first, 128), width)

    def zone(self, step):
        return (self.z + self.zones + step) % self.zones

    def held(self, zone, side):
        return self.full.at[zone * SIDES + side]

    def scatter(self):
        for step in (*range(1, self.zones), 0):
            self.send(
                None,
                self.partial_value.at[:, self.piece(self.zone(step), 1 - self.y)],
                self.beside.at[step],
                self.s_y.at[step],
                self.r_y.at[step],
                (self.z * SIDES + 1 - self.y, self.tp),
            )

    def both_sides(self, step):
        landed(self.beside.at[step], self.r_y.at[step])
        mine = self.partial_value[:, self.piece(self.zone(step), self.y)]
        return mine.astype(jnp.float32) + self.beside[step].astype(jnp.float32)

    def halve(self):
        for step in range(1, self.zones):
            self.halves[step - 1] = self.both_sides(step).astype(jnp.bfloat16)
            self.send(
                None,
                self.halves.at[step - 1],
                self.along.at[step - 1],
                self.s_z.at[step - 1],
                self.r_z.at[step - 1],
                (self.zone(step) * SIDES + self.y, self.tp),
            )

    def to_side(self, step, block):
        self.send(
            None,
            block,
            block,
            self.s_side.at[step],
            self.r_side.at[step],
            (self.z * SIDES + 1 - self.y, self.tp),
        )

    def to_zone(self, kind, block, zone):
        self.send(
            None,
            block,
            block,
            self.s_up.at[kind],
            self.r_up.at[kind],
            (zone * SIDES + self.y, self.tp),
        )

    def spread(self):
        total = self.both_sides(0)
        for step in range(1, self.zones):
            landed(self.along.at[step - 1], self.r_z.at[step - 1])
            total += self.along[step - 1].astype(jnp.float32)
        self.full[self.fs] = total.astype(jnp.bfloat16)
        block = self.held(self.z, self.y)
        self.to_zone(0, block, self.over)
        self.to_zone(1, block, self.near)
        self.to_side(0, block)

    def pass_on(self):
        block = self.held(self.over, self.y)
        landed(block, self.r_up.at[0])
        self.to_zone(2, block, self.near)
        self.to_side(1, block)

    def side(self):
        for kind, zone in ((1, self.near), (2, self.last)):
            block = self.held(zone, self.y)
            landed(block, self.r_up.at[kind])
            self.to_side(kind + 1, block)

    def norm(self, normed, scales, out):
        for step, zone in enumerate((self.z, self.over, self.near, self.last)):
            landed(self.held(zone, 1 - self.y), self.r_side.at[step])

        def mixed(some):
            block = jnp.concatenate(
                [
                    self.full[k, some, :].astype(jnp.float32)
                    for k in range(self.full.shape[0])
                ],
                axis=1,
            )
            old = 1.6817928 * scales[...] * normed[some, :].astype(jnp.float32)
            return old + 0.5 * block

        norm_rows(mixed, out)


def norm_rows(values, out):
    tall = 16

    def some_rows(index, carry):
        some = pl.ds(pl.multiple_of(index * tall, tall), tall)
        out[some, :] = plain_norm(values(some)).astype(jnp.bfloat16)
        return carry

    lax.fori_loop(0, out.shape[0] // tall, some_rows, 0)


def greet(partners, meanwhile=None):
    barrier = pltpu.get_barrier_semaphore()
    for partner in partners:
        pl.semaphore_signal(barrier, inc=1, device_id=partner, device_id_type=MESH)
    if meanwhile is not None:
        meanwhile()
    pl.semaphore_wait(barrier, len(partners))


def by_tiles(src, stage, sem, put):
    tall = stage.shape[1]
    count = src.shape[0] // tall

    def fetch(k):
        return pltpu.make_async_copy(
            src.at[pl.ds(k * tall, tall), :], stage.at[k % 2], sem.at[k % 2]
        )

    fetch(0).start()
    for k in range(count):
        if k + 1 < count:
            fetch(k + 1).start()
        fetch(k).wait()

        def tile(index, carry, k=k):
            first = pl.multiple_of(index * 16, 16)
            rows = pl.ds(pl.multiple_of(k * tall + index * 16, 16), 16)
            put(rows, stage[k % 2, pl.ds(first, 16), :])
            return carry

        lax.fori_loop(0, tall // 16, tile, 0)


def close_scratch(rows, width, count):
    held = lambda many: pltpu.VMEM((many, rows, width // count), jnp.bfloat16)
    zones = count // SIDES
    dma = pltpu.SemaphoreType.DMA
    sems = [dma((many,)) for many in (zones, zones - 1, zones - 1, zones)]
    return [held(zones), held(zones - 1), held(zones - 1), held(count)] + [
        sem for sem in sems for _ in range(2)
    ]


def placing():
    fs = lax.axis_index("fs")
    tp = lax.axis_index("tp")
    z, x, c = fs // SIDES, tp // CORES, tp % CORES
    return dict(
        fs=fs,
        tp=tp,
        z=z,
        y=fs % SIDES,
        x=x,
        c=c,
        half=z // 2,
        aligned=x == z // 2,
        primary=c == z % 2,
        peer=(1 - x) * CORES + c,
        sibling=x * CORES + 1 - c,
    )


def sender():
    started = []

    def send(*args):
        one = Send(*args)
        one.start()
        started.append(one)

    return send, started


def multiply(normed, weights, sums, partial_value):
    gate, up, down = weights
    deep = gate.shape[0] // CUTS
    wide = down.shape[1] // CUTS
    for k in range(CUTS):
        n = normed[:, k * deep : (k + 1) * deep]
        for weight, total in zip((gate, up), sums):
            term = jnp.dot(
                n,
                weight[k * deep : (k + 1) * deep, :],
                preferred_element_type=jnp.float32,
            )
            if k:
                total[...] += term
            else:
                total[...] = term
    hidden = (jax.nn.silu(sums[0][...]) * sums[1][...]).astype(jnp.bfloat16)
    for k in range(CUTS):
        partial_value[:, k * wide : (k + 1) * wide] = jnp.dot(
            hidden,
            down[:, k * wide : (k + 1) * wide],
            preferred_element_type=jnp.float32,
        ).astype(jnp.bfloat16)


def collect_kernel(*refs):
    (tg1, tu1, t1, tg2, tu2, t2, tokens, scales, picks), refs = refs[:9], refs[9:]
    (w1, v1, x1, w2, v2, x2, out), refs = refs[:7], refs[7:]
    (passing, folded, d1, d2), refs = refs[:4], refs[4:]
    (stage_wide, stage_down, stage_sem), refs = refs[:3], refs[3:]
    (gate_sum, up_sum), refs = refs[:2], refs[2:]
    (normed, partial_value), refs = refs[:2], refs[2:]
    sems, refs = refs[:11], refs[11:]
    close_scratches = refs
    place = placing()
    fs, tp = place["fs"], place["tp"]
    count = lax.axis_size("fs")
    aligned = place["aligned"]
    unaligned = jnp.logical_not(aligned)
    send, started = sender()
    one, two = (
        Hand(
            place,
            send,
            (gate, up),
            (whole_gate, whole_up),
            down,
            whole_down,
            passing.at[h],
            [sem.at[h] for sem in sems],
        )
        for h, (gate, up, down, whole_gate, whole_up, whole_down) in enumerate(
            (
                (folded.at[0], folded.at[1], d1, w1, v1, x1),
                (folded.at[2], folded.at[3], d2, w2, v2, x2),
            )
        )
    )
    close = Close(place, send, partial_value, *close_scratches[:4], close_scratches[4:])
    turns = [(m, side) for m in range(2) for side in range(SIDES)]

    def first_folds():
        one.fold_wide(0, tg1, picks.at[0], stage_wide, stage_sem.at[1])

    greet(
        [((fs + step) % count, tp) for step in range(1, count)]
        + [(fs, place["peer"]), (fs, place["sibling"])],
        first_folds,
    )

    for m in range(2):
        if m:
            one.fold_wide(1, tu1, picks.at[0], stage_wide, stage_sem.at[1])
        for side in range(SIDES):
            one.cross(m, side)
            one.plane_far(m, side)
            one.plane_near(m, side)
    one.fold_down(t1, stage_down, stage_sem.at[0])
    one.send_down(None)
    one.home_block()
    one.keep_folded()
    one.relay(0, 0)
    two.fold_wide(0, tg2, picks.at[1], stage_wide, stage_sem.at[1])
    two.fold_wide(1, tu2, picks.at[1], stage_wide, stage_sem.at[1])
    two.fold_down(t2, stage_down, stage_sem.at[0])
    two.keep_folded()
    two.cross(0, 0)
    two.plane_far(0, 0)
    one.whole_block(0, 0)
    one.whole_block(0, 1)
    one.relay(0, 1)
    one.whole_block(0, 2)
    one.whole_block(0, 3)
    one.relay(1, 0)
    one.whole_block(1, 0)
    one.whole_block(1, 1)
    one.relay(1, 1)
    one.whole_block(1, 2)
    one.whole_block(1, 3)
    for m, side in turns:
        two.plane_near(m, side)
    norm_rows(lambda some: tokens[some, :], normed)
    one.pass_down()
    for step in range(2 * SIDES):
        one.main_block(0, step)
    two.home_block()
    two.cross(0, 1)
    two.plane_far(0, 1)
    two.relay(0, 0)
    for step in range(2 * SIDES):
        one.main_block(1, step)
    two.send_down(aligned)
    for step in range(2 * SIDES):
        one.minor_block(0, step)
    for step in range(2 * SIDES):
        one.minor_block(1, step)
    two.relay(0, 1)
    one.second()
    two.cross(1, 0)
    multiply(
        normed,
        (w1, v1, x1),
        (gate_sum, up_sum),
        partial_value,
    )
    close.scatter()
    two.cross(1, 1)
    two.send_down(unaligned)
    two.whole_block(0, 0)
    close.halve()
    two.plane_far(1, 0)
    two.relay(1, 0)
    two.whole_block(0, 1)
    two.whole_block(0, 2)
    close.spread()
    two.plane_far(1, 1)
    two.relay(1, 1)
    two.whole_block(0, 3)
    two.whole_block(1, 0)
    two.whole_block(1, 1)
    two.whole_block(1, 2)
    two.whole_block(1, 3)
    close.pass_on()
    two.pass_down()
    for step in range(2 * SIDES):
        two.main_block(0, step)
    close.side()
    for step in range(2 * SIDES):
        two.main_block(1, step)
    close.norm(normed, scales, out)
    for step in range(2 * SIDES):
        two.minor_block(0, step)
    for step in range(2 * SIDES):
        two.minor_block(1, step)
    two.second()
    for copy in started:
        copy.wait_send()


def collect(first, second, tokens, scales, picks):
    gate, _, down = first
    rows, columns = gate.shape
    fs, tp = lax.axis_size("fs"), lax.axis_size("tp")
    width = columns * tp // fs
    main = rows - far_part(rows)
    tall, wide = tokens.shape
    whole = pltpu.VMEM((rows * fs, width), jnp.bfloat16)
    whole_down = pltpu.VMEM((down.shape[0], down.shape[1] * tp), jnp.bfloat16)
    any_place = pl.BlockSpec(memory_space=pl.ANY)
    vmem = pl.BlockSpec(memory_space=pltpu.VMEM)
    dma = pltpu.SemaphoreType.DMA
    held = lambda *shape: pltpu.VMEM(shape, jnp.bfloat16)
    relayed = dma((2, 2, SIDES, CHUNKS))
    by_owner = dma((2, 2, fs))
    *weights, normed_one = pl.pallas_call(
        collect_kernel,
        out_shape=(whole, whole, whole_down) * 2
        + (pltpu.VMEM(tokens.shape, tokens.dtype),),
        in_specs=[any_place] * 6 + [vmem] * 3,
        out_specs=(vmem,) * 7,
        scratch_shapes=[
            held(2, 2, SIDES, main, width),
            held(4, *gate.shape),
            held(*down.shape),
            held(*down.shape),
            pltpu.VMEM((2, gate.shape[0] // CUTS, gate.shape[1]), jnp.float32),
            pltpu.VMEM((2, down.shape[0] // CUTS, down.shape[1]), jnp.float32),
            dma((2, 2)),
            pltpu.VMEM((tall, width), jnp.float32),
            pltpu.VMEM((tall, width), jnp.float32),
            held(tall, wide),
            held(tall, wide),
            dma((2, 2, SIDES)),
            relayed,
            relayed,
            relayed,
            by_owner,
            by_owner,
            by_owner,
            by_owner,
            by_owner,
            dma((2, 3)),
            dma((2, 3)),
            *close_scratch(tall, wide, fs),
        ],
        compiler_params=pltpu.CompilerParams(
            has_side_effects=True, collective_id=0, vmem_limit_bytes=COLLECT_VMEM
        ),
    )(*first, *second, tokens, scales[None, :], picks[:, :, None])
    return weights[:3], weights[3:], normed_one


def in_vmem(*arrays):
    return [pltpu.with_memory_space_constraint(a, pltpu.VMEM) for a in arrays]


def serve_kernel(*refs):
    normed, refs = refs[0], refs[1:]
    weights, served, refs = refs[:6], refs[6:12], refs[12:]
    partial_value, gate_sum, up_sum, leave = refs
    copies = [
        pltpu.make_async_copy(weights[m], served[m], leave.at[m]) for m in range(6)
    ]
    for copy in copies:
        copy.start()
    multiply(normed, weights[3:], (gate_sum, up_sum), partial_value)
    for copy in copies:
        copy.wait()


def serve(normed, first, second):
    rows, width = normed.shape
    gate = first[0]
    vmem = pl.BlockSpec(memory_space=pltpu.VMEM)
    any_place = pl.BlockSpec(memory_space=pl.ANY)
    same = lambda a: jax.ShapeDtypeStruct(a.shape, a.dtype)
    weights = (*first, *second)
    sums = pltpu.VMEM((rows, gate.shape[1]), jnp.float32)
    *served, partial_value = pl.pallas_call(
        serve_kernel,
        out_shape=tuple(same(a) for a in weights)
        + (pltpu.VMEM(normed.shape, normed.dtype),),
        in_specs=[vmem] * 7,
        out_specs=(any_place,) * 6 + (vmem,),
        scratch_shapes=[sums, sums, pltpu.SemaphoreType.DMA((6,))],
        compiler_params=pltpu.CompilerParams(vmem_limit_bytes=SERVE_VMEM),
        cost_estimate=pl.CostEstimate(
            flops=6 * rows * gate.size, bytes_accessed=12 * gate.size, transcendentals=0
        ),
    )(*in_vmem(normed, *weights))
    return served[:3], served[3:], partial_value


def close_kernel(partial_value, normed, scales, out, *scratches):
    place = placing()
    send, started = sender()
    close = Close(place, send, partial_value, *scratches[:4], scratches[4:])
    greet(
        [(close.zone(step) * SIDES + close.y, close.tp) for step in range(1, close.zones)]
        + [(close.z * SIDES + 1 - close.y, close.tp)]
    )
    close.scatter()
    close.halve()
    close.spread()
    close.pass_on()
    close.side()
    close.norm(normed, scales, out)
    for copy in started:
        copy.wait_send()


def close(partial_value, normed, scales):
    rows, width = normed.shape
    vmem = pl.BlockSpec(memory_space=pltpu.VMEM)
    return pl.pallas_call(
        close_kernel,
        out_shape=pltpu.VMEM((rows, width), jnp.bfloat16),
        in_specs=[vmem] * 3,
        out_specs=vmem,
        scratch_shapes=close_scratch(rows, width, lax.axis_size("fs")),
        compiler_params=pltpu.CompilerParams(
            has_side_effects=True, collective_id=1, vmem_limit_bytes=SERVE_VMEM
        ),
    )(*in_vmem(partial_value, normed), scales[None, :])


def on_device(
    use_kernels,
    tokens,
    gain_first,
    gain_second,
    gate_first,
    up_first,
    down_first,
    gate_second,
    up_second,
    down_second,
):
    row_count = gate_first.shape[0]
    offset = lax.axis_index("fs") * row_count
    pick = lambda scales: lax.dynamic_slice_in_dim(scales, offset, row_count, 0)

    def fold_gain(weight, scales):
        return (pick(scales)[:, None] * weight).astype(jnp.bfloat16)

    if use_kernels:
        first, second, normed_one = collect(
            (gate_first, up_first, down_first),
            (gate_second, up_second, down_second),
            tokens,
            gain_first,
            jnp.stack([pick(gain_first), pick(gain_second)]),
        )
        first, second, partial_value = serve(normed_one, first, second)
        result_rows = close(partial_value, normed_one, gain_second)
    else:
        first = collect_plain(
            fold_gain(gate_first, gain_first),
            fold_gain(up_first, gain_first),
            down_first.astype(jnp.bfloat16),
        )
        second = collect_plain(
            fold_gain(gate_second, gain_second),
            fold_gain(up_second, gain_second),
            down_second.astype(jnp.bfloat16),
        )
        normed_zero = plain_norm(tokens).astype(jnp.bfloat16)
        normed_one = half_step_plain(normed_zero, gain_first, *first)
        result_rows = half_step_plain(normed_one, gain_second, *second)
    return (result_rows, *first, *second)


def solution(mesh):
    fs, tp = mesh.shape["fs"], mesh.shape["tp"]
    use_kernels = tp == 2 * CORES and fs == tp * SIDES
    placed = (P("tp", None), P(), P()) + (P("fs", "tp"),) * 6
    served = (P(None, "fs"), P(None, "fs"), P("fs", None))
    return jax.shard_map(
        functools.partial(on_device, use_kernels),
        mesh=mesh,
        in_specs=placed,
        out_specs=(P("tp", None),) + served + served,
        check_vma=False,
    )
```

```python
import functools

import jax
import jax.numpy as jnp
from jax import lax
from jax.experimental import pallas as pl
from jax.experimental.pallas import tpu as pltpu
from jax.sharding import PartitionSpec as P

MESH = pl.DeviceIdType.MESH
CORES = 2
SIDES = 2
COLLECT_VMEM = 24 * 2**20
SERVE_VMEM = 24 * 2**20
CUTS = 4
FAR = 5, 24
CHUNKS = 4


def plain_norm(values):
    values = values.astype(jnp.float32)
    center = jnp.mean(values, axis=-1, keepdims=True)
    spread = jnp.mean(jnp.square(values - center), axis=-1, keepdims=True)
    return (values - center) * lax.rsqrt(spread + 1e-05)


def sum_over_hidden(partial_value):
    pieces = lax.all_to_all(
        partial_value.astype(jnp.bfloat16), "fs", split_axis=1, concat_axis=0, tiled=True
    )
    rows = partial_value.shape[0]
    pieces = pieces.reshape(-1, rows, pieces.shape[1]).astype(jnp.float32)
    summed = jnp.sum(pieces, axis=0).astype(jnp.bfloat16)
    return lax.all_gather(summed, "fs", axis=1, tiled=True).astype(jnp.float32)


def regroup(folded):
    spread = lax.all_to_all(folded, "tp", split_axis=0, concat_axis=1, tiled=True)
    parts = lax.axis_size("fs")
    rows = spread.shape[0]
    owned = lax.all_to_all(spread, "fs", split_axis=1, concat_axis=0, tiled=True)
    owned = owned.reshape(parts, rows, owned.shape[1])
    whole = lax.all_gather(owned, "tp", axis=1, tiled=True)
    return whole.reshape(-1, whole.shape[2])


def collect_plain(gate, up, down):
    return (
        regroup(gate),
        regroup(up),
        lax.all_gather(down, "tp", axis=1, tiled=True),
    )


def half_step_plain(normed, scales, w_gate, w_rising, w_down):
    gate_part = jnp.dot(normed, w_gate, preferred_element_type=jnp.float32)
    rising = jnp.dot(normed, w_rising, preferred_element_type=jnp.float32)
    hidden = (jax.nn.silu(gate_part) * rising).astype(jnp.bfloat16)
    partial_value = jnp.dot(hidden, w_down, preferred_element_type=jnp.float32)
    block = sum_over_hidden(partial_value)
    mixed = 1.6817928 * scales[None, :] * normed.astype(jnp.float32) + 0.5 * block
    return plain_norm(mixed).astype(jnp.bfloat16)


class Send:
    def __init__(self, when, src, dst, send, recv, to):
        self.when = when
        self.copy = pltpu.make_async_remote_copy(
            src_ref=src,
            dst_ref=dst,
            send_sem=send,
            recv_sem=recv,
            device_id=to,
            device_id_type=MESH,
        )

    def start(self):
        if self.when is None:
            self.copy.start()
        else:
            pl.when(self.when)(self.copy.start)

    def wait_send(self):
        if self.when is None:
            self.copy.wait_send()
        else:
            pl.when(self.when)(self.copy.wait_send)


def landed(ref, sem):
    pltpu.make_async_copy(ref, ref, sem).wait()


def far_part(rows):
    return rows * FAR[0] // FAR[1] // 16 * 16


def chunks(rows):
    edges = [rows // 16 * k // CHUNKS * 16 for k in range(CHUNKS + 1)]
    return [(a, b - a) for a, b in zip(edges, edges[1:])]


class Hand:
    def __init__(self, place, send, sources, wholes, down, whole_down, scratch, sems):
        self.__dict__.update(place)
        self.send = send
        self.sources, self.wholes = sources, wholes
        self.down, self.whole_down = down, whole_down
        self.passing = scratch
        (
            self.s_plane,
            self.s_cross,
            self.r_cross,
            self.s_pass,
            self.r_main,
            self.r_minor,
            self.s_main,
            self.s_minor,
            self.s_over,
            self.s_down,
            self.r_down,
        ) = sems
        self.rows = sources[0].shape[0]
        self.width = wholes[0].shape[1]
        self.part = far_part(self.rows)
        self.main = self.rows - self.part
        self.main_at = jnp.where(self.aligned, self.part, 0)
        self.over_at = jnp.where(self.aligned, self.main, 0)
        self.minor_at = jnp.where(self.aligned, 0, self.main)

    def here(self, col):
        return (self.fs, col)

    def cols(self, m, start, size, side):
        return self.sources[m].at[pl.ds(start, size), pl.ds(side * self.width, self.width)]

    def at(self, m, owner, start, size):
        first = pl.multiple_of(owner * self.rows + start, 16)
        return self.wholes[m].at[pl.ds(first, size), :]

    def column(self, col):
        lanes = self.down.shape[1]
        return self.whole_down.at[:, pl.ds(pl.multiple_of(col * lanes, 128), lanes)]

    def own(self, m):
        first = pl.multiple_of(self.y * self.width, 128)
        return self.sources[m].at[:, pl.ds(first, self.width)]

    def cross(self, m, side):
        for k, (start, size) in enumerate(chunks(self.main)):
            self.send(
                jnp.logical_not(self.aligned),
                self.cols(m, start, size, side),
                self.passing.at[m, side, pl.ds(start, size)],
                self.s_cross.at[m, side, k],
                self.r_cross.at[m, side, k],
                self.here(self.peer),
            )

    def plane_far(self, m, side):
        self.send(
            jnp.logical_not(self.aligned),
            self.cols(m, self.part, self.main, side),
            self.at(m, self.fs, self.part, self.main),
            self.s_plane.at[m, side],
            self.r_main.at[m, self.fs],
            (self.tp * SIDES + side, self.tp),
        )

    def plane_near(self, m, side):
        owner = self.tp * SIDES + side
        self.send(
            jnp.logical_and(self.aligned, owner != self.fs),
            self.cols(m, 0, self.rows, side),
            self.at(m, self.fs, 0, self.rows),
            self.s_plane.at[m, side],
            self.r_main.at[m, self.fs],
            (owner, self.tp),
        )

    def send_down(self, when):
        for k, to in enumerate((self.peer, self.sibling)):
            self.send(
                when,
                self.down,
                self.column(self.tp),
                self.s_down.at[k],
                self.r_down.at[k],
                self.here(to),
            )

    def home_block(self):
        home = jnp.logical_and(self.aligned, self.primary)
        for m in range(2):
            for sem, to in ((self.s_over, self.peer), (self.s_main, self.sibling)):
                self.send(
                    home,
                    self.own(m),
                    self.at(m, self.fs, 0, self.rows),
                    sem.at[m, self.fs],
                    self.r_main.at[m, self.fs],
                    self.here(to),
                )

    def fold_down(self, trained, stage, sem):
        lanes = self.down.shape[1]
        mine = pl.ds(pl.multiple_of(self.tp * lanes, 128), lanes)

        def put(rows, tile):
            self.down[rows, :] = tile.astype(jnp.bfloat16)
            self.whole_down[rows, mine] = tile.astype(jnp.bfloat16)

        by_tiles(trained, stage, sem, put)

    def fold_wide(self, m, trained, scales, stage, sem):
        def put(rows, tile):
            self.sources[m][rows, :] = (scales[rows, :] * tile).astype(jnp.bfloat16)

        by_tiles(trained, stage, sem, put)

    def keep_folded(self):
        mine = pl.ds(pl.multiple_of(self.y * self.width, 128), self.width)

        def tile(index, carry):
            rows = pl.ds(pl.multiple_of(index * 16, 16), 16)
            first = pl.multiple_of(self.fs * self.rows + index * 16, 16)
            for m in range(2):
                self.wholes[m][pl.ds(first, 16), :] = self.sources[m][rows, mine]
            return carry

        def block():
            lax.fori_loop(0, self.rows // 16, tile, 0)

        guarded(jnp.logical_and(self.aligned, self.primary), block)

    def relay(self, m, side):
        zone = (1 - self.x) * CORES + self.c
        for k, (start, size) in enumerate(chunks(self.main)):
            held = self.passing.at[m, side, pl.ds(start, size)]
            guarded(self.aligned, landed, held, self.r_cross.at[m, side, k])
            self.send(
                self.aligned,
                held,
                self.at(m, self.fs, start, size),
                self.s_pass.at[m, side, k],
                self.r_main.at[m, self.fs],
                (zone * SIDES + side, self.tp),
            )

    def near(self, step):
        return self.half * 2 * SIDES + (self.fs + step) % (2 * SIDES)

    def far(self, step):
        return (1 - self.half) * 2 * SIDES + (self.fs + step) % (2 * SIDES)

    def whole_block(self, m, step):
        owner = self.near(step)
        block = self.at(m, owner, 0, self.rows)
        got = self.primary
        if step == 0:
            got = jnp.logical_and(got, jnp.logical_not(self.aligned))
        guarded(got, landed, block, self.r_main.at[m, owner])
        if step:
            self.send(
                jnp.logical_and(self.primary, self.aligned),
                block,
                block,
                self.s_over.at[m, owner],
                self.r_main.at[m, owner],
                self.here(self.peer),
            )
        self.send(
            got,
            block,
            block,
            self.s_main.at[m, owner],
            self.r_main.at[m, owner],
            self.here(self.sibling),
        )

    def pass_down(self):
        got = self.column(self.peer)
        landed(got, self.r_down.at[0])
        self.send(
            None, got, got, self.s_down.at[2], self.r_down.at[2], self.here(self.sibling)
        )

    def main_block(self, m, step):
        owner = self.far(step)
        block = self.at(m, owner, self.main_at, self.main)
        over = self.at(m, owner, self.over_at, self.part)
        guarded(self.primary, landed, block, self.r_main.at[m, owner])
        self.send(
            self.primary,
            over,
            over,
            self.s_over.at[m, owner],
            self.r_minor.at[m, owner],
            self.here(self.peer),
        )
        self.send(
            self.primary,
            block,
            block,
            self.s_main.at[m, owner],
            self.r_main.at[m, owner],
            self.here(self.sibling),
        )

    def minor_block(self, m, step):
        owner = self.far(step)
        block = self.at(m, owner, self.minor_at, self.part)
        guarded(self.primary, landed, block, self.r_minor.at[m, owner])
        self.send(
            self.primary,
            block,
            block,
            self.s_minor.at[m, owner],
            self.r_minor.at[m, owner],
            self.here(self.sibling),
        )

    def second(self):
        other = jnp.logical_not(self.primary)
        for m in range(2):
            for step in range(2 * SIDES):
                owner = self.near(step)
                block = self.at(m, owner, 0, self.rows)
                guarded(other, landed, block, self.r_main.at[m, owner])
                owner = self.far(step)
                block = self.at(m, owner, self.main_at, self.main)
                guarded(other, landed, block, self.r_main.at[m, owner])
                block = self.at(m, owner, self.minor_at, self.part)
                guarded(other, landed, block, self.r_minor.at[m, owner])
        landed(self.column(self.sibling), self.r_down.at[1])
        landed(self.column((1 - self.x) * CORES + 1 - self.c), self.r_down.at[2])


def guarded(when, act, *args):
    if when is None:
        act(*args)
    else:
        pl.when(when)(functools.partial(act, *args))


def beside_zone(zone):
    return zone + 1 - 2 * (zone % 2)


class Close:
    def __init__(self, place, send, partial_value, beside, halves, along, full, sems):
        self.__dict__.update(place)
        self.send = send
        self.partial_value, self.beside = partial_value, beside
        self.halves, self.along, self.full = halves, along, full
        (
            self.s_y,
            self.r_y,
            self.s_z,
            self.r_z,
            self.s_up,
            self.r_up,
            self.s_side,
            self.r_side,
        ) = sems
        self.zones = beside.shape[0]
        self.near = beside_zone(self.z)
        self.over = (self.z + 2) % self.zones
        self.last = beside_zone(self.over)

    def piece(self, zone, side):
        width = self.full.shape[2]
        first = (zone * SIDES + side) * width
        return pl.ds(pl.multiple_of(first, 128), width)

    def zone(self, step):
        return (self.z + self.zones + step) % self.zones

    def held(self, zone, side):
        return self.full.at[zone * SIDES + side]

    def scatter(self):
        for step in (*range(1, self.zones), 0):
            self.send(
                None,
                self.partial_value.at[:, self.piece(self.zone(step), 1 - self.y)],
                self.beside.at[step],
                self.s_y.at[step],
                self.r_y.at[step],
                (self.z * SIDES + 1 - self.y, self.tp),
            )

    def both_sides(self, step):
        landed(self.beside.at[step], self.r_y.at[step])
        mine = self.partial_value[:, self.piece(self.zone(step), self.y)]
        return mine.astype(jnp.float32) + self.beside[step].astype(jnp.float32)

    def halve(self):
        for step in range(1, self.zones):
            self.halves[step - 1] = self.both_sides(step).astype(jnp.bfloat16)
            self.send(
                None,
                self.halves.at[step - 1],
                self.along.at[step - 1],
                self.s_z.at[step - 1],
                self.r_z.at[step - 1],
                (self.zone(step) * SIDES + self.y, self.tp),
            )

    def to_side(self, step, block):
        self.send(
            None,
            block,
            block,
            self.s_side.at[step],
            self.r_side.at[step],
            (self.z * SIDES + 1 - self.y, self.tp),
        )

    def to_zone(self, kind, block, zone):
        self.send(
            None,
            block,
            block,
            self.s_up.at[kind],
            self.r_up.at[kind],
            (zone * SIDES + self.y, self.tp),
        )

    def spread(self):
        total = self.both_sides(0)
        for step in range(1, self.zones):
            landed(self.along.at[step - 1], self.r_z.at[step - 1])
            total += self.along[step - 1].astype(jnp.float32)
        self.full[self.fs] = total.astype(jnp.bfloat16)
        block = self.held(self.z, self.y)
        self.to_zone(0, block, self.over)
        self.to_zone(1, block, self.near)
        self.to_side(0, block)

    def pass_on(self):
        block = self.held(self.over, self.y)
        landed(block, self.r_up.at[0])
        self.to_zone(2, block, self.near)
        self.to_side(1, block)

    def side(self):
        for kind, zone in ((1, self.near), (2, self.last)):
            block = self.held(zone, self.y)
            landed(block, self.r_up.at[kind])
            self.to_side(kind + 1, block)

    def norm(self, normed, scales, out):
        for step, zone in enumerate((self.z, self.over, self.near, self.last)):
            landed(self.held(zone, 1 - self.y), self.r_side.at[step])

        def mixed(some):
            block = jnp.concatenate(
                [
                    self.full[k, some, :].astype(jnp.float32)
                    for k in range(self.full.shape[0])
                ],
                axis=1,
            )
            old = 1.6817928 * scales[...] * normed[some, :].astype(jnp.float32)
            return old + 0.5 * block

        norm_rows(mixed, out)


def norm_rows(values, out):
    tall = 16

    def some_rows(index, carry):
        some = pl.ds(pl.multiple_of(index * tall, tall), tall)
        out[some, :] = plain_norm(values(some)).astype(jnp.bfloat16)
        return carry

    lax.fori_loop(0, out.shape[0] // tall, some_rows, 0)


def greet(partners, meanwhile=None):
    barrier = pltpu.get_barrier_semaphore()
    for partner in partners:
        pl.semaphore_signal(barrier, inc=1, device_id=partner, device_id_type=MESH)
    if meanwhile is not None:
        meanwhile()
    pl.semaphore_wait(barrier, len(partners))


def by_tiles(src, stage, sem, put):
    tall = stage.shape[1]
    count = src.shape[0] // tall

    def fetch(k):
        return pltpu.make_async_copy(
            src.at[pl.ds(k * tall, tall), :], stage.at[k % 2], sem.at[k % 2]
        )

    fetch(0).start()
    for k in range(count):
        if k + 1 < count:
            fetch(k + 1).start()
        fetch(k).wait()

        def tile(index, carry, k=k):
            first = pl.multiple_of(index * 16, 16)
            rows = pl.ds(pl.multiple_of(k * tall + index * 16, 16), 16)
            put(rows, stage[k % 2, pl.ds(first, 16), :])
            return carry

        lax.fori_loop(0, tall // 16, tile, 0)


def close_scratch(rows, width, count):
    held = lambda many: pltpu.VMEM((many, rows, width // count), jnp.bfloat16)
    zones = count // SIDES
    dma = pltpu.SemaphoreType.DMA
    sems = [dma((many,)) for many in (zones, zones - 1, zones - 1, zones)]
    return [held(zones), held(zones - 1), held(zones - 1), held(count)] + [
        sem for sem in sems for _ in range(2)
    ]


def placing():
    fs = lax.axis_index("fs")
    tp = lax.axis_index("tp")
    z, x, c = fs // SIDES, tp // CORES, tp % CORES
    return dict(
        fs=fs,
        tp=tp,
        z=z,
        y=fs % SIDES,
        x=x,
        c=c,
        half=z // 2,
        aligned=x == z // 2,
        primary=c == z % 2,
        peer=(1 - x) * CORES + c,
        sibling=x * CORES + 1 - c,
    )


def sender():
    started = []

    def send(*args):
        one = Send(*args)
        one.start()
        started.append(one)

    return send, started


def multiply(normed, weights, sums, partial_value):
    gate, up, down = weights
    deep = gate.shape[0] // CUTS
    wide = down.shape[1] // CUTS
    for k in range(CUTS):
        n = normed[:, k * deep : (k + 1) * deep]
        for weight, total in zip((gate, up), sums):
            term = jnp.dot(
                n,
                weight[k * deep : (k + 1) * deep, :],
                preferred_element_type=jnp.float32,
            )
            if k:
                total[...] += term
            else:
                total[...] = term
    hidden = (jax.nn.silu(sums[0][...]) * sums[1][...]).astype(jnp.bfloat16)
    for k in range(CUTS):
        partial_value[:, k * wide : (k + 1) * wide] = jnp.dot(
            hidden,
            down[:, k * wide : (k + 1) * wide],
            preferred_element_type=jnp.float32,
        ).astype(jnp.bfloat16)


def collect_kernel(*refs):
    (tg1, tu1, t1, tg2, tu2, t2, tokens, scales), refs = refs[:8], refs[8:]
    picks, refs = refs[:2], refs[2:]
    (w1, v1, x1, w2, v2, x2, out), refs = refs[:7], refs[7:]
    (passing, folded, d1, d2), refs = refs[:4], refs[4:]
    (stage_wide, stage_down, stage_sem), refs = refs[:3], refs[3:]
    (gate_sum, up_sum), refs = refs[:2], refs[2:]
    (normed, partial_value), refs = refs[:2], refs[2:]
    sems, refs = refs[:11], refs[11:]
    close_scratches = refs
    place = placing()
    fs, tp = place["fs"], place["tp"]
    count = lax.axis_size("fs")
    aligned = place["aligned"]
    unaligned = jnp.logical_not(aligned)
    send, started = sender()
    one, two = (
        Hand(
            place,
            send,
            (gate, up),
            (whole_gate, whole_up),
            down,
            whole_down,
            passing.at[h],
            [sem.at[h] for sem in sems],
        )
        for h, (gate, up, down, whole_gate, whole_up, whole_down) in enumerate(
            (
                (folded.at[0], folded.at[1], d1, w1, v1, x1),
                (folded.at[2], folded.at[3], d2, w2, v2, x2),
            )
        )
    )
    close = Close(place, send, partial_value, *close_scratches[:4], close_scratches[4:])
    turns = [(m, side) for m in range(2) for side in range(SIDES)]

    def first_folds():
        one.fold_wide(0, tg1, picks[0], stage_wide, stage_sem.at[1])

    greet(
        [((fs + step) % count, tp) for step in range(1, count)]
        + [(fs, place["peer"]), (fs, place["sibling"])],
        first_folds,
    )

    for m in range(2):
        if m:
            one.fold_wide(1, tu1, picks[0], stage_wide, stage_sem.at[1])
        for side in range(SIDES):
            one.cross(m, side)
            one.plane_far(m, side)
            one.plane_near(m, side)
    one.fold_down(t1, stage_down, stage_sem.at[0])
    one.send_down(None)
    one.home_block()
    one.keep_folded()
    one.relay(0, 0)
    two.fold_wide(0, tg2, picks[1], stage_wide, stage_sem.at[1])
    two.fold_wide(1, tu2, picks[1], stage_wide, stage_sem.at[1])
    two.fold_down(t2, stage_down, stage_sem.at[0])
    two.keep_folded()
    two.cross(0, 0)
    two.plane_far(0, 0)
    one.whole_block(0, 0)
    one.whole_block(0, 1)
    one.relay(0, 1)
    one.whole_block(0, 2)
    one.whole_block(0, 3)
    one.relay(1, 0)
    one.whole_block(1, 0)
    one.whole_block(1, 1)
    one.relay(1, 1)
    one.whole_block(1, 2)
    one.whole_block(1, 3)
    for m, side in turns:
        two.plane_near(m, side)
    norm_rows(lambda some: tokens[some, :], normed)
    one.pass_down()
    for step in range(2 * SIDES):
        one.main_block(0, step)
    two.home_block()
    two.cross(0, 1)
    two.plane_far(0, 1)
    two.relay(0, 0)
    for step in range(2 * SIDES):
        one.main_block(1, step)
    two.send_down(aligned)
    for step in range(2 * SIDES):
        one.minor_block(0, step)
    for step in range(2 * SIDES):
        one.minor_block(1, step)
    two.relay(0, 1)
    one.second()
    two.cross(1, 0)
    multiply(
        normed,
        (w1, v1, x1),
        (gate_sum, up_sum),
        partial_value,
    )
    close.scatter()
    two.cross(1, 1)
    two.send_down(unaligned)
    two.whole_block(0, 0)
    close.halve()
    two.plane_far(1, 0)
    two.relay(1, 0)
    two.whole_block(0, 1)
    two.whole_block(0, 2)
    close.spread()
    two.plane_far(1, 1)
    two.relay(1, 1)
    two.whole_block(0, 3)
    two.whole_block(1, 0)
    two.whole_block(1, 1)
    two.whole_block(1, 2)
    two.whole_block(1, 3)
    close.pass_on()
    two.pass_down()
    for step in range(2 * SIDES):
        two.main_block(0, step)
    close.side()
    for step in range(2 * SIDES):
        two.main_block(1, step)
    close.norm(normed, scales, out)
    for step in range(2 * SIDES):
        two.minor_block(0, step)
    for step in range(2 * SIDES):
        two.minor_block(1, step)
    two.second()
    for copy in started:
        copy.wait_send()


def collect(first, second, tokens, scales, picks):
    gate, _, down = first
    rows, columns = gate.shape
    fs, tp = lax.axis_size("fs"), lax.axis_size("tp")
    width = columns * tp // fs
    main = rows - far_part(rows)
    tall, wide = tokens.shape
    whole = pltpu.VMEM((rows * fs, width), jnp.bfloat16)
    whole_down = pltpu.VMEM((down.shape[0], down.shape[1] * tp), jnp.bfloat16)
    any_place = pl.BlockSpec(memory_space=pl.ANY)
    vmem = pl.BlockSpec(memory_space=pltpu.VMEM)
    dma = pltpu.SemaphoreType.DMA
    held = lambda *shape: pltpu.VMEM(shape, jnp.bfloat16)
    relayed = dma((2, 2, SIDES, CHUNKS))
    by_owner = dma((2, 2, fs))
    *weights, normed_one = pl.pallas_call(
        collect_kernel,
        out_shape=(whole, whole, whole_down) * 2
        + (pltpu.VMEM(tokens.shape, tokens.dtype),),
        in_specs=[any_place] * 6 + [vmem] * 4,
        out_specs=(vmem,) * 7,
        scratch_shapes=[
            held(2, 2, SIDES, main, width),
            held(4, *gate.shape),
            held(*down.shape),
            held(*down.shape),
            pltpu.VMEM((2, gate.shape[0] // CUTS, gate.shape[1]), jnp.float32),
            pltpu.VMEM((2, down.shape[0] // CUTS, down.shape[1]), jnp.float32),
            dma((2, 2)),
            pltpu.VMEM((tall, width), jnp.float32),
            pltpu.VMEM((tall, width), jnp.float32),
            held(tall, wide),
            held(tall, wide),
            dma((2, 2, SIDES)),
            relayed,
            relayed,
            relayed,
            by_owner,
            by_owner,
            by_owner,
            by_owner,
            by_owner,
            dma((2, 3)),
            dma((2, 3)),
            *close_scratch(tall, wide, fs),
        ],
        compiler_params=pltpu.CompilerParams(
            has_side_effects=True, collective_id=0, vmem_limit_bytes=COLLECT_VMEM
        ),
    )(*first, *second, tokens, scales[None, :], *(pick[:, None] for pick in picks))
    return weights[:3], weights[3:], normed_one


def in_vmem(*arrays):
    return [pltpu.with_memory_space_constraint(a, pltpu.VMEM) for a in arrays]


def serve_kernel(*refs):
    normed, refs = refs[0], refs[1:]
    weights, served, refs = refs[:6], refs[6:12], refs[12:]
    partial_value, gate_sum, up_sum, leave = refs
    copies = [
        pltpu.make_async_copy(weights[m], served[m], leave.at[m]) for m in range(6)
    ]
    for copy in copies:
        copy.start()
    multiply(normed, weights[3:], (gate_sum, up_sum), partial_value)
    for copy in copies:
        copy.wait()


def serve(normed, first, second):
    rows, width = normed.shape
    gate = first[0]
    vmem = pl.BlockSpec(memory_space=pltpu.VMEM)
    any_place = pl.BlockSpec(memory_space=pl.ANY)
    same = lambda a: jax.ShapeDtypeStruct(a.shape, a.dtype)
    weights = (*first, *second)
    sums = pltpu.VMEM((rows, gate.shape[1]), jnp.float32)
    *served, partial_value = pl.pallas_call(
        serve_kernel,
        out_shape=tuple(same(a) for a in weights)
        + (pltpu.VMEM(normed.shape, normed.dtype),),
        in_specs=[vmem] * 7,
        out_specs=(any_place,) * 6 + (vmem,),
        scratch_shapes=[sums, sums, pltpu.SemaphoreType.DMA((6,))],
        compiler_params=pltpu.CompilerParams(vmem_limit_bytes=SERVE_VMEM),
        cost_estimate=pl.CostEstimate(
            flops=6 * rows * gate.size, bytes_accessed=12 * gate.size, transcendentals=0
        ),
    )(*in_vmem(normed, *weights))
    return served[:3], served[3:], partial_value


def close_kernel(partial_value, normed, scales, out, *scratches):
    place = placing()
    send, started = sender()
    close = Close(place, send, partial_value, *scratches[:4], scratches[4:])
    greet(
        [(close.zone(step) * SIDES + close.y, close.tp) for step in range(1, close.zones)]
        + [(close.z * SIDES + 1 - close.y, close.tp)]
    )
    close.scatter()
    close.halve()
    close.spread()
    close.pass_on()
    close.side()
    close.norm(normed, scales, out)
    for copy in started:
        copy.wait_send()


def close(partial_value, normed, scales):
    rows, width = normed.shape
    vmem = pl.BlockSpec(memory_space=pltpu.VMEM)
    return pl.pallas_call(
        close_kernel,
        out_shape=pltpu.VMEM((rows, width), jnp.bfloat16),
        in_specs=[vmem] * 3,
        out_specs=vmem,
        scratch_shapes=close_scratch(rows, width, lax.axis_size("fs")),
        compiler_params=pltpu.CompilerParams(
            has_side_effects=True, collective_id=1, vmem_limit_bytes=SERVE_VMEM
        ),
    )(*in_vmem(partial_value, normed), scales[None, :])


def on_device(
    use_kernels,
    tokens,
    gain_first,
    gain_second,
    gate_first,
    up_first,
    down_first,
    gate_second,
    up_second,
    down_second,
):
    row_count = gate_first.shape[0]
    offset = lax.axis_index("fs") * row_count
    pick = lambda scales: lax.dynamic_slice_in_dim(scales, offset, row_count, 0)

    def fold_gain(weight, scales):
        return (pick(scales)[:, None] * weight).astype(jnp.bfloat16)

    if use_kernels:
        first, second, normed_one = collect(
            (gate_first, up_first, down_first),
            (gate_second, up_second, down_second),
            tokens,
            gain_first,
            (pick(gain_first), pick(gain_second)),
        )
        first, second, partial_value = serve(normed_one, first, second)
        result_rows = close(partial_value, normed_one, gain_second)
    else:
        first = collect_plain(
            fold_gain(gate_first, gain_first),
            fold_gain(up_first, gain_first),
            down_first.astype(jnp.bfloat16),
        )
        second = collect_plain(
            fold_gain(gate_second, gain_second),
            fold_gain(up_second, gain_second),
            down_second.astype(jnp.bfloat16),
        )
        normed_zero = plain_norm(tokens).astype(jnp.bfloat16)
        normed_one = half_step_plain(normed_zero, gain_first, *first)
        result_rows = half_step_plain(normed_one, gain_second, *second)
    return (result_rows, *first, *second)


def solution(mesh):
    fs, tp = mesh.shape["fs"], mesh.shape["tp"]
    use_kernels = tp == 2 * CORES and fs == tp * SIDES
    placed = (P("tp", None), P(), P()) + (P("fs", "tp"),) * 6
    served = (P(None, "fs"), P(None, "fs"), P("fs", None))
    return jax.shard_map(
        functools.partial(on_device, use_kernels),
        mesh=mesh,
        in_specs=placed,
        out_specs=(P("tp", None),) + served + served,
        check_vma=False,
    )
```
